128 devices in a mesh: sp: 16 (over z, x), tp: 8 (over y, core).
Axes of the slice: x: 4, y: 4, z: 4, core: 2. Of those that a mesh axis runs over, the one named last changes fastest.
Arguments:
- tokens: bfloat16 [16384, 4096], P('sp'), may hold values from -6 to 6
- input_norm_scale: bfloat16 [4096], replicated, may hold values from 0.099609375 to 1.8984375
- mean_input_weight: bfloat16 [4096, 2048], P('sp', 'tp'), may hold values from -0.09375 to 0.09375
- query_matrix: bfloat16 [4096, 2048], P('sp', 'tp'), may hold values from -0.09375 to 0.09375
- key_matrix: bfloat16 [4096, 2048], P('sp', 'tp'), may hold values from -0.09375 to 0.09375
- value_matrix: bfloat16 [4096, 2048], P('sp', 'tp'), may hold values from -0.09375 to 0.09375
- strength_weight: bfloat16 [4096, 16], P('sp', 'tp'), may hold values from -0.09375 to 0.09375
- decay_input_weight: bfloat16 [4096, 16], P('sp', 'tp'), may hold values from -0.25 to 0.25
- causal_filter_weight: bfloat16 [4, 3, 2048], replicated, may hold values from -3 to 3
- head_decay_logrates: float32 [16], replicated, may hold values from -13.2 to -2.9
- decay_input_shift: float32 [16], replicated, may hold values from -1 to 1
- strength_shift: float32 [16], replicated, may hold values from -5 to -3
- decay_spike: float32 [16384, 16], P('sp', 'tp'), may hold values from -1.3 to 0
- head_norm_scale: bfloat16 [128], replicated, may hold values from 0.099609375 to 1.8984375
- group_mixing_weight: bfloat16 [16, 128, 128], replicated, may hold values from -0.5 to 0.5
- mean_channel_scale: bfloat16 [2048], replicated, may hold values from 0.099609375 to 1.8984375
- mean_output_weight: bfloat16 [2048, 4096], P('tp', 'sp'), may hold values from -0.09375 to 0.09375
- delta_output_weight: bfloat16 [2048, 4096], P('tp', 'sp'), may hold values from -0.09375 to 0.09375
Outputs:
- mixed_out: bfloat16 [16384, 4096], P(('sp', 'tp'))
The draws below stay inside these ranges and needn't reach their ends.
All inputs are finite; a program needn't handle non-finite values.
Results may differ from the reference program's by a relative error of at most 0.015.
Values may be sent and summed in bfloat16 or wider, within the bound.
A program may use at most 128 MiB of HBM per device.

```python
import jax
import jax.numpy as jnp
from jax import lax

D = 4096
POOL_GROUPS = 16
GROUP_DIM = 128
MIXER_HEADS = 16
HEAD_DIM = 128
CONV = 4
BLOCK = 64
TOK_DEV = 1024
POOL_W = 2048
GDN_W = 2048
SEQUENCE_TOKENS = 16384
N_TP = 8


def draw_head_decay_logrates(key, part):
    ranking = jax.random.permutation(jax.random.fold_in(key, 11), MIXER_HEADS)
    fast_count = MIXER_HEADS // 2
    fast_rate = jax.random.uniform(jax.random.fold_in(key, 12), (MIXER_HEADS,), jnp.float32, jnp.log(0.012), jnp.log(0.035))
    slow_rate = jax.random.uniform(jax.random.fold_in(key, 13), (MIXER_HEADS,), jnp.float32, jnp.log(2e-06), jnp.log(2e-05))
    return jnp.where(ranking < fast_count, fast_rate, slow_rate).astype(jnp.float32)


def draw_decay_spike(key, part):
    block_ids = jnp.arange(SEQUENCE_TOKENS) // TOK_DEV
    block_rates = jnp.exp(jax.random.uniform(jax.random.fold_in(key, 21), (SEQUENCE_TOKENS // TOK_DEV, MIXER_HEADS), jnp.float32, jnp.log(1e-06), jnp.log(2e-05)))
    stable_portion = -block_rates[block_ids]
    spike_rows = jax.random.randint(jax.random.fold_in(key, 22), (2, MIXER_HEADS), 0, SEQUENCE_TOKENS)
    error_values = jax.random.uniform(jax.random.fold_in(key, 23), (2, MIXER_HEADS), jnp.float32, 0.2, 0.45)
    match_flags = jnp.arange(SEQUENCE_TOKENS)[:, None, None] == spike_rows[None, :, :]
    spike_portion = jnp.sum(jnp.where(match_flags, jnp.log(1.0 - error_values)[None, :, :], 0.0), axis=1)
    return (stable_portion + spike_portion).astype(jnp.float32)


def block_levels(stream_key, dims, split, smallest, largest):
    factor_of, own = 1.0, jax.random.fold_in(stream_key, 6)
    for dim, shards_of in split:
        heights = jnp.exp(jax.random.uniform(jax.random.fold_in(own, dim), (shards_of,), jnp.float32, smallest / len(split), largest / len(split)))
        factor_of = factor_of * jnp.repeat(heights, dims[dim] // shards_of).reshape([-1 if axis == dim else 1 for axis in range(len(dims))])
    return factor_of


def bell_draw(own_key, shape, scale, reach, split=(), held_as=jnp.bfloat16):
    drawn = jax.random.normal(own_key, shape, jnp.float32) * scale
    if len(split) > 0:
        drawn = block_levels(own_key, shape, split, -0.22, 0.18) * drawn
    return jnp.clip(drawn, min=-reach, max=reach).astype(held_as)


def setup_inputs(seed: int = 0) -> dict:
    seeds = jax.random.split(jax.random.key(seed), 19)
    return {
        "tokens": bell_draw(seeds[0], (SEQUENCE_TOKENS, D), 1.0, 6.0, ((0, 16),)),
        "input_norm_scale": jnp.clip(1.0 + 0.18 * jax.random.normal(seeds[1], (D,), jnp.float32), 0.099609375, 1.8984375).astype(jnp.bfloat16),
        "mean_input_weight": bell_draw(seeds[2], (D, POOL_W), D ** -0.5, 0.09375, ((0, 16), (1, 8))),
        "query_matrix": bell_draw(seeds[3], (D, GDN_W), D ** -0.5, 0.09375, ((0, 16), (1, 8))),
        "key_matrix": bell_draw(seeds[4], (D, GDN_W), D ** -0.5, 0.09375, ((0, 16), (1, 8))),
        "value_matrix": bell_draw(seeds[5], (D, GDN_W), D ** -0.5, 0.09375, ((0, 16), (1, 8))),
        "strength_weight": bell_draw(seeds[6], (D, MIXER_HEADS), D ** -0.5, 0.09375, ((0, 16), (1, 8))),
        "decay_input_weight": bell_draw(seeds[7], (D, MIXER_HEADS), (D // 9) ** -0.5, 0.25, ((0, 16), (1, 8))),
        "causal_filter_weight": bell_draw(seeds[8], (CONV, 3, GDN_W), CONV ** -0.5, 3.0),
        "head_decay_logrates": draw_head_decay_logrates(jax.random.fold_in(seeds[18], 71), 0),
        "decay_input_shift": jnp.clip(jax.random.uniform(seeds[10], (MIXER_HEADS,), jnp.float32, -1.0, 1.0), -1.0, 1.0),
        "strength_shift": jnp.clip(jax.random.uniform(seeds[11], (MIXER_HEADS,), jnp.float32, -5.0, -3.0), -5.0, -3.0),
        "decay_spike": draw_decay_spike(jax.random.fold_in(seeds[18], 71), 0),
        "head_norm_scale": jnp.clip(1.0 + 0.18 * jax.random.normal(seeds[13], (HEAD_DIM,), jnp.float32), 0.099609375, 1.8984375).astype(jnp.bfloat16),
        "group_mixing_weight": bell_draw(seeds[14], (POOL_GROUPS, GROUP_DIM, GROUP_DIM), GROUP_DIM ** -0.5, 0.5),
        "mean_channel_scale": jnp.clip(1.0 + 0.18 * jax.random.normal(seeds[15], (POOL_W,), jnp.float32), 0.099609375, 1.8984375).astype(jnp.bfloat16),
        "mean_output_weight": bell_draw(seeds[16], (POOL_W, D), (POOL_W + GDN_W) ** -0.5, 0.09375, ((0, 8), (1, 16))),
        "delta_output_weight": bell_draw(seeds[17], (GDN_W, D), (POOL_W + GDN_W) ** -0.5, 0.09375, ((0, 8), (1, 16))),
    }


EPSILON = 1e-06

def scale_rows(values, gain_vec):
    squares = lax.optimization_barrier(jnp.mean(values * values, axis=-1, keepdims=True))
    return values * lax.rsqrt(squares + EPSILON) * gain_vec.astype(jnp.float32)

def unit_rows(values):
    return values * lax.rsqrt(lax.optimization_barrier(jnp.sum(values * values, axis=-1, keepdims=True)) + EPSILON)

def causal_taps(extended, taps, rows_out):
    tap_sum = jnp.zeros((rows_out, taps.shape[1]), jnp.float32)
    for tap_index in range(taps.shape[0]):
        tap_sum = tap_sum + taps[tap_index] * extended[tap_index:tap_index + rows_out]
    return jax.nn.silu(tap_sum)

def pool_means(previous, current, group_ids, positions):
    pool_reach = 15
    rows_out = current.shape[0]
    extended = jnp.concatenate([previous, current], axis=0).astype(jnp.float32)
    window_size = jnp.left_shift(jnp.int32(2), (group_ids % 4).astype(jnp.int32))
    windowed = jnp.zeros(current.shape, jnp.float32)
    for lag_rows in range(pool_reach + 1):
        shifted = extended[pool_reach - lag_rows:pool_reach - lag_rows + rows_out]
        windowed = windowed + jnp.where(lag_rows < window_size[None, :], shifted, 0.0)
    counts = jnp.minimum(positions[:, None] + 1, window_size[None, :]).astype(jnp.float32)
    return (windowed / counts - extended[pool_reach:]).astype(jnp.bfloat16)

def block_terms(query, keys, values, decay_logarithm, beta):
    blocks = keys.shape[0] // BLOCK

    def to_blocks(tensor):
        return jnp.swapaxes(tensor.reshape((blocks, BLOCK) + tensor.shape[1:]), 1, 2)
    query_b = to_blocks(query)
    keys_b = to_blocks(keys)
    values_b = to_blocks(values)
    decay_b = to_blocks(decay_logarithm)
    beta_b = to_blocks(beta)
    cumulative = jnp.cumsum(decay_b, axis=-1)
    positions = jnp.arange(BLOCK)
    causal = positions[:, None] >= positions[None, :]
    strict = positions[:, None] > positions[None, :]
    spread = cumulative[..., :, None] - cumulative[..., None, :]
    weights = jnp.where(causal, jnp.exp(jnp.where(causal, spread, 0.0)), 0.0)
    keys_beta = keys_b * beta_b[..., None]
    values_beta = values_b * beta_b[..., None]
    intersection = jnp.einsum('nhid,nhjd->nhij', keys_beta, keys_b, precision=lax.Precision.HIGHEST)
    lower_part = jnp.where(strict, intersection * weights, 0.0) + jnp.eye(BLOCK, dtype=jnp.float32)
    right_side = jnp.concatenate([values_beta, keys_beta * jnp.exp(cumulative)[..., None]], axis=-1)
    solved = jax.scipy.linalg.solve_triangular(lower_part, right_side, lower=True, unit_diagonal=True)
    value_depth = values.shape[-1]
    update = solved[..., :value_depth]
    project = solved[..., value_depth:]
    scores = jnp.einsum('nhid,nhjd->nhij', query_b, keys_b, precision=lax.Precision.HIGHEST) * weights
    query_dec = query_b * jnp.exp(cumulative)[..., None]
    keys_dec = keys_b * jnp.exp(cumulative[..., -1:] - cumulative)[..., None]
    carry_decay = jnp.exp(cumulative[..., -1])
    return (scores, query_dec, keys_dec, update, project, carry_decay)

def run_blocks(state, terms):

    def advance(carried, inputs):
        scores, query_dec, keys_dec, update, project, carry_decay = inputs
        fresh = update - jnp.einsum('hcd,hde->hce', project, carried, precision=lax.Precision.HIGHEST)
        output = jnp.einsum('hcd,hde->hce', query_dec, carried, precision=lax.Precision.HIGHEST)
        output = output + jnp.einsum('hij,hje->hie', scores, fresh, precision=lax.Precision.HIGHEST)
        carried = carried * carry_decay[:, None, None] + jnp.einsum('hcd,hce->hde', keys_dec, fresh, precision=lax.Precision.HIGHEST)
        return (carried, output)
    final_state, outputs = lax.scan(advance, state, terms)
    return outputs

def reference(tokens, input_norm_scale, mean_input_weight, query_matrix, key_matrix, value_matrix, strength_weight, decay_input_weight, causal_filter_weight, head_decay_logrates, decay_input_shift, strength_shift, decay_spike, head_norm_scale, group_mixing_weight, mean_channel_scale, mean_output_weight, delta_output_weight):
    normed = scale_rows(tokens.astype(jnp.float32), input_norm_scale).astype(jnp.bfloat16)
    pool_raw = jnp.dot(normed.astype(jnp.float32), mean_input_weight.astype(jnp.float32), preferred_element_type=jnp.float32).astype(jnp.bfloat16)
    query_raw = jnp.dot(normed.astype(jnp.float32), query_matrix.astype(jnp.float32), preferred_element_type=jnp.float32).astype(jnp.bfloat16)
    key_raw = jnp.dot(normed.astype(jnp.float32), key_matrix.astype(jnp.float32), preferred_element_type=jnp.float32).astype(jnp.bfloat16)
    value_raw = jnp.dot(normed.astype(jnp.float32), value_matrix.astype(jnp.float32), preferred_element_type=jnp.float32).astype(jnp.bfloat16)
    beta_raw = jnp.dot(normed.astype(jnp.float32), strength_weight.astype(jnp.float32), preferred_element_type=jnp.float32).astype(jnp.bfloat16)
    decay_unshaped = jnp.dot(normed.astype(jnp.float32), decay_input_weight.astype(jnp.float32), preferred_element_type=jnp.float32).astype(jnp.bfloat16)
    qkv_raw = jnp.concatenate([query_raw, key_raw, value_raw], axis=1)
    extended_qkv = jnp.concatenate([jnp.zeros((CONV - 1, 3 * GDN_W), jnp.bfloat16), qkv_raw], axis=0).astype(jnp.float32)
    convolved = causal_taps(extended_qkv, causal_filter_weight.reshape(CONV, 3 * GDN_W).astype(jnp.float32), SEQUENCE_TOKENS)
    query = unit_rows(convolved[:, :GDN_W].reshape(SEQUENCE_TOKENS, MIXER_HEADS, HEAD_DIM)) * HEAD_DIM ** (-0.5)
    keys = unit_rows(convolved[:, GDN_W:2 * GDN_W].reshape(SEQUENCE_TOKENS, MIXER_HEADS, HEAD_DIM))
    values = convolved[:, 2 * GDN_W:].reshape(SEQUENCE_TOKENS, MIXER_HEADS, HEAD_DIM)
    beta = jax.nn.sigmoid(beta_raw.astype(jnp.float32) + strength_shift)
    decay_logarithm = -jnp.exp(head_decay_logrates) * jax.nn.softplus(decay_unshaped.astype(jnp.float32) + decay_input_shift) + decay_spike
    terms = block_terms(query, keys, values, decay_logarithm, beta)
    outputs = run_blocks(jnp.zeros((MIXER_HEADS, HEAD_DIM, HEAD_DIM), jnp.float32), terms)
    delta_rows = jnp.swapaxes(outputs, 1, 2).reshape(SEQUENCE_TOKENS, MIXER_HEADS, HEAD_DIM)
    delta_mixed = scale_rows(delta_rows, head_norm_scale).astype(jnp.bfloat16).reshape(SEQUENCE_TOKENS, GDN_W)
    group_ids = (jnp.arange(POOL_W) // GROUP_DIM).astype(jnp.int32)
    positions = jnp.arange(SEQUENCE_TOKENS).astype(jnp.int32)
    pool_diff = pool_means(jnp.zeros((15, POOL_W), jnp.bfloat16), pool_raw, group_ids, positions)
    pooled = jnp.einsum('tgc,gcd->tgd', pool_diff.astype(jnp.float32).reshape(SEQUENCE_TOKENS, POOL_GROUPS, GROUP_DIM), group_mixing_weight.astype(jnp.float32))
    pool_mixed = (pooled.reshape(SEQUENCE_TOKENS, POOL_W) * mean_channel_scale.astype(jnp.float32)).astype(jnp.bfloat16)
    pool_slice = POOL_W // N_TP
    delta_slice = GDN_W // N_TP
    summed = jnp.zeros((SEQUENCE_TOKENS, D), jnp.float32)
    for shard_index in range(N_TP):
        pool_part = pool_mixed[:, shard_index * pool_slice:(shard_index + 1) * pool_slice]
        delta_part = delta_mixed[:, shard_index * delta_slice:(shard_index + 1) * delta_slice]
        rows_in = jnp.concatenate([pool_part, delta_part], axis=1)
        weight_rows = jnp.concatenate([mean_output_weight[shard_index * pool_slice:(shard_index + 1) * pool_slice], delta_output_weight[shard_index * delta_slice:(shard_index + 1) * delta_slice]], axis=0)
        partial_sum = jnp.dot(rows_in.astype(jnp.float32), weight_rows.astype(jnp.float32), preferred_element_type=jnp.float32).astype(jnp.bfloat16)
        summed = summed + partial_sum.astype(jnp.float32)
    return summed.astype(jnp.bfloat16)
```

```python
import jax
import jax.numpy as jnp
from jax import lax
from jax.experimental import pallas as pl
from jax.experimental.pallas import tpu as pltpu
from jax.sharding import Mesh
from jax.sharding import PartitionSpec as P

GROUP_DIM = 128
HEAD_DIM = 128
CONV = 4
CHUNK = 256
HALO = 16
EPSILON = 1e-06
SP = ("sp_0", "sp_1")
SP_TP = ("sp_0", "sp_1", "tp")
MESH_ID = pl.DeviceIdType.MESH
F32 = jnp.float32
BF16 = jnp.bfloat16
VMEM_LIMIT = 60 * 1024 * 1024


def dot(a, b):
    return jnp.dot(a, b, preferred_element_type=F32)


def dot_nt(a, b):
    return lax.dot_general(a, b, (((1,), (1,)), ((), ())), preferred_element_type=F32)


def dot_tn(a, b):
    return lax.dot_general(a, b, (((0,), (0,)), ((), ())), preferred_element_type=F32)


def unit_rows(values):
    return values * lax.rsqrt(jnp.sum(values * values, axis=-1, keepdims=True) + EPSILON)


def fill_masks(masks_ref):
    rows = lax.broadcasted_iota(jnp.int32, (CHUNK, CHUNK), 0)
    cols = lax.broadcasted_iota(jnp.int32, (CHUNK, CHUNK), 1)
    apart = jnp.bitwise_xor(rows, cols)
    for level in range(masks_ref.shape[0]):
        inside = (rows > cols) & (apart >= 2**level) & (apart < 2 ** (level + 1))
        masks_ref[level] = jnp.where(inside, 1.0, 0.0).astype(BF16)


def fill_gates(beta, decay, grow_ref, gcol_ref, bcol_ref):
    lane = lax.broadcasted_iota(jnp.int32, decay.shape, 1)
    total = decay
    step = 1
    while step < CHUNK:
        total = total + jnp.where(lane >= step, pltpu.roll(total, step, 1), 0.0)
        step *= 2
    for row in range(decay.shape[0]):
        grow_ref[row] = jnp.broadcast_to(total[row : row + 1], (8, CHUNK))
        gcol_ref[row] = jnp.broadcast_to(total[row : row + 1], (128, CHUNK)).T
        bcol_ref[row] = jnp.broadcast_to(beta[row : row + 1], (128, CHUNK)).T


def conv_rows(raw_ref, taps_ref, start, part):
    lanes = slice(part * 128, part * 128 + 128)
    rows = raw_ref[pl.ds(pl.multiple_of(start + HALO - 8, 8), CHUNK + 8), lanes]
    mixed = taps_ref[CONV - 1 : CONV, lanes] * rows[8:]
    for back in range(1, CONV):
        tap = taps_ref[CONV - 1 - back : CONV - back, lanes]
        mixed = mixed + tap * pltpu.roll(rows, back, 0)[8:]
    return mixed / (1.0 + jnp.exp(-mixed))


def delta_chunk(chunk, heads, chunks, raw_ref, taps_ref, grow_ref, gcol_ref, bcol_ref, masks_ref,
                map_ref, from_state_ref, local_ref):
    start = chunk * CHUNK
    rows = lax.broadcasted_iota(jnp.int32, (CHUNK, CHUNK), 0)
    cols = lax.broadcasted_iota(jnp.int32, (CHUNK, CHUNK), 1)
    work = []
    for head in range(heads):
        row = head * chunks + chunk
        query = unit_rows(conv_rows(raw_ref, taps_ref, start, head)) * HEAD_DIM ** (-0.5)
        key = unit_rows(conv_rows(raw_ref, taps_ref, start, heads + head))
        value = conv_rows(raw_ref, taps_ref, start, 2 * heads + head)
        gcol, bcol, grow = gcol_ref[row], bcol_ref[row], grow_ref[row][0:1]
        key_b = key.astype(BF16)
        both = jnp.concatenate([query.astype(BF16), key_b], axis=0)
        inner = dot_nt(both, key_b)
        spread = jnp.exp(jnp.minimum(jnp.concatenate([gcol, gcol], axis=1) - grow, 0.0))
        scores = jnp.where(rows >= cols, inner[:CHUNK] * spread, 0.0).astype(BF16)
        strict = jnp.where(rows > cols, inner[CHUNK:] * spread, 0.0)
        strict = (strict * jnp.concatenate([bcol, bcol], axis=1)).astype(BF16)
        grown = jnp.exp(gcol)
        right = jnp.concatenate([value * bcol, key * bcol * grown], axis=1).astype(BF16)
        last = grow[:, CHUNK - 1 : CHUNK]
        key_dec = (key * jnp.exp(last - gcol)).astype(BF16)
        inverse = jnp.where(rows == cols, 1.0, 0.0).astype(BF16) - strict * masks_ref[0]
        work.append([strict, inverse, scores, right, key_dec, query * grown, jnp.exp(last)])
    for level in range(1, masks_ref.shape[0]):
        inner = [dot(w[0] * masks_ref[level], w[1]).astype(BF16) for w in work]
        for w, part in zip(work, inner):
            w[1] = w[1] - dot(w[1], part).astype(BF16)
    for head in range(heads):
        _, inverse, scores, right, key_dec, query_dec, kept = work[head]
        solved = dot(inverse, right).astype(BF16)
        seen = dot(scores, solved)
        moved = dot_tn(key_dec, solved)
        current = map_ref[head]
        current_b = current.astype(BF16)
        asked = (query_dec - seen[:, 128:]).astype(BF16)
        answer = dot(asked, current_b)
        where_rows = pl.ds(pl.multiple_of(start, CHUNK), CHUNK)
        from_state_ref[head, where_rows, :] = answer[:, :128].astype(BF16)
        local_ref[head, where_rows, :] = answer[:, 128:] + seen[:, :128]
        added = jnp.concatenate([jnp.zeros((128, 128), F32), moved[:, :128]], axis=1)
        map_ref[head] = current * kept - dot(moved[:, 128:].astype(BF16), current_b) + added


def local_kernel(heads, chunks, raw_ref, taps_ref, beta_ref, decay_ref, from_state_ref, local_ref,
                 map_out_ref, grow_ref, gcol_ref, bcol_ref, masks_ref, map_ref):
    fill_masks(masks_ref)
    fill_gates(beta_ref[...], decay_ref[...], grow_ref, gcol_ref, bcol_ref)
    rows = lax.broadcasted_iota(jnp.int32, (128, 256), 0)
    cols = lax.broadcasted_iota(jnp.int32, (128, 256), 1)
    for head in range(heads):
        map_ref[head] = jnp.where(rows == cols, 1.0, 0.0)

    @pl.loop(0, chunks)
    def _(chunk):
        delta_chunk(chunk, heads, chunks, raw_ref, taps_ref, grow_ref, gcol_ref, bcol_ref,
                    masks_ref, map_ref, from_state_ref, local_ref)

    map_out_ref[...] = map_ref[...].astype(BF16)


def local_maps(raw, taps, beta, decay, heads):
    tok_rows = raw.shape[0] - HALO
    chunks = tok_rows // CHUNK
    vmem = pl.BlockSpec(memory_space=pltpu.VMEM)
    return pl.pallas_call(
        lambda *refs: local_kernel(heads, chunks, *refs),
        out_shape=(
            jax.ShapeDtypeStruct((heads, tok_rows, 128), BF16),
            jax.ShapeDtypeStruct((heads, tok_rows, 128), F32),
            jax.ShapeDtypeStruct((heads, 128, 256), BF16),
        ),
        in_specs=[vmem] * 4,
        out_specs=(vmem, vmem, vmem),
        scratch_shapes=[
            pltpu.VMEM((heads * chunks, 8, CHUNK), F32),
            pltpu.VMEM((heads * chunks, CHUNK, 128), F32),
            pltpu.VMEM((heads * chunks, CHUNK, 128), F32),
            pltpu.VMEM((8, CHUNK, CHUNK), BF16),
            pltpu.VMEM((heads, 128, 256), F32),
        ],
        compiler_params=pltpu.CompilerParams(vmem_limit_bytes=VMEM_LIMIT),
        name="local_maps",
    )(raw, taps, beta, decay)


def after(later, earlier):
    offset = jnp.concatenate([jnp.zeros((128, 128), F32), later[:, 128:].astype(F32)], axis=1)
    return dot(later[:, :128], earlier.astype(BF16)) + offset


def prefix_kernel(heads, n_z, n_x, own_ref, state_ref, row_ref, total_ref, column_ref, send_x,
                  recv_x, send_z, recv_z):
    z, x = lax.axis_index("sp_0"), lax.axis_index("sp_1")
    barrier = pltpu.get_barrier_semaphore()
    for step in range(1, n_x):
        to = lax.rem(x + step, n_x)
        pl.semaphore_signal(barrier, 1, device_id={"sp_1": to}, device_id_type=MESH_ID)
    for step in range(1, n_z):
        to = lax.rem(z + step, n_z)
        pl.semaphore_signal(barrier, 1, device_id={"sp_0": to}, device_id_type=MESH_ID)
    pl.semaphore_wait(barrier, n_x + n_z - 2)

    copies = []
    for step in range(1, n_x):
        copy = pltpu.make_async_remote_copy(
            src_ref=own_ref, dst_ref=row_ref.at[step], send_sem=send_x.at[step],
            recv_sem=recv_x.at[step], device_id={"sp_1": lax.rem(x + step, n_x)},
            device_id_type=MESH_ID)
        copy.start()
        copies.append(copy)
    row_ref[0] = own_ref[...]
    for copy in copies:
        copy.wait()
    inside, total = [None] * heads, [None] * heads
    rows = lax.broadcasted_iota(jnp.int32, (128, 256), 0)
    cols = lax.broadcasted_iota(jnp.int32, (128, 256), 1)
    identity = jnp.where(rows == cols, 1.0, 0.0)
    for head in range(heads):
        so_far = identity
        before = identity
        for k in range(n_x):
            piece = row_ref[lax.rem(x - k + n_x, n_x), head]
            so_far = piece.astype(F32) if k == 0 else after(piece, so_far)
            before = jnp.where(k < x, so_far, before)
        inside[head] = before
        total_ref[head] = so_far.astype(BF16)
    copies = []
    for step in range(1, n_z):
        copy = pltpu.make_async_remote_copy(
            src_ref=total_ref, dst_ref=column_ref.at[step], send_sem=send_z.at[step],
            recv_sem=recv_z.at[step], device_id={"sp_0": lax.rem(z + step, n_z)},
            device_id_type=MESH_ID)
        copy.start()
        copies.append(copy)
    column_ref[0] = total_ref[...]
    for copy in copies:
        copy.wait()
    for head in range(heads):
        so_far = jnp.zeros((128, 128), F32)
        state = so_far
        for k in range(n_z - 1):
            piece = column_ref[lax.rem(z - k + n_z, n_z), head]
            offset = piece[:, 128:].astype(F32)
            so_far = offset if k == 0 else dot(piece[:, :128], so_far.astype(BF16)) + offset
            state = jnp.where(k < z, so_far, state)
        entering = dot(inside[head][:, :128].astype(BF16), state.astype(BF16))
        state_ref[head] = (entering + inside[head][:, 128:]).astype(BF16)


def incoming_state(own, n_z, n_x):
    heads = own.shape[0]
    vmem = pl.BlockSpec(memory_space=pltpu.VMEM)
    return pl.pallas_call(
        lambda *refs: prefix_kernel(heads, n_z, n_x, *refs),
        out_shape=jax.ShapeDtypeStruct((heads, 128, 128), BF16),
        in_specs=[vmem],
        out_specs=vmem,
        scratch_shapes=[
            pltpu.VMEM((n_x, heads, 128, 256), BF16),
            pltpu.VMEM((heads, 128, 256), BF16),
            pltpu.VMEM((n_z, heads, 128, 256), BF16),
            pltpu.SemaphoreType.DMA((n_x,)),
            pltpu.SemaphoreType.DMA((n_x,)),
            pltpu.SemaphoreType.DMA((n_z,)),
            pltpu.SemaphoreType.DMA((n_z,)),
        ],
        compiler_params=pltpu.CompilerParams(collective_id=0, has_side_effects=True),
        name="incoming_state",
    )(own)


def pooled_rows(pool_ref, position, wide, mix_ref, scale_ref, out_ref, start):
    for group in range(2):
        lanes = slice(group * 128, group * 128 + 128)
        rows = pool_ref[pl.ds(pl.multiple_of(start, 8), CHUNK + HALO), lanes]
        reach = 1
        sums = rows
        for _ in range(group + 1):
            sums = sums + pltpu.roll(sums, reach, 0)
            reach *= 2
        broad = sums
        for _ in range(2):
            broad = broad + pltpu.roll(broad, reach, 0)
            reach *= 2
        short, long = 2 << group, 8 << group
        seen = lax.broadcasted_iota(jnp.int32, (CHUNK, 128), 0) + (position + 1)
        count = jnp.minimum(seen, jnp.where(wide, long, short)).astype(F32)
        window = jnp.where(wide, broad[HALO:], sums[HALO:])
        diff = (window / count - rows[HALO:]).astype(BF16)
        mixed = dot(diff, mix_ref[group]) * scale_ref[0:1, lanes]
        out_ref[pl.ds(pl.multiple_of(start, CHUNK), CHUNK), lanes] = mixed.astype(BF16)


def finish_kernel(heads, chunks, from_state_ref, local_ref, state_ref, gain_ref, pool_ref, mix_ref,
                  scale_ref, out_ref):
    tok_rows = chunks * CHUNK
    token = (lax.axis_index("sp_0") * lax.axis_size("sp_1") + lax.axis_index("sp_1")) * tok_rows
    wide = lax.rem(lax.axis_index("tp"), 2) == 1

    @pl.loop(0, chunks)
    def _(chunk):
        start = chunk * CHUNK
        where_rows = pl.ds(pl.multiple_of(start, CHUNK), CHUNK)
        pooled_rows(pool_ref, token + start, wide, mix_ref, scale_ref, out_ref, start)
        for head in range(heads):
            raw = dot(from_state_ref[head, where_rows, :], state_ref[head])
            raw = raw + local_ref[head, where_rows, :]
            squares = jnp.mean(raw * raw, axis=-1, keepdims=True)
            normed = raw * lax.rsqrt(squares + EPSILON) * gain_ref[...]
            out_ref[where_rows, 256 + head * 128 : 384 + head * 128] = normed.astype(BF16)


def finish(from_state, local, state, gain, pool_raw, mix, scale):
    heads, tok_rows, _ = from_state.shape
    vmem = pl.BlockSpec(memory_space=pltpu.VMEM)
    return pl.pallas_call(
        lambda *refs: finish_kernel(heads, tok_rows // CHUNK, *refs),
        out_shape=jax.ShapeDtypeStruct((tok_rows, 512), BF16),
        in_specs=[vmem] * 7,
        out_specs=vmem,
        compiler_params=pltpu.CompilerParams(vmem_limit_bytes=VMEM_LIMIT),
        name="finish",
    )(from_state, local, state, gain, pool_raw, mix, scale)


def side_by_side(arrays, axis, dim, along):
    widths = [a.shape[along] for a in arrays]
    both = jnp.concatenate(arrays, axis=along)
    result = lax.all_gather(both, axis, axis=dim, tiled=True)
    return tuple(jnp.split(result, [sum(widths[:k]) for k in range(1, len(widths))], axis=along))


def shifted(block, axis, distance):
    devices = range(lax.axis_size(axis))
    route = [(i - distance, i) for i in devices if i - distance in devices]
    return lax.ppermute(block, axis, route)


def scale_rows(values, gain_vec):
    squares = jnp.mean(values * values, axis=-1, keepdims=True)
    return values * lax.rsqrt(squares + EPSILON) * gain_vec.astype(F32)


def per_device(tokens, input_norm_scale, mean_input_weight, query_matrix, key_matrix, value_matrix,
               strength_weight, decay_input_weight, causal_filter_weight, head_decay_logrates,
               decay_input_shift, strength_shift, decay_spike, head_norm_scale,
               group_mixing_weight, mean_channel_scale, mean_output_weight, delta_output_weight):
    tok_rows = tokens.shape[0]
    pool_cols = mean_input_weight.shape[1]
    delta_cols = query_matrix.shape[1]
    heads = strength_weight.shape[1]
    groups = pool_cols // GROUP_DIM
    chunks = tok_rows // CHUNK
    tp = lax.axis_index("tp")
    normed = scale_rows(tokens.astype(F32), input_norm_scale).astype(BF16)
    pieces = side_by_side(
        (mean_input_weight, query_matrix, key_matrix, value_matrix, strength_weight,
         decay_input_weight), SP, 0, 1)
    wide = jnp.dot(normed, jnp.concatenate(pieces[:4], axis=1), preferred_element_type=F32)
    narrow = jnp.dot(normed, jnp.concatenate(pieces[4:], axis=1), preferred_element_type=F32)
    before = shifted(wide[tok_rows - HALO :].astype(BF16), SP, 1)
    extended = jnp.concatenate([before.astype(F32), wide], axis=0)
    taps = lax.dynamic_slice_in_dim(causal_filter_weight, tp * delta_cols, delta_cols, 2)
    taps = taps.reshape(CONV, 3 * delta_cols).astype(F32)

    def own(vector):
        return lax.dynamic_slice_in_dim(vector, tp * heads, heads)

    beta = jax.nn.sigmoid(narrow[:, :heads] + own(strength_shift))
    decay = (-jnp.exp(own(head_decay_logrates))
             * jax.nn.softplus(narrow[:, heads:] + own(decay_input_shift)) + decay_spike)
    from_state, local, own_map = local_maps(
        extended[:, pool_cols:], taps, beta.T.reshape(heads * chunks, CHUNK),
        decay.T.reshape(heads * chunks, CHUNK), heads)
    state = incoming_state(own_map, lax.axis_size("sp_0"), lax.axis_size("sp_1"))
    mix = lax.dynamic_slice_in_dim(group_mixing_weight, tp * groups, groups, 0)
    scale = lax.dynamic_slice_in_dim(mean_channel_scale, tp * pool_cols, pool_cols)
    mixed = finish(from_state, local, state, head_norm_scale.astype(F32).reshape(1, HEAD_DIM),
                   extended[:, :pool_cols], mix, scale.astype(F32).reshape(1, pool_cols))
    out_weight = jnp.concatenate(
        side_by_side((mean_output_weight, delta_output_weight), SP, 1, 0), axis=0)
    return lax.psum_scatter(
        jnp.dot(mixed, out_weight, preferred_element_type=F32).astype(BF16),
        "tp", scatter_dimension=0, tiled=True)


def solution(mesh):
    finer = Mesh(mesh.devices.reshape(4, 4, mesh.shape["tp"]), SP_TP)
    in_specs = (
        P(SP, None), P(), P(SP, "tp"), P(SP, "tp"), P(SP, "tp"), P(SP, "tp"), P(SP, "tp"),
        P(SP, "tp"), P(), P(), P(), P(), P(SP, "tp"), P(), P(), P(), P("tp", SP), P("tp", SP),
    )
    return jax.shard_map(
        per_device, mesh=finer, in_specs=in_specs, out_specs=P(SP_TP, None), check_vma=False
    )
```

```python
import jax
import jax.numpy as jnp
from jax import lax
from jax.experimental import pallas as pl
from jax.experimental.pallas import tpu as pltpu
from jax.sharding import Mesh
from jax.sharding import PartitionSpec as P

GROUP_DIM = 128
HEAD_DIM = 128
CONV = 4
CHUNK = 256
HALO = 16
EPSILON = 1e-06
SP = ("sp_0", "sp_1")
SP_TP = ("sp_0", "sp_1", "tp")
MESH_ID = pl.DeviceIdType.MESH
F32 = jnp.float32
BF16 = jnp.bfloat16
VMEM_LIMIT = 60 * 1024 * 1024


def dot(a, b):
    return jnp.dot(a, b, preferred_element_type=F32)


def dot_nt(a, b):
    return lax.dot_general(a, b, (((1,), (1,)), ((), ())), preferred_element_type=F32)


def dot_tn(a, b):
    return lax.dot_general(a, b, (((0,), (0,)), ((), ())), preferred_element_type=F32)


def unit_rows(values):
    return values * lax.rsqrt(jnp.sum(values * values, axis=-1, keepdims=True) + EPSILON)


def fill_masks(masks_ref):
    rows = lax.broadcasted_iota(jnp.int32, (CHUNK, CHUNK), 0)
    cols = lax.broadcasted_iota(jnp.int32, (CHUNK, CHUNK), 1)
    apart = jnp.bitwise_xor(rows, cols)
    for level in range(masks_ref.shape[0]):
        inside = (rows > cols) & (apart >= 2**level) & (apart < 2 ** (level + 1))
        masks_ref[level] = jnp.where(inside, 1.0, 0.0).astype(BF16)


def conv_rows(raw_ref, taps_ref, start, part):
    lanes = slice(part * 128, part * 128 + 128)
    rows = raw_ref[pl.ds(pl.multiple_of(start + HALO - 8, 8), CHUNK + 8), lanes]
    mixed = taps_ref[CONV - 1 : CONV, lanes] * rows[8:]
    for back in range(1, CONV):
        tap = taps_ref[CONV - 1 - back : CONV - back, lanes]
        mixed = mixed + tap * pltpu.roll(rows, back, 0)[8:]
    return mixed / (1.0 + jnp.exp(-mixed))


def delta_chunk(chunk, heads, chunks, raw_ref, taps_ref, grow_ref, gcol_ref, bcol_ref, masks_ref,
                map_ref, from_state_ref, local_ref):
    start = chunk * CHUNK
    rows = lax.broadcasted_iota(jnp.int32, (CHUNK, CHUNK), 0)
    cols = lax.broadcasted_iota(jnp.int32, (CHUNK, CHUNK), 1)
    work = []
    for head in range(heads):
        row = head * chunks + chunk
        query = unit_rows(conv_rows(raw_ref, taps_ref, start, head)) * HEAD_DIM ** (-0.5)
        key = unit_rows(conv_rows(raw_ref, taps_ref, start, heads + head))
        value = conv_rows(raw_ref, taps_ref, start, 2 * heads + head)
        gcol, bcol, grow = gcol_ref[row], bcol_ref[row], grow_ref[row][0:1]
        key_b = key.astype(BF16)
        both = jnp.concatenate([query.astype(BF16), key_b], axis=0)
        inner = dot_nt(both, key_b)
        spread = jnp.exp(jnp.minimum(jnp.concatenate([gcol, gcol], axis=1) - grow, 0.0))
        scores = jnp.where(rows >= cols, inner[:CHUNK] * spread, 0.0).astype(BF16)
        strict = jnp.where(rows > cols, inner[CHUNK:] * spread, 0.0)
        strict = (strict * jnp.concatenate([bcol, bcol], axis=1)).astype(BF16)
        grown = jnp.exp(gcol)
        right = jnp.concatenate([value * bcol, key * bcol * grown], axis=1).astype(BF16)
        last = grow[:, CHUNK - 1 : CHUNK]
        key_dec = (key * jnp.exp(last - gcol)).astype(BF16)
        inverse = jnp.where(rows == cols, 1.0, 0.0).astype(BF16) - strict * masks_ref[0]
        work.append([strict, inverse, scores, right, key_dec, query * grown, jnp.exp(last)])
    for level in range(1, masks_ref.shape[0]):
        inner = [dot(w[0] * masks_ref[level], w[1]).astype(BF16) for w in work]
        for w, part in zip(work, inner):
            w[1] = w[1] - dot(w[1], part).astype(BF16)
    for head in range(heads):
        _, inverse, scores, right, key_dec, query_dec, kept = work[head]
        solved = dot(inverse, right).astype(BF16)
        seen = dot(scores, solved)
        moved = dot_tn(key_dec, solved)
        current = map_ref[head]
        current_b = current.astype(BF16)
        asked = (query_dec - seen[:, 128:]).astype(BF16)
        answer = dot(asked, current_b)
        where_rows = pl.ds(pl.multiple_of(start, CHUNK), CHUNK)
        from_state_ref[head, where_rows, :] = answer[:, :128].astype(BF16)
        local_ref[head, where_rows, :] = answer[:, 128:] + seen[:, :128]
        added = jnp.concatenate([jnp.zeros((128, 128), F32), moved[:, :128]], axis=1)
        map_ref[head] = current * kept - dot(moved[:, 128:].astype(BF16), current_b) + added


ROWS_A = (272, 768)
SPLIT_A = 128
ROWS_B = (768, 256)
SPLIT_B = 384
ORDER = ((0, 1), (0, -1), (1, 0), (-1, 0), (1, 1), (1, -1), (-1, 1), (-1, -1), (0, 2), (2, 0),
         (1, 2), (-1, 2), (2, 1), (2, -1), (2, 2))


class PlaneGather:
    def __init__(self, buf, split, send_sems, recv_sems):
        self.buf, self.split = buf, split
        self.send_sems, self.recv_sems = send_sems, recv_sems
        self.z, self.x = lax.axis_index("sp_0"), lax.axis_index("sp_1")
        self.copies = {}

    def shard(self, dz, dx):
        return lax.rem(self.z + dz + 4, 4) * 4 + lax.rem(self.x + dx + 4, 4)

    def rows(self, part):
        split, total = self.split, self.buf.shape[1]
        quarter = split // 32 * 16
        rest = split + (total - split) // 32 * 16
        return {"a": (0, split), "b": (split, total), "a0": (0, quarter), "a1": (quarter, split),
                "b0": (split, rest), "b1": (rest, total)}[part]

    def region(self, dz, dx, part):
        low, high = self.rows(part)
        return self.buf.at[self.shard(dz, dx), pl.ds(low, high - low), :]

    def send(self, name, source, part, way):
        index = len(self.copies)
        ref = self.region(source[0], source[1], part)
        copy = pltpu.make_async_remote_copy(
            src_ref=ref, dst_ref=ref, send_sem=self.send_sems.at[index],
            recv_sem=self.recv_sems.at[index],
            device_id={"sp_0": lax.rem(self.z + way[0] + 4, 4),
                       "sp_1": lax.rem(self.x + way[1] + 4, 4)},
            device_id_type=MESH_ID)
        copy.start()
        self.copies[name, way] = (copy, index, source, part)

    def got(self, name, way):
        _, index, source, part = self.copies[name, way]
        ref = self.region(source[0] - way[0], source[1] - way[1], part)
        pltpu.make_async_remote_copy(
            src_ref=ref, dst_ref=ref, send_sem=self.send_sems.at[index],
            recv_sem=self.recv_sems.at[index],
            device_id={"sp_0": lax.rem(self.z + way[0] + 4, 4),
                       "sp_1": lax.rem(self.x + way[1] + 4, 4)},
            device_id_type=MESH_ID).wait_recv()

    def own(self):
        for step in (1, -1):
            self.send("a", (0, 0), "a", (0, step))
            self.send("b", (0, 0), "b", (step, 0))
        for step in (1, -1):
            self.send("b", (0, 0), "b", (0, step))
            self.send("a", (0, 0), "a", (step, 0))

    def first(self):
        for step in (1, -1):
            self.got("a", (0, step))
            self.got("b", (step, 0))
        self.send("a2", (0, -1), "a0", (0, 1))
        self.send("a2", (0, 1), "a1", (0, -1))
        self.send("b2", (-1, 0), "b0", (1, 0))
        self.send("b2", (1, 0), "b1", (-1, 0))
        for at in (1, -1):
            for step in (1, -1):
                self.send(("a3", at), (0, at), "a", (step, 0))
                self.send(("b3", at), (at, 0), "b", (0, step))

    def second(self):
        for step in (1, -1):
            self.got("b", (0, step))
            self.got("a", (step, 0))
        self.send(("a4", 0), (-1, 0), "a", (1, 0))
        self.send(("b4", 0), (0, -1), "b", (0, 1))

    def third(self):
        for step in (1, -1):
            self.got("a2", (0, step))
            self.got("b2", (step, 0))
        for step in (-1, 1):
            self.send(("a3", 2), (0, 2), "a", (step, 0))
            self.send(("b3", 2), (2, 0), "b", (0, step))

    def fourth(self):
        for at in (1, -1):
            for step in (1, -1):
                self.got(("a3", at), (step, 0))
                self.got(("b3", at), (0, step))
        for at in (1, -1):
            self.send(("a4", at), (-at, at), "a", (at, 0))
            self.send(("b4", at), (at, -at), "b", (0, at))

    def fifth(self):
        for step in (1, -1):
            self.got(("a3", 2), (step, 0))
            self.got(("b3", 2), (0, step))
        self.send(("a4", 2), (1, 2), "a", (-1, 0))
        self.send(("b4", 2), (2, 1), "b", (0, -1))

    def last(self, dz, dx):
        side = {0: 1, 1: 1, -1: -1, 2: -1}
        if dz == 2:
            self.got(("a4", dx), (side[dx], 0))
        if dx == 2:
            self.got(("b4", dz), (0, side[dz]))

    def drain(self):
        for copy, _, _, _ in self.copies.values():
            copy.wait_send()


def norm_rows(tok_ref, gain_ref, start, count):
    @pl.loop(0, count // 16)
    def _(step):
        rows = pl.ds(pl.multiple_of(start + step * 16, 16), 16)
        values = tok_ref[rows, :].astype(F32)
        squares = jnp.mean(values * values, axis=-1, keepdims=True)
        tok_ref[rows, :] = (values * lax.rsqrt(squares + EPSILON) * gain_ref[...]).astype(BF16)


def front_kernel(heads, tok_hbm, pool_hbm, query_hbm, key_hbm, value_hbm, pool_out_hbm,
                 delta_out_hbm, gain_ref, strength_ref, decay_ref, taps_ref, spike_ref, rate_ref,
                 decay_shift_ref, strength_shift_ref,
                 from_state_ref, local_ref, map_out_ref, pool_acc_ref, out_w_hbm,
                 tok_ref, wide_ref, late_ref, acc_ref, thin_ref, grow_ref, gcol_ref, bcol_ref,
                 masks_ref, map_ref, tok_sems, load_sems, halo_send, halo_recv,
                 send_a, recv_a, send_b, recv_b, out_sem):
    z, x, tp = lax.axis_index("sp_0"), lax.axis_index("sp_1"), lax.axis_index("tp")
    tok_rows = tok_hbm.shape[0]
    chunks = tok_rows // CHUNK
    mine = z * 4 + x
    loads = []
    for k, (hbm, ref, rows, lanes) in enumerate((
            (query_hbm, wide_ref, 0, 0), (key_hbm, wide_ref, 0, 256), (value_hbm, wide_ref, 0, 512),
            (pool_hbm, late_ref, 0, 0), (pool_out_hbm, late_ref, 256, 0),
            (delta_out_hbm, late_ref, 512, 0))):
        load = pltpu.make_async_copy(
            hbm, ref.at[mine, pl.ds(rows, 256), pl.ds(lanes, 256)], load_sems.at[k])
        load.start()
        loads.append(load)
    tok_loads = []
    for k in range(chunks):
        load = pltpu.make_async_copy(
            tok_hbm.at[pl.ds(k * CHUNK, CHUNK), :],
            tok_ref.at[pl.ds(HALO + k * CHUNK, CHUNK), :], tok_sems.at[k])
        load.start()
        tok_loads.append(load)
    at = lax.broadcasted_iota(jnp.int32, (16, 256), 0)
    thin = jnp.zeros((16, 256), F32)
    for k, (ref, row) in enumerate(((strength_ref, 0), (strength_ref, 1), (decay_ref, 0),
                                    (decay_ref, 1))):
        row_values = ref[...].astype(F32)[row : row + 1]
        thin = jnp.where(at == k, jnp.broadcast_to(row_values, (16, 256)), thin)
    wide_ref[mine, 256:272, 0:256] = thin.astype(BF16)
    wide_ref[mine, 256:272, 256:768] = jnp.zeros((16, 512), BF16)

    following = lax.rem(mine + 1, 16)
    before = lax.rem(mine + 15, 16)
    barrier = pltpu.get_barrier_semaphore()
    for dz, dx in ((0, 1), (0, -1), (1, 0), (-1, 0)):
        pl.semaphore_signal(
            barrier, 1, device_id={"sp_0": lax.rem(z + dz + 4, 4), "sp_1": lax.rem(x + dx + 4, 4)},
            device_id_type=MESH_ID)
    for other in (following, before):
        pl.semaphore_signal(
            barrier, 1, device_id={"sp_0": other // 4, "sp_1": lax.rem(other, 4)},
            device_id_type=MESH_ID)
    fill_masks(masks_ref)
    for load in loads:
        load.wait()
    pl.semaphore_wait(barrier, 6)

    early = PlaneGather(wide_ref, SPLIT_A, send_a, recv_a)
    early.own()
    halo = pltpu.make_async_remote_copy(
        src_ref=tok_hbm.at[pl.ds(tok_rows - HALO, HALO), :], dst_ref=tok_ref.at[pl.ds(0, HALO), :],
        send_sem=halo_send, recv_sem=halo_recv,
        device_id={"sp_0": following // 4, "sp_1": lax.rem(following, 4)}, device_id_type=MESH_ID)
    halo.start()
    for k in range(chunks):
        tok_loads[k].wait()
        norm_rows(tok_ref, gain_ref, HALO + k * CHUNK, CHUNK)
    halo.wait()

    @pl.when(mine == 0)
    def _():
        tok_ref[0:HALO, :] = jnp.zeros((HALO, tok_ref.shape[1]), BF16)

    norm_rows(tok_ref, gain_ref, 0, HALO)

    tile = 208

    def project(gather, dz, dx, into, first=False):
        shard = gather.shard(dz, dx)
        lanes = pl.ds(pl.multiple_of(shard * 256, 256), 256)

        @pl.loop(0, acc_ref.shape[0] // tile)
        def _(step):
            rows = pl.ds(pl.multiple_of(step * tile, 16), tile)
            normed = tok_ref[rows, lanes]
            product = dot(normed, gather.buf[shard, 0:256, :])
            into[rows, :] = product if first else into[rows, :] + product
            if gather is early:
                narrow = dot_nt(normed, gather.buf[shard, 256:272, 0:256])
                thin_ref[rows, :] = narrow if first else thin_ref[rows, :] + narrow

    project(early, 0, 0, acc_ref, first=True)
    early.first()
    early.second()
    for dz, dx in ORDER[:4]:
        project(early, dz, dx, acc_ref)
    early.third()
    early.fourth()
    for dz, dx in ORDER[4:8]:
        project(early, dz, dx, acc_ref)
    early.fifth()
    late = PlaneGather(late_ref, SPLIT_B, send_b, recv_b)
    late.own()
    for dz, dx in ORDER[8:]:
        early.last(dz, dx)
        project(early, dz, dx, acc_ref)

    narrow = thin_ref[HALO:, :].T
    total = tok_rows
    heads_at = lax.broadcasted_iota(jnp.int32, (16, total), 0)

    def own_scalar(ref, head):
        return ref[tp * heads + head]

    for head in range(heads):
        strength = narrow[head : head + 1] + own_scalar(strength_shift_ref, head)
        beta = 1.0 / (1.0 + jnp.exp(-strength))
        level = narrow[heads + head : heads + head + 1] + own_scalar(decay_shift_ref, head)
        soft = jnp.maximum(level, 0.0) + jnp.log1p(jnp.exp(-jnp.abs(level)))
        rate = jnp.exp(jnp.full((1, total), own_scalar(rate_ref, head), F32))
        decay = spike_ref[head : head + 1, :] - rate * soft
        lane = lax.rem(lax.broadcasted_iota(jnp.int32, (8, total), 1), CHUNK)
        summed = jnp.broadcast_to(decay, (8, total))
        step = 1
        while step < CHUNK:
            summed = summed + jnp.where(lane >= step, pltpu.roll(summed, step, 1), 0.0)
            step *= 2
        for chunk in range(chunks):
            row = head * chunks + chunk
            part = slice(chunk * CHUNK, chunk * CHUNK + CHUNK)
            grow_ref[row] = summed[:, part]
            gcol_ref[row] = jnp.broadcast_to(summed[0:1, part], (128, CHUNK)).T
            bcol_ref[row] = jnp.broadcast_to(beta[:, part], (128, CHUNK)).T
    rows = lax.broadcasted_iota(jnp.int32, (128, 256), 0)
    cols = lax.broadcasted_iota(jnp.int32, (128, 256), 1)
    for head in range(heads):
        map_ref[head] = jnp.where(rows == cols, 1.0, 0.0)

    def delta(low, high):
        @pl.loop(low, high)
        def _(chunk):
            delta_chunk(chunk, heads, chunks, acc_ref, taps_ref, grow_ref, gcol_ref, bcol_ref,
                        masks_ref, map_ref, from_state_ref, local_ref)

    late.first()
    late.second()
    delta(0, chunks // 2)
    late.third()
    late.fourth()
    delta(chunks // 2, chunks)
    map_out_ref[...] = map_ref[...].astype(BF16)
    late.fifth()
    project(late, 0, 0, pool_acc_ref, first=True)
    for dz, dx in ORDER[:8]:
        project(late, dz, dx, pool_acc_ref)
    for dz, dx in ORDER[8:]:
        late.last(dz, dx)
        project(late, dz, dx, pool_acc_ref)
    result = pltpu.make_async_copy(late_ref.at[:, pl.ds(256, 512), :], out_w_hbm, out_sem)
    result.start()
    early.drain()
    late.drain()
    result.wait()


def front(tokens, weights, out_weights, gain, strength, decay, taps, spike, rate, decay_shift,
          strength_shift, heads):
    tok_rows, depth = tokens.shape
    chunks = tok_rows // CHUNK
    vmem = pl.BlockSpec(memory_space=pltpu.VMEM)
    smem = pl.BlockSpec(memory_space=pltpu.SMEM)
    hbm = pl.BlockSpec(memory_space=pl.ANY)
    pairs = heads * chunks
    dma = pltpu.SemaphoreType.DMA
    return pl.pallas_call(
        lambda *refs: front_kernel(heads, *refs),
        out_shape=(
            jax.ShapeDtypeStruct((heads, tok_rows, 128), BF16),
            jax.ShapeDtypeStruct((heads, tok_rows, 128), F32),
            jax.ShapeDtypeStruct((heads, 128, 256), BF16),
            jax.ShapeDtypeStruct((tok_rows + HALO, 256), F32),
            jax.ShapeDtypeStruct((16, 512, 256), BF16),
        ),
        in_specs=[hbm] * 7 + [vmem] * 5 + [smem] * 3,
        out_specs=(vmem, vmem, vmem, vmem, hbm),
        scratch_shapes=[
            pltpu.VMEM((tok_rows + HALO, depth), BF16),
            pltpu.VMEM((16,) + ROWS_A, BF16),
            pltpu.VMEM((16,) + ROWS_B, BF16),
            pltpu.VMEM((tok_rows + HALO, 768), F32),
            pltpu.VMEM((tok_rows + HALO, 16), F32),
            pltpu.VMEM((pairs, 8, CHUNK), F32),
            pltpu.VMEM((pairs, CHUNK, 128), F32),
            pltpu.VMEM((pairs, CHUNK, 128), F32),
            pltpu.VMEM((8, CHUNK, CHUNK), BF16),
            pltpu.VMEM((heads, 128, 256), F32),
            dma((chunks,)), dma((6,)), dma(()), dma(()),
            dma((32,)), dma((32,)), dma((32,)), dma((32,)), dma(()),
        ],
        compiler_params=pltpu.CompilerParams(
            vmem_limit_bytes=VMEM_LIMIT, collective_id=1, has_side_effects=True),
        name="front",
    )(tokens, *weights, *out_weights, gain, strength, decay, taps, spike, rate, decay_shift,
      strength_shift)


def after(later, earlier):
    offset = jnp.concatenate([jnp.zeros((128, 128), F32), later[:, 128:].astype(F32)], axis=1)
    return dot(later[:, :128], earlier.astype(BF16)) + offset


def prefix_kernel(heads, n_z, n_x, own_ref, state_ref, row_ref, total_ref, column_ref, send_x,
                  recv_x, send_z, recv_z):
    z, x = lax.axis_index("sp_0"), lax.axis_index("sp_1")
    barrier = pltpu.get_barrier_semaphore()
    for step in range(1, n_x):
        to = lax.rem(x + step, n_x)
        pl.semaphore_signal(barrier, 1, device_id={"sp_1": to}, device_id_type=MESH_ID)
    for step in range(1, n_z):
        to = lax.rem(z + step, n_z)
        pl.semaphore_signal(barrier, 1, device_id={"sp_0": to}, device_id_type=MESH_ID)
    pl.semaphore_wait(barrier, n_x + n_z - 2)

    copies = []
    for step in range(1, n_x):
        copy = pltpu.make_async_remote_copy(
            src_ref=own_ref, dst_ref=row_ref.at[step], send_sem=send_x.at[step],
            recv_sem=recv_x.at[step], device_id={"sp_1": lax.rem(x + step, n_x)},
            device_id_type=MESH_ID)
        copy.start()
        copies.append(copy)
    row_ref[0] = own_ref[...]
    for copy in copies:
        copy.wait()
    inside, total = [None] * heads, [None] * heads
    rows = lax.broadcasted_iota(jnp.int32, (128, 256), 0)
    cols = lax.broadcasted_iota(jnp.int32, (128, 256), 1)
    identity = jnp.where(rows == cols, 1.0, 0.0)
    for head in range(heads):
        so_far = identity
        before = identity
        for k in range(n_x):
            piece = row_ref[lax.rem(x - k + n_x, n_x), head]
            so_far = piece.astype(F32) if k == 0 else after(piece, so_far)
            before = jnp.where(k < x, so_far, before)
        inside[head] = before
        total_ref[head] = so_far.astype(BF16)
    copies = []
    for step in range(1, n_z):
        copy = pltpu.make_async_remote_copy(
            src_ref=total_ref, dst_ref=column_ref.at[step], send_sem=send_z.at[step],
            recv_sem=recv_z.at[step], device_id={"sp_0": lax.rem(z + step, n_z)},
            device_id_type=MESH_ID)
        copy.start()
        copies.append(copy)
    column_ref[0] = total_ref[...]
    for copy in copies:
        copy.wait()
    for head in range(heads):
        so_far = jnp.zeros((128, 128), F32)
        state = so_far
        for k in range(n_z - 1):
            piece = column_ref[lax.rem(z - k + n_z, n_z), head]
            offset = piece[:, 128:].astype(F32)
            so_far = offset if k == 0 else dot(piece[:, :128], so_far.astype(BF16)) + offset
            state = jnp.where(k < z, so_far, state)
        entering = dot(inside[head][:, :128].astype(BF16), state.astype(BF16))
        state_ref[head] = (entering + inside[head][:, 128:]).astype(BF16)


def incoming_state(own, n_z, n_x):
    heads = own.shape[0]
    vmem = pl.BlockSpec(memory_space=pltpu.VMEM)
    return pl.pallas_call(
        lambda *refs: prefix_kernel(heads, n_z, n_x, *refs),
        out_shape=jax.ShapeDtypeStruct((heads, 128, 128), BF16),
        in_specs=[vmem],
        out_specs=vmem,
        scratch_shapes=[
            pltpu.VMEM((n_x, heads, 128, 256), BF16),
            pltpu.VMEM((heads, 128, 256), BF16),
            pltpu.VMEM((n_z, heads, 128, 256), BF16),
            pltpu.SemaphoreType.DMA((n_x,)),
            pltpu.SemaphoreType.DMA((n_x,)),
            pltpu.SemaphoreType.DMA((n_z,)),
            pltpu.SemaphoreType.DMA((n_z,)),
        ],
        compiler_params=pltpu.CompilerParams(collective_id=0, has_side_effects=True),
        name="incoming_state",
    )(own)


def pooled_rows(pool_ref, position, wide, mix_ref, scale_ref, out_ref, start):
    for group in range(2):
        lanes = slice(group * 128, group * 128 + 128)
        rows = pool_ref[pl.ds(pl.multiple_of(start, 8), CHUNK + HALO), lanes]
        reach = 1
        sums = rows
        for _ in range(group + 1):
            sums = sums + pltpu.roll(sums, reach, 0)
            reach *= 2
        broad = sums
        for _ in range(2):
            broad = broad + pltpu.roll(broad, reach, 0)
            reach *= 2
        short, long = 2 << group, 8 << group
        seen = lax.broadcasted_iota(jnp.int32, (CHUNK, 128), 0) + (position + 1)
        count = jnp.minimum(seen, jnp.where(wide, long, short)).astype(F32)
        window = jnp.where(wide, broad[HALO:], sums[HALO:])
        diff = (window / count - rows[HALO:]).astype(BF16)
        mixed = dot(diff, mix_ref[group]) * scale_ref[0:1, lanes]
        out_ref[pl.ds(pl.multiple_of(start, CHUNK), CHUNK), lanes] = mixed.astype(BF16)


def finish_kernel(heads, chunks, from_state_ref, local_ref, state_ref, gain_ref, pool_ref, mix_ref,
                  scale_ref, out_ref):
    tok_rows = chunks * CHUNK
    token = (lax.axis_index("sp_0") * lax.axis_size("sp_1") + lax.axis_index("sp_1")) * tok_rows
    wide = lax.rem(lax.axis_index("tp"), 2) == 1

    @pl.loop(0, chunks)
    def _(chunk):
        start = chunk * CHUNK
        where_rows = pl.ds(pl.multiple_of(start, CHUNK), CHUNK)
        pooled_rows(pool_ref, token + start, wide, mix_ref, scale_ref, out_ref, start)
        for head in range(heads):
            raw = dot(from_state_ref[head, where_rows, :], state_ref[head])
            raw = raw + local_ref[head, where_rows, :]
            squares = jnp.mean(raw * raw, axis=-1, keepdims=True)
            normed = raw * lax.rsqrt(squares + EPSILON) * gain_ref[...]
            out_ref[where_rows, 256 + head * 128 : 384 + head * 128] = normed.astype(BF16)


def finish(from_state, local, state, gain, pool_raw, mix, scale):
    heads, tok_rows, _ = from_state.shape
    vmem = pl.BlockSpec(memory_space=pltpu.VMEM)
    return pl.pallas_call(
        lambda *refs: finish_kernel(heads, tok_rows // CHUNK, *refs),
        out_shape=jax.ShapeDtypeStruct((tok_rows, 512), BF16),
        in_specs=[vmem] * 7,
        out_specs=vmem,
        compiler_params=pltpu.CompilerParams(vmem_limit_bytes=VMEM_LIMIT),
        name="finish",
    )(from_state, local, state, gain, pool_raw, mix, scale)


def per_device(tokens, input_norm_scale, mean_input_weight, query_matrix, key_matrix, value_matrix,
               strength_weight, decay_input_weight, causal_filter_weight, head_decay_logrates,
               decay_input_shift, strength_shift, decay_spike, head_norm_scale,
               group_mixing_weight, mean_channel_scale, mean_output_weight, delta_output_weight):
    pool_cols = mean_input_weight.shape[1]
    delta_cols = query_matrix.shape[1]
    heads = strength_weight.shape[1]
    groups = pool_cols // GROUP_DIM
    tp = lax.axis_index("tp")
    taps = lax.dynamic_slice_in_dim(causal_filter_weight, tp * delta_cols, delta_cols, 2)
    taps = taps.reshape(CONV, 3 * delta_cols).astype(F32)
    from_state, local, own_map, pool_raw, out_weight = front(
        tokens, (mean_input_weight, query_matrix, key_matrix, value_matrix),
        (mean_output_weight, delta_output_weight), input_norm_scale.astype(F32).reshape(1, -1),
        strength_weight.T, decay_input_weight.T, taps, decay_spike.T, head_decay_logrates,
        decay_input_shift, strength_shift, heads)
    state = incoming_state(own_map, lax.axis_size("sp_0"), lax.axis_size("sp_1"))
    mix = lax.dynamic_slice_in_dim(group_mixing_weight, tp * groups, groups, 0)
    scale = lax.dynamic_slice_in_dim(mean_channel_scale, tp * pool_cols, pool_cols)
    mixed = finish(from_state, local, state, head_norm_scale.astype(F32).reshape(1, HEAD_DIM),
                   pool_raw, mix, scale.astype(F32).reshape(1, pool_cols))
    out_weight = jnp.transpose(out_weight, (1, 0, 2)).reshape(512, -1)
    return lax.psum_scatter(
        jnp.dot(mixed, out_weight, preferred_element_type=F32).astype(BF16),
        "tp", scatter_dimension=0, tiled=True)


def solution(mesh):
    finer = Mesh(mesh.devices.reshape(4, 4, mesh.shape["tp"]), SP_TP)
    in_specs = (
        P(SP, None), P(), P(SP, "tp"), P(SP, "tp"), P(SP, "tp"), P(SP, "tp"), P(SP, "tp"),
        P(SP, "tp"), P(), P(), P(), P(), P(SP, "tp"), P(), P(), P(), P("tp", SP), P("tp", SP),
    )
    return jax.shard_map(
        per_device, mesh=finer, in_specs=in_specs, out_specs=P(SP_TP, None), check_vma=False
    )
```

```python
import jax
import jax.numpy as jnp
from jax import lax
from jax.experimental import pallas as pl
from jax.experimental.pallas import tpu as pltpu
from jax.sharding import Mesh
from jax.sharding import PartitionSpec as P

GROUP_DIM = 128
HEAD_DIM = 128
CONV = 4
CHUNK = 256
HALO = 16
EPSILON = 1e-06
SP = ("sp_0", "sp_1")
SP_TP = ("sp_0", "sp_1", "tp")
MESH_ID = pl.DeviceIdType.MESH
F32 = jnp.float32
BF16 = jnp.bfloat16
VMEM_LIMIT = 60 * 1024 * 1024


def dot(a, b):
    return jnp.dot(a, b, preferred_element_type=F32)


def dot_nt(a, b):
    return lax.dot_general(a, b, (((1,), (1,)), ((), ())), preferred_element_type=F32)


def dot_tn(a, b):
    return lax.dot_general(a, b, (((0,), (0,)), ((), ())), preferred_element_type=F32)


def unit_rows(values):
    return values * lax.rsqrt(jnp.sum(values * values, axis=-1, keepdims=True) + EPSILON)


def fill_masks(masks_ref):
    rows = lax.broadcasted_iota(jnp.int32, (CHUNK, CHUNK), 0)
    cols = lax.broadcasted_iota(jnp.int32, (CHUNK, CHUNK), 1)
    apart = jnp.bitwise_xor(rows, cols)
    for level in range(masks_ref.shape[0]):
        inside = (rows > cols) & (apart >= 2**level) & (apart < 2 ** (level + 1))
        masks_ref[level] = jnp.where(inside, 1.0, 0.0).astype(BF16)


def conv_rows(raw_ref, taps_ref, start, part):
    lanes = slice(part * 128, part * 128 + 128)
    rows = raw_ref[pl.ds(pl.multiple_of(start + HALO - 8, 8), CHUNK + 8), lanes]
    mixed = taps_ref[CONV - 1 : CONV, lanes] * rows[8:]
    for back in range(1, CONV):
        tap = taps_ref[CONV - 1 - back : CONV - back, lanes]
        mixed = mixed + tap * pltpu.roll(rows, back, 0)[8:]
    return mixed / (1.0 + jnp.exp(-mixed))


def delta_chunk(chunk, heads, chunks, raw_ref, taps_ref, grow_ref, gcol_ref, bcol_ref, masks_ref,
                map_ref, from_state_ref, local_ref):
    start = chunk * CHUNK
    rows = lax.broadcasted_iota(jnp.int32, (CHUNK, CHUNK), 0)
    cols = lax.broadcasted_iota(jnp.int32, (CHUNK, CHUNK), 1)
    work = []
    for head in range(heads):
        row = head * chunks + chunk
        query = unit_rows(conv_rows(raw_ref, taps_ref, start, head)) * HEAD_DIM ** (-0.5)
        key = unit_rows(conv_rows(raw_ref, taps_ref, start, heads + head))
        value = conv_rows(raw_ref, taps_ref, start, 2 * heads + head)
        gcol, bcol, grow = gcol_ref[row], bcol_ref[row], grow_ref[row][0:1]
        key_b = key.astype(BF16)
        both = jnp.concatenate([query.astype(BF16), key_b], axis=0)
        inner = dot_nt(both, key_b)
        spread = jnp.exp(jnp.minimum(jnp.concatenate([gcol, gcol], axis=1) - grow, 0.0))
        scores = jnp.where(rows >= cols, inner[:CHUNK] * spread, 0.0).astype(BF16)
        strict = jnp.where(rows > cols, inner[CHUNK:] * spread, 0.0)
        strict = (strict * jnp.concatenate([bcol, bcol], axis=1)).astype(BF16)
        grown = jnp.exp(gcol)
        right = jnp.concatenate([value * bcol, key * bcol * grown], axis=1).astype(BF16)
        last = grow[:, CHUNK - 1 : CHUNK]
        key_dec = (key * jnp.exp(last - gcol)).astype(BF16)
        inverse = jnp.where(rows == cols, 1.0, 0.0).astype(BF16) - strict * masks_ref[0]
        work.append([strict, inverse, scores, right, key_dec, query * grown, jnp.exp(last)])
    for level in range(1, masks_ref.shape[0]):
        inner = [dot(w[0] * masks_ref[level], w[1]).astype(BF16) for w in work]
        for w, part in zip(work, inner):
            w[1] = w[1] - dot(w[1], part).astype(BF16)
    for head in range(heads):
        _, inverse, scores, right, key_dec, query_dec, kept = work[head]
        solved = dot(inverse, right).astype(BF16)
        seen = dot(scores, solved)
        moved = dot_tn(key_dec, solved)
        current = map_ref[head]
        current_b = current.astype(BF16)
        asked = (query_dec - seen[:, 128:]).astype(BF16)
        answer = dot(asked, current_b)
        where_rows = pl.ds(pl.multiple_of(start, CHUNK), CHUNK)
        from_state_ref[head, where_rows, :] = answer[:, :128].astype(BF16)
        local_ref[head, where_rows, :] = answer[:, 128:] + seen[:, :128]
        added = jnp.concatenate([jnp.zeros((128, 128), F32), moved[:, :128]], axis=1)
        map_ref[head] = current * kept - dot(moved[:, 128:].astype(BF16), current_b) + added


ROWS_A = (272, 768)
SPLIT_A = 128
ROWS_B = (768, 256)
SPLIT_B = 384
ORDER = ((0, 1), (0, -1), (1, 0), (-1, 0), (1, 1), (1, -1), (-1, 1), (-1, -1), (0, 2), (2, 0),
         (1, 2), (-1, 2), (2, 1), (2, -1), (2, 2))


class PlaneGather:
    def __init__(self, buf, split, send_sems, recv_sems):
        self.buf, self.split = buf, split
        self.send_sems, self.recv_sems = send_sems, recv_sems
        self.z, self.x = lax.axis_index("sp_0"), lax.axis_index("sp_1")
        self.copies = {}

    def shard(self, dz, dx):
        return lax.rem(self.z + dz + 4, 4) * 4 + lax.rem(self.x + dx + 4, 4)

    def rows(self, part):
        split, total = self.split, self.buf.shape[1]
        quarter = split // 32 * 16
        rest = split + (total - split) // 32 * 16
        return {"a": (0, split), "b": (split, total), "a0": (0, quarter), "a1": (quarter, split),
                "b0": (split, rest), "b1": (rest, total)}[part]

    def region(self, dz, dx, part):
        low, high = self.rows(part)
        return self.buf.at[self.shard(dz, dx), pl.ds(low, high - low), :]

    def send(self, name, source, part, way):
        index = len(self.copies)
        ref = self.region(source[0], source[1], part)
        copy = pltpu.make_async_remote_copy(
            src_ref=ref, dst_ref=ref, send_sem=self.send_sems.at[index],
            recv_sem=self.recv_sems.at[index],
            device_id={"sp_0": lax.rem(self.z + way[0] + 4, 4),
                       "sp_1": lax.rem(self.x + way[1] + 4, 4)},
            device_id_type=MESH_ID)
        copy.start()
        self.copies[name, way] = (copy, index, source, part)

    def got(self, name, way):
        _, index, source, part = self.copies[name, way]
        ref = self.region(source[0] - way[0], source[1] - way[1], part)
        pltpu.make_async_remote_copy(
            src_ref=ref, dst_ref=ref, send_sem=self.send_sems.at[index],
            recv_sem=self.recv_sems.at[index],
            device_id={"sp_0": lax.rem(self.z + way[0] + 4, 4),
                       "sp_1": lax.rem(self.x + way[1] + 4, 4)},
            device_id_type=MESH_ID).wait_recv()

    def own(self):
        for step in (1, -1):
            self.send("a", (0, 0), "a", (0, step))
            self.send("b", (0, 0), "b", (step, 0))
        for step in (1, -1):
            self.send("b", (0, 0), "b", (0, step))
            self.send("a", (0, 0), "a", (step, 0))

    def first(self):
        for step in (1, -1):
            self.got("a", (0, step))
            self.got("b", (step, 0))
        self.send("a2", (0, -1), "a0", (0, 1))
        self.send("a2", (0, 1), "a1", (0, -1))
        self.send("b2", (-1, 0), "b0", (1, 0))
        self.send("b2", (1, 0), "b1", (-1, 0))
        for at in (1, -1):
            for step in (1, -1):
                self.send(("a3", at), (0, at), "a", (step, 0))
                self.send(("b3", at), (at, 0), "b", (0, step))

    def second(self):
        for step in (1, -1):
            self.got("b", (0, step))
            self.got("a", (step, 0))
        self.send(("a4", 0), (-1, 0), "a", (1, 0))
        self.send(("b4", 0), (0, -1), "b", (0, 1))

    def third(self):
        for step in (1, -1):
            self.got("a2", (0, step))
            self.got("b2", (step, 0))
        for step in (-1, 1):
            self.send(("a3", 2), (0, 2), "a", (step, 0))
            self.send(("b3", 2), (2, 0), "b", (0, step))

    def fourth(self):
        for at in (1, -1):
            for step in (1, -1):
                self.got(("a3", at), (step, 0))
                self.got(("b3", at), (0, step))
        for at in (1, -1):
            self.send(("a4", at), (-at, at), "a", (at, 0))
            self.send(("b4", at), (at, -at), "b", (0, at))

    def fifth(self):
        for step in (1, -1):
            self.got(("a3", 2), (step, 0))
            self.got(("b3", 2), (0, step))
        self.send(("a4", 2), (1, 2), "a", (-1, 0))
        self.send(("b4", 2), (2, 1), "b", (0, -1))

    def last(self, dz, dx):
        side = {0: 1, 1: 1, -1: -1, 2: -1}
        if dz == 2:
            self.got(("a4", dx), (side[dx], 0))
        if dx == 2:
            self.got(("b4", dz), (0, side[dz]))

    def drain(self):
        for copy, _, _, _ in self.copies.values():
            copy.wait_send()


def norm_rows(tok_ref, gain_ref, start, count):
    @pl.loop(0, count // 16)
    def _(step):
        rows = pl.ds(pl.multiple_of(start + step * 16, 16), 16)
        values = tok_ref[rows, :].astype(F32)
        squares = jnp.mean(values * values, axis=-1, keepdims=True)
        tok_ref[rows, :] = (values * lax.rsqrt(squares + EPSILON) * gain_ref[...]).astype(BF16)


def front_kernel(heads, tok_hbm, pool_hbm, query_hbm, key_hbm, value_hbm, pool_out_hbm,
                 delta_out_hbm, gain_ref, strength_ref, decay_ref, taps_ref, spike_ref, rate_ref,
                 decay_shift_ref, strength_shift_ref,
                 from_state_ref, local_ref, map_out_ref, pool_acc_ref, out_w_hbm,
                 tok_ref, wide_ref, late_ref, acc_ref, thin_ref, grow_ref, gcol_ref, bcol_ref,
                 masks_ref, map_ref, tok_sems, load_sems, halo_send, halo_recv,
                 send_a, recv_a, send_b, recv_b, out_sem):
    z, x, tp = lax.axis_index("sp_0"), lax.axis_index("sp_1"), lax.axis_index("tp")
    tok_rows = tok_hbm.shape[0]
    chunks = tok_rows // CHUNK
    mine = z * 4 + x
    loads = []
    for k, (hbm, ref, rows, lanes) in enumerate((
            (query_hbm, wide_ref, 0, 0), (key_hbm, wide_ref, 0, 256), (value_hbm, wide_ref, 0, 512),
            (pool_hbm, late_ref, 0, 0), (pool_out_hbm, late_ref, 256, 0),
            (delta_out_hbm, late_ref, 512, 0))):
        load = pltpu.make_async_copy(
            hbm, ref.at[mine, pl.ds(rows, 256), pl.ds(lanes, 256)], load_sems.at[k])
        load.start()
        loads.append(load)
    tok_loads = []
    for k in range(chunks):
        load = pltpu.make_async_copy(
            tok_hbm.at[pl.ds(k * CHUNK, CHUNK), :],
            tok_ref.at[pl.ds(HALO + k * CHUNK, CHUNK), :], tok_sems.at[k])
        load.start()
        tok_loads.append(load)
    at = lax.broadcasted_iota(jnp.int32, (16, 256), 0)
    thin = jnp.zeros((16, 256), F32)
    for k, (ref, row) in enumerate(((strength_ref, 0), (strength_ref, 1), (decay_ref, 0),
                                    (decay_ref, 1))):
        row_values = ref[...].astype(F32)[row : row + 1]
        thin = jnp.where(at == k, jnp.broadcast_to(row_values, (16, 256)), thin)
    wide_ref[mine, 256:272, 0:256] = thin.astype(BF16)
    wide_ref[mine, 256:272, 256:768] = jnp.zeros((16, 512), BF16)

    following = lax.rem(mine + 1, 16)
    before = lax.rem(mine + 15, 16)
    barrier = pltpu.get_barrier_semaphore()
    for dz, dx in ((0, 1), (0, -1), (1, 0), (-1, 0)):
        pl.semaphore_signal(
            barrier, 1, device_id={"sp_0": lax.rem(z + dz + 4, 4), "sp_1": lax.rem(x + dx + 4, 4)},
            device_id_type=MESH_ID)
    for other in (following, before):
        pl.semaphore_signal(
            barrier, 1, device_id={"sp_0": other // 4, "sp_1": lax.rem(other, 4)},
            device_id_type=MESH_ID)
    fill_masks(masks_ref)
    for load in loads:
        load.wait()
    pl.semaphore_wait(barrier, 6)

    early = PlaneGather(wide_ref, SPLIT_A, send_a, recv_a)
    early.own()
    halo = pltpu.make_async_remote_copy(
        src_ref=tok_hbm.at[pl.ds(tok_rows - HALO, HALO), :], dst_ref=tok_ref.at[pl.ds(0, HALO), :],
        send_sem=halo_send, recv_sem=halo_recv,
        device_id={"sp_0": following // 4, "sp_1": lax.rem(following, 4)}, device_id_type=MESH_ID)
    halo.start()
    for k in range(chunks):
        tok_loads[k].wait()
        norm_rows(tok_ref, gain_ref, HALO + k * CHUNK, CHUNK)
    halo.wait()

    @pl.when(mine == 0)
    def _():
        tok_ref[0:HALO, :] = jnp.zeros((HALO, tok_ref.shape[1]), BF16)

    norm_rows(tok_ref, gain_ref, 0, HALO)

    tile = 208

    def project(gather, dz, dx, into, first=False):
        shard = gather.shard(dz, dx)
        lanes = pl.ds(pl.multiple_of(shard * 256, 256), 256)

        @pl.loop(0, acc_ref.shape[0] // tile)
        def _(step):
            rows = pl.ds(pl.multiple_of(step * tile, 16), tile)
            normed = tok_ref[rows, lanes]
            product = dot(normed, gather.buf[shard, 0:256, :])
            into[rows, :] = product if first else into[rows, :] + product
            if gather is early:
                narrow = dot_nt(normed, gather.buf[shard, 256:272, 0:256])
                thin_ref[rows, :] = narrow if first else thin_ref[rows, :] + narrow

    project(early, 0, 0, acc_ref, first=True)
    early.first()
    early.second()
    for dz, dx in ORDER[:4]:
        project(early, dz, dx, acc_ref)
    early.third()
    early.fourth()
    for dz, dx in ORDER[4:8]:
        project(early, dz, dx, acc_ref)
    early.fifth()
    late = PlaneGather(late_ref, SPLIT_B, send_b, recv_b)
    late.own()
    for dz, dx in ORDER[8:]:
        early.last(dz, dx)
        project(early, dz, dx, acc_ref)

    narrow = thin_ref[HALO:, :].T
    total = tok_rows
    heads_at = lax.broadcasted_iota(jnp.int32, (16, total), 0)

    def own_scalar(ref, head):
        return ref[tp * heads + head]

    for head in range(heads):
        strength = narrow[head : head + 1] + own_scalar(strength_shift_ref, head)
        beta = 1.0 / (1.0 + jnp.exp(-strength))
        level = narrow[heads + head : heads + head + 1] + own_scalar(decay_shift_ref, head)
        soft = jnp.maximum(level, 0.0) + jnp.log1p(jnp.exp(-jnp.abs(level)))
        rate = jnp.exp(jnp.full((1, total), own_scalar(rate_ref, head), F32))
        decay = spike_ref[head : head + 1, :] - rate * soft
        lane = lax.rem(lax.broadcasted_iota(jnp.int32, (8, total), 1), CHUNK)
        summed = jnp.broadcast_to(decay, (8, total))
        step = 1
        while step < CHUNK:
            summed = summed + jnp.where(lane >= step, pltpu.roll(summed, step, 1), 0.0)
            step *= 2
        for chunk in range(chunks):
            row = head * chunks + chunk
            part = slice(chunk * CHUNK, chunk * CHUNK + CHUNK)
            grow_ref[row] = summed[:, part]
            gcol_ref[row] = jnp.broadcast_to(summed[0:1, part], (128, CHUNK)).T
            bcol_ref[row] = jnp.broadcast_to(beta[:, part], (128, CHUNK)).T
    rows = lax.broadcasted_iota(jnp.int32, (128, 256), 0)
    cols = lax.broadcasted_iota(jnp.int32, (128, 256), 1)
    for head in range(heads):
        map_ref[head] = jnp.where(rows == cols, 1.0, 0.0)

    def delta(low, high):
        @pl.loop(low, high)
        def _(chunk):
            delta_chunk(chunk, heads, chunks, acc_ref, taps_ref, grow_ref, gcol_ref, bcol_ref,
                        masks_ref, map_ref, from_state_ref, local_ref)

    late.first()
    late.second()
    delta(0, chunks // 2)
    late.third()
    late.fourth()
    delta(chunks // 2, chunks)
    map_out_ref[...] = map_ref[...].astype(BF16)
    late.fifth()
    project(late, 0, 0, pool_acc_ref, first=True)
    for dz, dx in ORDER[:8]:
        project(late, dz, dx, pool_acc_ref)
    for dz, dx in ORDER[8:]:
        late.last(dz, dx)
        project(late, dz, dx, pool_acc_ref)
    result = pltpu.make_async_copy(late_ref.at[:, pl.ds(256, 512), :], out_w_hbm, out_sem)
    result.start()
    early.drain()
    late.drain()
    result.wait()


def front(tokens, weights, out_weights, gain, strength, decay, taps, spike, rate, decay_shift,
          strength_shift, heads):
    tok_rows, depth = tokens.shape
    chunks = tok_rows // CHUNK
    vmem = pl.BlockSpec(memory_space=pltpu.VMEM)
    smem = pl.BlockSpec(memory_space=pltpu.SMEM)
    hbm = pl.BlockSpec(memory_space=pl.ANY)
    pairs = heads * chunks
    dma = pltpu.SemaphoreType.DMA
    return pl.pallas_call(
        lambda *refs: front_kernel(heads, *refs),
        out_shape=(
            jax.ShapeDtypeStruct((heads, tok_rows, 128), BF16),
            jax.ShapeDtypeStruct((heads, tok_rows, 128), F32),
            jax.ShapeDtypeStruct((heads, 128, 256), BF16),
            jax.ShapeDtypeStruct((tok_rows + HALO, 256), F32),
            jax.ShapeDtypeStruct((16, 512, 256), BF16),
        ),
        in_specs=[hbm] * 7 + [vmem] * 5 + [smem] * 3,
        out_specs=(vmem, vmem, vmem, vmem, hbm),
        scratch_shapes=[
            pltpu.VMEM((tok_rows + HALO, depth), BF16),
            pltpu.VMEM((16,) + ROWS_A, BF16),
            pltpu.VMEM((16,) + ROWS_B, BF16),
            pltpu.VMEM((tok_rows + HALO, 768), F32),
            pltpu.VMEM((tok_rows + HALO, 16), F32),
            pltpu.VMEM((pairs, 8, CHUNK), F32),
            pltpu.VMEM((pairs, CHUNK, 128), F32),
            pltpu.VMEM((pairs, CHUNK, 128), F32),
            pltpu.VMEM((8, CHUNK, CHUNK), BF16),
            pltpu.VMEM((heads, 128, 256), F32),
            dma((chunks,)), dma((6,)), dma(()), dma(()),
            dma((32,)), dma((32,)), dma((32,)), dma((32,)), dma(()),
        ],
        compiler_params=pltpu.CompilerParams(
            vmem_limit_bytes=VMEM_LIMIT, collective_id=1, has_side_effects=True),
        name="front",
    )(tokens, *weights, *out_weights, gain, strength, decay, taps, spike, rate, decay_shift,
      strength_shift)


def after(later, earlier):
    offset = jnp.concatenate([jnp.zeros((128, 128), F32), later[:, 128:].astype(F32)], axis=1)
    return dot(later[:, :128], earlier.astype(BF16)) + offset


PIECE = 1024


def device_at(z=0, x=0, tp=0):
    place = {}
    for name, step in (("sp_0", z), ("sp_1", x), ("tp", tp)):
        if step:
            size = lax.axis_size(name)
            place[name] = lax.rem(lax.axis_index(name) + step + size, size)
    return place


def remote(src, dst, send_sem, recv_sem, place):
    return pltpu.make_async_remote_copy(
        src_ref=src, dst_ref=dst, send_sem=send_sem, recv_sem=recv_sem, device_id=place,
        device_id_type=MESH_ID)


def pooled_rows(pool_ref, chunk, position, wide, mix_ref, scale_ref):
    parts = []
    for group in range(2):
        lanes = slice(group * 128, group * 128 + 128)
        rows = pool_ref[pl.ds(pl.multiple_of(chunk * CHUNK, CHUNK), CHUNK + HALO), lanes]
        reach = 1
        sums = rows
        for _ in range(group + 1):
            sums = sums + pltpu.roll(sums, reach, 0)
            reach *= 2
        broad = sums
        for _ in range(2):
            broad = broad + pltpu.roll(broad, reach, 0)
            reach *= 2
        short, long = 2 << group, 8 << group
        seen = lax.broadcasted_iota(jnp.int32, (CHUNK, 128), 0) + (position + chunk * CHUNK + 1)
        count = jnp.minimum(seen, jnp.where(wide, long, short)).astype(F32)
        window = jnp.where(wide, broad[HALO:], sums[HALO:])
        diff = (window / count - rows[HALO:]).astype(BF16)
        parts.append((dot(diff, mix_ref[group]) * scale_ref[0:1, lanes]).astype(BF16))
    return parts


def back_kernel(heads, own_ref, gain_ref, mix_ref, scale_ref, from_state_hbm, local_hbm, pool_hbm,
                out_w_hbm, out_ref,
                from_state_ref, local_ref, pool_ref, out_w_ref, row_ref, total_ref, column_ref,
                state_ref, mixed_ref, part_ref, pair_out_ref, pair_in_ref, ring_out_ref,
                half_ref, final_ref, load_sems, send_x, recv_x, send_z, recv_z, pair_send,
                pair_recv, ring_send, ring_recv):
    z, x, tp = lax.axis_index("sp_0"), lax.axis_index("sp_1"), lax.axis_index("tp")
    n_z, n_x = lax.axis_size("sp_0"), lax.axis_size("sp_1")
    y, core = tp // 2, lax.rem(tp, 2)
    n_y = lax.axis_size("tp") // 2
    chunks = pool_ref.shape[0] // CHUNK
    position = (z * n_x + x) * (chunks * CHUNK)
    loads = []
    for k, (hbm, ref) in enumerate(((pool_hbm, pool_ref), (from_state_hbm, from_state_ref),
                                    (local_hbm, local_ref), (out_w_hbm, out_w_ref))):
        load = pltpu.make_async_copy(hbm, ref, load_sems.at[k])
        load.start()
        loads.append(load)
    other = {"tp": y * 2 + (1 - core)}
    peers = [device_at(x=step) for step in range(1, n_x)]
    peers += [device_at(z=step) for step in range(1, n_z)]
    peers += [other, device_at(tp=2), device_at(tp=-2)]
    barrier = pltpu.get_barrier_semaphore()
    for peer in peers:
        pl.semaphore_signal(barrier, 1, device_id=peer, device_id_type=MESH_ID)
    pl.semaphore_wait(barrier, len(peers))

    along_x = [remote(own_ref, row_ref.at[step], send_x.at[step], recv_x.at[step],
                      device_at(x=step)) for step in range(1, n_x)]
    for copy in along_x:
        copy.start()
    row_ref[0] = own_ref[...]
    loads[0].wait()
    wide = core == 1

    def store_halves(chunk, lanes, values):
        for half in range(2):
            slot = lax.rem(half + core, 2)
            mixed_ref[chunk, pl.ds(pl.multiple_of(slot * 128, 128), 128), lanes] = (
                values[half * 128 : half * 128 + 128])

    @pl.loop(0, chunks)
    def _(chunk):
        for group, values in enumerate(
                pooled_rows(pool_ref, chunk, position, wide, mix_ref, scale_ref)):
            store_halves(chunk, slice(group * 128, group * 128 + 128), values)

    for copy in along_x:
        copy.wait_recv()
    inside = []
    rows = lax.broadcasted_iota(jnp.int32, (128, 256), 0)
    cols = lax.broadcasted_iota(jnp.int32, (128, 256), 1)
    for head in range(heads):
        so_far = before = jnp.where(rows == cols, 1.0, 0.0)
        for k in range(n_x):
            piece = row_ref[lax.rem(x - k + n_x, n_x), head]
            so_far = piece.astype(F32) if k == 0 else after(piece, so_far)
            before = jnp.where(k < x, so_far, before)
        inside.append(before)
        total_ref[head] = so_far.astype(BF16)
    along_z = [remote(total_ref, column_ref.at[step], send_z.at[step], recv_z.at[step],
                      device_at(z=step)) for step in range(1, n_z)]
    for copy in along_z:
        copy.start()
    column_ref[0] = total_ref[...]
    for load in loads[1:]:
        load.wait()
    for copy in along_z:
        copy.wait_recv()
    for head in range(heads):
        so_far = state = jnp.zeros((128, 128), F32)
        for k in range(n_z - 1):
            piece = column_ref[lax.rem(z - k + n_z, n_z), head]
            offset = piece[:, 128:].astype(F32)
            so_far = offset if k == 0 else dot(piece[:, :128], so_far.astype(BF16)) + offset
            state = jnp.where(k < z, so_far, state)
        entering = dot(inside[head][:, :128].astype(BF16), state.astype(BF16))
        state_ref[head] = (entering + inside[head][:, 128:]).astype(BF16)

    pairs, rings = {}, []

    def produce(ahead, order):
        chunk = lax.rem(y + ahead, n_y)
        where_rows = pl.ds(pl.multiple_of(chunk * CHUNK, CHUNK), CHUNK)
        for head in range(heads):
            raw = dot(from_state_ref[head, where_rows, :], state_ref[head])
            raw = raw + local_ref[head, where_rows, :]
            squares = jnp.mean(raw * raw, axis=-1, keepdims=True)
            normed = (raw * lax.rsqrt(squares + EPSILON) * gain_ref[...]).astype(BF16)
            store_halves(chunk, slice(256 + head * 128, 384 + head * 128), normed)
        for piece in order:
            @pl.loop(0, PIECE // 256)
            def _(block):
                lanes = pl.ds(pl.multiple_of(block * 256, 256), 256)
                product = dot(mixed_ref[chunk], out_w_ref[piece * (PIECE // 256) + block])
                part_ref[ahead, piece, :, lanes] = product[:128]
                pair_out_ref[ahead, piece, :, lanes] = product[128:].astype(BF16)

            index = ahead * 4 + piece
            copy = remote(pair_out_ref.at[ahead, piece], pair_in_ref.at[ahead, piece],
                          pair_send.at[index], pair_recv.at[index], other)
            copy.start()
            pairs[ahead, piece] = copy

    def chip_sum(ahead, piece):
        pairs[ahead, piece].wait_recv()
        return part_ref[ahead, piece] + pair_in_ref[ahead, piece].astype(F32)

    def pass_on(ahead, piece, value, place, target):
        slot = ahead - 1
        ring_out_ref[slot, piece] = value.astype(BF16)
        index = len(rings)
        copy = remote(ring_out_ref.at[slot, piece], target, ring_send.at[index],
                      ring_recv.at[index], place)
        copy.start()
        rings.append(copy)
        return copy

    up, down = device_at(tp=2), device_at(tp=-2)
    produce(2, (0, 2, 1, 3))
    halves = {}
    for piece in (0, 2, 1, 3):
        halves[piece] = pass_on(2, piece, chip_sum(2, piece), up if piece < 2 else down,
                                half_ref.at[piece])
    finals = {}
    produce(1, (2, 3, 0, 1))
    produce(3, (0, 1, 2, 3))
    for k in range(2):
        piece = 2 + k
        finals[1, piece] = pass_on(1, piece, chip_sum(1, piece), up, final_ref.at[0, piece])
        piece = k
        finals[3, piece] = pass_on(3, piece, chip_sum(3, piece), down, final_ref.at[1, piece])
    produce(0, (0, 1, 2, 3))
    for k in range(2):
        for ahead, piece, place, side in ((1, k, up, 0), (3, 2 + k, down, 1)):
            value = chip_sum(ahead, piece)
            halves[piece].wait_recv()
            value = value + half_ref[piece].astype(F32)
            finals[ahead, piece] = pass_on(ahead, piece, value, place, final_ref.at[side, piece])
    for piece in range(4):
        part_ref[0, piece] = chip_sum(0, piece)
    for first, second in ((2, 0), (3, 1), (0, 2), (1, 3)):
        for side, ahead, piece in ((0, 1, first), (1, 3, second)):
            finals[ahead, piece].wait_recv()
            part_ref[0, piece] = part_ref[0, piece] + final_ref[side, piece].astype(F32)
    for piece in range(4):
        out_ref[:, piece * PIECE : piece * PIECE + PIECE] = part_ref[0, piece].astype(BF16)
    for copy in along_x + along_z + list(pairs.values()) + rings:
        copy.wait_send()


def back(own_map, gain, mix, scale, from_state, local, pool_raw, out_weight):
    heads, tok_rows, _ = from_state.shape
    n_z, n_x = lax.axis_size("sp_0"), lax.axis_size("sp_1")
    width = out_weight.shape[0] * 256
    chunks = tok_rows // CHUNK
    pieces = width // PIECE
    vmem = pl.BlockSpec(memory_space=pltpu.VMEM)
    hbm = pl.BlockSpec(memory_space=pl.ANY)
    dma = pltpu.SemaphoreType.DMA
    return pl.pallas_call(
        lambda *refs: back_kernel(heads, *refs),
        out_shape=jax.ShapeDtypeStruct((128, width), BF16),
        in_specs=[vmem] * 4 + [hbm] * 4,
        out_specs=vmem,
        scratch_shapes=[
            pltpu.VMEM(from_state.shape, BF16),
            pltpu.VMEM(local.shape, F32),
            pltpu.VMEM(pool_raw.shape, F32),
            pltpu.VMEM(out_weight.shape, BF16),
            pltpu.VMEM((n_x, heads, 128, 256), BF16),
            pltpu.VMEM((heads, 128, 256), BF16),
            pltpu.VMEM((n_z, heads, 128, 256), BF16),
            pltpu.VMEM((heads, 128, 128), BF16),
            pltpu.VMEM((chunks, CHUNK, 512), BF16),
            pltpu.VMEM((4, pieces, 128, PIECE), F32),
            pltpu.VMEM((4, pieces, 128, PIECE), BF16),
            pltpu.VMEM((4, pieces, 128, PIECE), BF16),
            pltpu.VMEM((3, pieces, 128, PIECE), BF16),
            pltpu.VMEM((pieces, 128, PIECE), BF16),
            pltpu.VMEM((2, pieces, 128, PIECE), BF16),
            dma((4,)), dma((n_x,)), dma((n_x,)), dma((n_z,)), dma((n_z,)),
            dma((16,)), dma((16,)), dma((12,)), dma((12,)),
        ],
        compiler_params=pltpu.CompilerParams(
            vmem_limit_bytes=VMEM_LIMIT, collective_id=0, has_side_effects=True),
        name="back",
    )(own_map, gain, mix, scale, from_state, local, pool_raw, out_weight)


def per_device(tokens, input_norm_scale, mean_input_weight, query_matrix, key_matrix, value_matrix,
               strength_weight, decay_input_weight, causal_filter_weight, head_decay_logrates,
               decay_input_shift, strength_shift, decay_spike, head_norm_scale,
               group_mixing_weight, mean_channel_scale, mean_output_weight, delta_output_weight):
    pool_cols = mean_input_weight.shape[1]
    delta_cols = query_matrix.shape[1]
    heads = strength_weight.shape[1]
    groups = pool_cols // GROUP_DIM
    tp = lax.axis_index("tp")
    taps = lax.dynamic_slice_in_dim(causal_filter_weight, tp * delta_cols, delta_cols, 2)
    taps = taps.reshape(CONV, 3 * delta_cols).astype(F32)
    from_state, local, own_map, pool_raw, out_weight = front(
        tokens, (mean_input_weight, query_matrix, key_matrix, value_matrix),
        (mean_output_weight, delta_output_weight), input_norm_scale.astype(F32).reshape(1, -1),
        strength_weight.T, decay_input_weight.T, taps, decay_spike.T, head_decay_logrates,
        decay_input_shift, strength_shift, heads)
    mix = lax.dynamic_slice_in_dim(group_mixing_weight, tp * groups, groups, 0)
    scale = lax.dynamic_slice_in_dim(mean_channel_scale, tp * pool_cols, pool_cols)
    return back(own_map, head_norm_scale.astype(F32).reshape(1, HEAD_DIM), mix,
                scale.astype(F32).reshape(1, pool_cols), from_state, local, pool_raw, out_weight)


def solution(mesh):
    finer = Mesh(mesh.devices.reshape(4, 4, mesh.shape["tp"]), SP_TP)
    in_specs = (
        P(SP, None), P(), P(SP, "tp"), P(SP, "tp"), P(SP, "tp"), P(SP, "tp"), P(SP, "tp"),
        P(SP, "tp"), P(), P(), P(), P(), P(SP, "tp"), P(), P(), P(), P("tp", SP), P("tp", SP),
    )
    return jax.shard_map(
        per_device, mesh=finer, in_specs=in_specs, out_specs=P(SP_TP, None), check_vma=False
    )
```

```python
import jax
import jax.numpy as jnp
from jax import lax
from jax.experimental import pallas as pl
from jax.experimental.pallas import tpu as pltpu
from jax.sharding import Mesh
from jax.sharding import PartitionSpec as P

HEAD_DIM = 128
CONV = 4
CHUNK = 256
HALO = 16
EPSILON = 1e-06
SP = ("sp_0", "sp_1")
SP_TP = ("sp_0", "sp_1", "tp")
MESH_ID = pl.DeviceIdType.MESH
F32 = jnp.float32
BF16 = jnp.bfloat16
VMEM_LIMIT = 63 * 1000 * 1000


def dot(a, b):
    return jnp.dot(a, b, preferred_element_type=F32)


def dot_nt(a, b):
    return lax.dot_general(a, b, (((1,), (1,)), ((), ())), preferred_element_type=F32)


def dot_tn(a, b):
    return lax.dot_general(a, b, (((0,), (0,)), ((), ())), preferred_element_type=F32)


def unit_rows(values):
    return values * lax.rsqrt(jnp.sum(values * values, axis=-1, keepdims=True) + EPSILON)


def fill_masks(masks_ref):
    rows = lax.broadcasted_iota(jnp.int32, (CHUNK, CHUNK), 0)
    cols = lax.broadcasted_iota(jnp.int32, (CHUNK, CHUNK), 1)
    apart = jnp.bitwise_xor(rows, cols)
    for level in range(masks_ref.shape[0]):
        inside = (rows > cols) & (apart >= 2**level) & (apart < 2 ** (level + 1))
        masks_ref[level] = jnp.where(inside, 1.0, 0.0).astype(BF16)


def conv_rows(raw_ref, taps_ref, start, part):
    lanes = slice(part * 128, part * 128 + 128)
    tap_lanes = slice(part % 2 * 128, part % 2 * 128 + 128)
    rows = raw_ref[pl.ds(pl.multiple_of(start + HALO - 8, 8), CHUNK + 8), lanes]
    mixed = taps_ref[part // 2, CONV - 1 : CONV, tap_lanes] * rows[8:]
    for back in range(1, CONV):
        tap = taps_ref[part // 2, CONV - 1 - back : CONV - back, tap_lanes]
        mixed = mixed + tap * pltpu.roll(rows, back, 0)[8:]
    return mixed / (1.0 + jnp.exp(-mixed))


def delta_chunk(chunk, heads, chunks, raw_ref, taps_ref, grow_ref, gcol_ref, bcol_ref, masks_ref,
                map_ref, from_state_ref, local_ref):
    start = chunk * CHUNK
    rows = lax.broadcasted_iota(jnp.int32, (CHUNK, CHUNK), 0)
    cols = lax.broadcasted_iota(jnp.int32, (CHUNK, CHUNK), 1)
    work = []
    for head in range(heads):
        row = head * chunks + chunk
        query = unit_rows(conv_rows(raw_ref, taps_ref, start, head)) * HEAD_DIM ** (-0.5)
        key = unit_rows(conv_rows(raw_ref, taps_ref, start, heads + head))
        value = conv_rows(raw_ref, taps_ref, start, 2 * heads + head)
        gcol, bcol, grow = gcol_ref[row], bcol_ref[row], grow_ref[row][0:1]
        key_b = key.astype(BF16)
        both = jnp.concatenate([query.astype(BF16), key_b], axis=0)
        inner = dot_nt(both, key_b)
        spread = jnp.exp(jnp.minimum(jnp.concatenate([gcol, gcol], axis=1) - grow, 0.0))
        scores = jnp.where(rows >= cols, inner[:CHUNK] * spread, 0.0).astype(BF16)
        strict = jnp.where(rows > cols, inner[CHUNK:] * spread, 0.0)
        strict = (strict * jnp.concatenate([bcol, bcol], axis=1)).astype(BF16)
        grown = jnp.exp(gcol)
        right = jnp.concatenate([value * bcol, key * bcol * grown], axis=1).astype(BF16)
        last = grow[:, CHUNK - 1 : CHUNK]
        key_dec = (key * jnp.exp(last - gcol)).astype(BF16)
        inverse = jnp.where(rows == cols, 1.0, 0.0).astype(BF16) - strict * masks_ref[0]
        work.append([strict, inverse, scores, right, key_dec, query * grown, jnp.exp(last)])
    for level in range(1, masks_ref.shape[0]):
        inner = [dot(w[0] * masks_ref[level], w[1]).astype(BF16) for w in work]
        for w, part in zip(work, inner):
            w[1] = w[1] - dot(w[1], part).astype(BF16)
    for head in range(heads):
        _, inverse, scores, right, key_dec, query_dec, kept = work[head]
        solved = dot(inverse, right).astype(BF16)
        seen = dot(scores, solved)
        moved = dot_tn(key_dec, solved)
        current = map_ref[head]
        current_b = current.astype(BF16)
        asked = (query_dec - seen[:, 128:]).astype(BF16)
        answer = dot(asked, current_b)
        where_rows = pl.ds(pl.multiple_of(start, CHUNK), CHUNK)
        from_state_ref[head, where_rows, :] = answer[:, :128].astype(BF16)
        local_ref[head, where_rows, :] = answer[:, 128:] + seen[:, :128]
        added = jnp.concatenate([jnp.zeros((128, 128), F32), moved[:, :128]], axis=1)
        map_ref[head] = current * kept - dot(moved[:, 128:].astype(BF16), current_b) + added


SPLIT_A = 128
PIECE = 1024
ORDER = ((0, 0), (0, 1), (0, -1), (1, 0), (-1, 0), (1, 1), (1, -1), (-1, 1), (-1, -1), (0, 2), (2, 0),
         (1, 2), (-1, 2), (2, 1), (2, -1), (2, 2))


class PlaneGather:
    def __init__(self, buf, split, send_sems, recv_sems):
        self.buf, self.split = buf, split
        self.send_sems, self.recv_sems = send_sems, recv_sems
        self.z, self.x = lax.axis_index("sp_0"), lax.axis_index("sp_1")
        self.copies = {}

    def shard(self, dz, dx):
        return lax.rem(self.z + dz + 4, 4) * 4 + lax.rem(self.x + dx + 4, 4)

    def rows(self, part):
        split, total = self.split, self.buf.shape[1]
        quarter = split // 32 * 16
        rest = split + (total - split) // 32 * 16
        return {"a": (0, split), "b": (split, total), "a0": (0, quarter), "a1": (quarter, split),
                "b0": (split, rest), "b1": (rest, total)}[part]

    def region(self, dz, dx, part):
        low, high = self.rows(part)
        return self.buf.at[self.shard(dz, dx), pl.ds(low, high - low), :]

    def copy(self, name, way, source):
        index, _, part = self.copies[name, way]
        ref = self.region(source[0], source[1], part)
        return remote(ref, ref, self.send_sems.at[index], self.recv_sems.at[index],
                      {"sp_0": lax.rem(self.z + way[0] + 4, 4),
                       "sp_1": lax.rem(self.x + way[1] + 4, 4)})

    def send(self, name, source, part, way):
        self.copies[name, way] = (len(self.copies), source, part)
        self.copy(name, way, source).start()

    def got(self, name, way):
        source = self.copies[name, way][1]
        self.copy(name, way, (source[0] - way[0], source[1] - way[1])).wait_recv()

    def own(self):
        for step in (1, -1):
            self.send("a", (0, 0), "a", (0, step))
            self.send("b", (0, 0), "b", (step, 0))
        for step in (1, -1):
            self.send("b", (0, 0), "b", (0, step))
            self.send("a", (0, 0), "a", (step, 0))

    def first(self):
        for step in (1, -1):
            self.got("a", (0, step))
            self.got("b", (step, 0))
        self.send("a2", (0, -1), "a0", (0, 1))
        self.send("a2", (0, 1), "a1", (0, -1))
        self.send("b2", (-1, 0), "b0", (1, 0))
        self.send("b2", (1, 0), "b1", (-1, 0))
        for at in (1, -1):
            for step in (1, -1):
                self.send(("a3", at), (0, at), "a", (step, 0))
                self.send(("b3", at), (at, 0), "b", (0, step))

    def second(self):
        for step in (1, -1):
            self.got("b", (0, step))
            self.got("a", (step, 0))
        self.send(("a4", 0), (-1, 0), "a", (1, 0))
        self.send(("b4", 0), (0, -1), "b", (0, 1))

    def third(self, along="xz"):
        for step in (1, -1):
            self.got("a2", (0, step)) if "z" in along else None
            self.got("b2", (step, 0)) if "x" in along else None
        for step in (-1, 1):
            if "z" in along:
                self.send(("a3", 2), (0, 2), "a", (step, 0))
            if "x" in along:
                self.send(("b3", 2), (2, 0), "b", (0, step))

    def fourth(self):
        for at in (1, -1):
            for step in (1, -1):
                self.got(("a3", at), (step, 0))
                self.got(("b3", at), (0, step))
        for at in (1, -1):
            self.send(("a4", at), (-at, at), "a", (at, 0))
            self.send(("b4", at), (at, -at), "b", (0, at))

    def fifth(self):
        for step in (1, -1):
            self.got(("a3", 2), (step, 0))
            self.got(("b3", 2), (0, step))
        self.send(("a4", 2), (1, 2), "a", (-1, 0))
        self.send(("b4", 2), (2, 1), "b", (0, -1))

    def last(self, dz, dx):
        side = {0: 1, 1: 1, -1: -1, 2: -1}
        if dz == 2:
            self.got(("a4", dx), (side[dx], 0))
        if dx == 2:
            self.got(("b4", dz), (0, side[dz]))

    def drain(self):
        for (name, way), (_, source, _) in self.copies.items():
            self.copy(name, way, source).wait_send()


def after(later, earlier):
    offset = jnp.concatenate([jnp.zeros((128, 128), F32), later[:, 128:].astype(F32)], axis=1)
    return dot(later[:, :128], earlier.astype(BF16)) + offset


def device_at(z=0, x=0, tp=0):
    place = {}
    for name, step in (("sp_0", z), ("sp_1", x), ("tp", tp)):
        if step:
            size = lax.axis_size(name)
            place[name] = lax.rem(lax.axis_index(name) + step + size, size)
    return place


def remote(src, dst, send_sem, recv_sem, place):
    return pltpu.make_async_remote_copy(
        src_ref=src, dst_ref=dst, send_sem=send_sem, recv_sem=recv_sem, device_id=place,
        device_id_type=MESH_ID)


def pooled_rows(pool_ref, chunk, position, wide, mix_ref, scales):
    parts = []
    for group in range(2):
        lanes = slice(group * 128, group * 128 + 128)
        rows = pool_ref[pl.ds(pl.multiple_of(chunk * CHUNK, CHUNK), CHUNK + HALO), lanes]
        reach = 1
        sums = rows
        for _ in range(group + 1):
            sums = sums + pltpu.roll(sums, reach, 0)
            reach *= 2
        broad = sums
        for _ in range(2):
            broad = broad + pltpu.roll(broad, reach, 0)
            reach *= 2
        short, long = 2 << group, 8 << group
        seen = lax.broadcasted_iota(jnp.int32, (CHUNK, 128), 0) + (position + chunk * CHUNK + 1)
        count = jnp.minimum(seen, jnp.where(wide, long, short)).astype(F32)
        window = jnp.where(wide, broad[HALO:], sums[HALO:])
        diff = (window / count - rows[HALO:]).astype(BF16)
        parts.append((dot(diff, mix_ref[group]) * scales[group]).astype(BF16))
    return parts


def norm_rows(tok_ref, gain_ref, start, count, step_rows):
    @pl.loop(0, count // step_rows)
    def _(step):
        rows = pl.ds(pl.multiple_of(start + step * step_rows, 16), step_rows)
        values = tok_ref[rows, :].astype(F32)
        scale = lax.rsqrt(jnp.mean(values * values, axis=-1, keepdims=True) + EPSILON)
        tok_ref[rows, :] = (tok_ref[rows, :].astype(F32) * scale * gain_ref[0:1, :]).astype(BF16)


def layer_kernel(heads, tok_hbm, pool_hbm, query_hbm, key_hbm, value_hbm, pool_out_hbm,
                 delta_out_hbm, taps_hbm, mix_hbm, gain_in_ref, head_gain_ref, scale_in_ref,
                 strength_ref, decay_ref, spike_ref, rate_ref, decay_shift_ref, strength_shift_ref,
                 out_ref,
                 tok_ref, wide_ref, pool_w_ref, out_w_ref, acc_ref, pool_ref, thin_ref, gain_ref,
                 taps_in_ref, taps_ref, mix_ref, grow_ref, gcol_ref, bcol_ref, masks_ref, map_ref,
                 from_state_ref, local_ref, own_ref, row_ref, total_ref, column_ref, state_ref,
                 mixed_ref, part_ref, pair_out_ref, pair_in_ref, ring_out_ref, half_ref, final_ref,
                 tok_sems, load_sems, halo_send, halo_recv, send_a, recv_a, send_b, recv_b,
                 send_c, recv_c, send_x, recv_x, send_z, recv_z, pair_send, pair_recv, ring_send,
                 ring_recv):
    z, x, tp = lax.axis_index("sp_0"), lax.axis_index("sp_1"), lax.axis_index("tp")
    n_z, n_x, n_tp = lax.axis_size("sp_0"), lax.axis_size("sp_1"), lax.axis_size("tp")
    y, core = tp // 2, lax.rem(tp, 2)
    n_y = n_tp // 2
    tok_rows, depth = tok_hbm.shape
    chunks = tok_rows // CHUNK
    mine = z * n_x + x
    position = mine * tok_rows
    loads = []
    for k, (hbm, ref) in enumerate((
            (query_hbm, wide_ref.at[mine, pl.ds(0, 256), pl.ds(0, 256)]),
            (key_hbm, wide_ref.at[mine, pl.ds(0, 256), pl.ds(256, 256)]),
            (value_hbm, wide_ref.at[mine, pl.ds(0, 256), pl.ds(512, 256)]),
            (pool_hbm, pool_w_ref.at[mine]),
            (pool_out_hbm, out_w_ref.at[mine, pl.ds(0, 256), :]),
            (delta_out_hbm, out_w_ref.at[mine, pl.ds(256, 256), :]),
            (taps_hbm.at[:, :, pl.ds(pl.multiple_of(tp * 256, 256), 256)], taps_in_ref),
            (mix_hbm.at[pl.ds(tp * 2, 2)], mix_ref))):
        load = pltpu.make_async_copy(hbm, ref, load_sems.at[k])
        load.start()
        loads.append(load)
    tok_loads = []
    for k in range(chunks):
        load = pltpu.make_async_copy(
            tok_hbm.at[pl.ds(k * CHUNK, CHUNK), :],
            tok_ref.at[pl.ds(HALO + k * CHUNK, CHUNK), :], tok_sems.at[k])
        load.start()
        tok_loads.append(load)
    following, before = lax.rem(mine + 1, 16), lax.rem(mine + 15, 16)
    next_place = {"sp_0": following // 4, "sp_1": lax.rem(following, 4)}
    last_place = {"sp_0": before // 4, "sp_1": lax.rem(before, 4)}
    peers = [device_at(x=step) for step in range(1, n_x)]
    peers += [device_at(z=step) for step in range(1, n_z)]
    peers += [device_at(tp=step) for step in range(1, n_tp)]
    peers += [next_place, last_place]
    barrier = pltpu.get_barrier_semaphore()
    for peer in peers:
        pl.semaphore_signal(barrier, 1, device_id=peer, device_id_type=MESH_ID)
    at = lax.broadcasted_iota(jnp.int32, (16, 256), 0)
    thin = jnp.zeros((16, 256), F32)
    for k, (ref, row) in enumerate(((strength_ref, 0), (strength_ref, 1), (decay_ref, 0),
                                    (decay_ref, 1))):
        row_values = ref[...].astype(F32)[row : row + 1]
        thin = jnp.where(at == k, jnp.broadcast_to(row_values, (16, 256)), thin)
    wide_ref[mine, 256:272, 0:256] = thin.astype(BF16)
    wide_ref[mine, 256:272, 256:768] = jnp.zeros((16, 512), BF16)
    gains = gain_in_ref[...].astype(F32)
    for k in range(depth // 128):
        gain_ref[:, k * 128 : k * 128 + 128] = jnp.broadcast_to(gains[k : k + 1], (8, 128))
    fill_masks(masks_ref)
    for load in loads[:3]:
        load.wait()
    pl.semaphore_wait(barrier, len(peers))

    early = PlaneGather(wide_ref, SPLIT_A, send_a, recv_a)
    slices = depth // n_tp

    def halo_part(owner):
        return tok_ref.at[pl.ds(0, HALO), pl.ds(pl.multiple_of(owner * slices, 128), slices)]

    halos = [remote(
        tok_hbm.at[pl.ds(tok_rows - HALO, HALO), pl.ds(pl.multiple_of(tp * slices, 128), slices)],
        halo_part(tp), halo_send.at[0], halo_recv.at[0], next_place)]
    halos[0].start()
    early.own()
    tok_loads[0].wait()
    norm_rows(tok_ref, gain_ref, HALO, CHUNK, 64)
    halos[0].wait_recv()
    for step in range(1, n_tp):
        copy = remote(halo_part(tp), halo_part(tp), halo_send.at[step], halo_recv.at[step],
                      device_at(tp=step))
        copy.start()
        halos.append(copy)
    tok_loads[1].wait()
    norm_rows(tok_ref, gain_ref, HALO + CHUNK, CHUNK, 64)
    early.first()
    for k in range(2, chunks):
        tok_loads[k].wait()
        norm_rows(tok_ref, gain_ref, HALO + k * CHUNK, CHUNK, 64)
    for step in range(1, n_tp):
        owner = lax.rem(tp - step + n_tp, n_tp)
        remote(halo_part(owner), halo_part(owner), halo_send.at[step], halo_recv.at[step],
               device_at(tp=step)).wait_recv()
    for copy in halos:
        copy.wait_send()

    @pl.when(mine == 0)
    def _():
        tok_ref[0:HALO, :] = jnp.zeros((HALO, depth), BF16)

    norm_rows(tok_ref, gain_ref, 0, HALO, HALO)
    early.second()
    tile = 208

    def project(gather, places, into, first=False):
        @pl.loop(0, acc_ref.shape[0] // tile)
        def _(step):
            rows = pl.ds(pl.multiple_of(step * tile, 16), tile)
            total = None if first else into[rows, :]
            narrow = None if first or gather is not early else thin_ref[rows, :]
            for dz, dx in places:
                shard = gather.shard(dz, dx)
                normed = tok_ref[rows, pl.ds(pl.multiple_of(shard * 256, 256), 256)]
                term = dot(normed, gather.buf[shard, 0:256, :])
                total = term if total is None else total + term
                if gather is early:
                    term = dot_nt(normed, gather.buf[shard, 256:272, 0:256])
                    narrow = term if narrow is None else narrow + term
            into[rows, :] = total
            if gather is early:
                thin_ref[rows, :] = narrow

    project(early, ORDER[:1], acc_ref, first=True)
    project(early, ORDER[1:5], acc_ref)
    early.third()
    early.fourth()
    project(early, ORDER[5:9], acc_ref)
    early.fifth()
    for load in loads[3:]:
        load.wait()
    pool = PlaneGather(pool_w_ref, 128, send_b, recv_b)
    pool.own()
    for places in (ORDER[9:13], ORDER[13:]):
        for dz, dx in places:
            early.last(dz, dx)
        project(early, places, acc_ref)

    taps_ref[...] = taps_in_ref[...].astype(F32)
    narrow = thin_ref[HALO:, :].T
    for head in range(heads):
        strength = narrow[head : head + 1] + strength_shift_ref[tp * heads + head]
        beta = 1.0 / (1.0 + jnp.exp(-strength))
        level = narrow[heads + head : heads + head + 1] + decay_shift_ref[tp * heads + head]
        soft = jnp.maximum(level, 0.0) + jnp.log1p(jnp.exp(-jnp.abs(level)))
        rate = jnp.exp(jnp.full((1, tok_rows), rate_ref[tp * heads + head], F32))
        decay = spike_ref[head : head + 1, :] - rate * soft
        lane = lax.rem(lax.broadcasted_iota(jnp.int32, (8, tok_rows), 1), CHUNK)
        summed = jnp.broadcast_to(decay, (8, tok_rows))
        step = 1
        while step < CHUNK:
            summed = summed + jnp.where(lane >= step, pltpu.roll(summed, step, 1), 0.0)
            step *= 2
        for chunk in range(chunks):
            row = head * chunks + chunk
            part = slice(chunk * CHUNK, chunk * CHUNK + CHUNK)
            grow_ref[row] = summed[:, part]
            gcol_ref[row] = jnp.broadcast_to(summed[0:1, part], (128, CHUNK)).T
            bcol_ref[row] = jnp.broadcast_to(beta[:, part], (128, CHUNK)).T
    rows = lax.broadcasted_iota(jnp.int32, (128, 256), 0)
    cols = lax.broadcasted_iota(jnp.int32, (128, 256), 1)
    identity = jnp.where(rows == cols, 1.0, 0.0)
    for head in range(heads):
        map_ref[head] = identity

    out = PlaneGather(out_w_ref, 256, send_c, recv_c)

    @pl.loop(0, chunks)
    def _(chunk):
        @pl.when(chunk == 0)
        def _():
            pool.first()
            pool.second()

        @pl.when(chunk == 1)
        def _():
            pool.third()
            pool.fourth()

        @pl.when(chunk == 2)
        def _():
            pool.fifth()
            out.own()

        delta_chunk(chunk, heads, chunks, acc_ref, taps_ref, grow_ref, gcol_ref, bcol_ref,
                    masks_ref, map_ref, from_state_ref, local_ref)

    own_ref[...] = map_ref[...].astype(BF16)
    row_ref[0] = own_ref[...]
    along_x = [remote(own_ref, row_ref.at[step], send_x.at[step], recv_x.at[step],
                      device_at(x=step)) for step in range(1, n_x)]
    for copy in along_x:
        copy.start()
    out.first()
    for dz, dx in ORDER[9:]:
        pool.last(dz, dx)
    for k in range(4):
        project(pool, ORDER[4 * k : 4 * k + 4], pool_ref, first=k == 0)
    wide = core == 1
    scales_at = lax.broadcasted_iota(jnp.int32, scale_in_ref.shape, 0)
    scales = [jnp.sum(jnp.where(scales_at == tp * 2 + group, scale_in_ref[...].astype(F32), 0.0),
                      axis=0, keepdims=True) for group in range(2)]

    def store_halves(chunk, lanes, values):
        for half in range(2):
            slot = lax.rem(half + core, 2)
            mixed_ref[chunk, pl.ds(pl.multiple_of(slot * 128, 128), 128), lanes] = (
                values[half * 128 : half * 128 + 128])

    for copy in along_x:
        copy.wait_recv()
    inside = []
    for head in range(heads):
        so_far = before_here = identity
        for k in range(n_x):
            piece = row_ref[lax.rem(x - k + n_x, n_x), head]
            so_far = piece.astype(F32) if k == 0 else after(piece, so_far)
            before_here = jnp.where(k < x, so_far, before_here)
        inside.append(before_here)
        total_ref[head] = so_far.astype(BF16)
    along_z = [remote(total_ref, column_ref.at[step], send_z.at[step], recv_z.at[step],
                      device_at(z=step)) for step in range(1, n_z)]
    for copy in along_z:
        copy.start()
    column_ref[0] = total_ref[...]
    out.second()
    out.third()

    @pl.loop(0, chunks)
    def _(chunk):
        for group, values in enumerate(
                pooled_rows(pool_ref, chunk, position, wide, mix_ref, scales)):
            store_halves(chunk, slice(group * 128, group * 128 + 128), values)

    for copy in along_z:
        copy.wait_recv()
    for head in range(heads):
        so_far = state = jnp.zeros((128, 128), F32)
        for k in range(n_z - 1):
            piece = column_ref[lax.rem(z - k + n_z, n_z), head]
            offset = piece[:, 128:].astype(F32)
            so_far = offset if k == 0 else dot(piece[:, :128], so_far.astype(BF16)) + offset
            state = jnp.where(k < z, so_far, state)
        entering = dot(inside[head][:, :128].astype(BF16), state.astype(BF16))
        state_ref[head] = (entering + inside[head][:, 128:]).astype(BF16)
    out.fourth()

    head_gain = head_gain_ref[...].astype(F32)
    partner = {"tp": y * 2 + (1 - core)}
    pairs, rings, finals, halves = {}, [], {}, {}
    slots = {2: 0, 1: 1, 3: 2, 0: 0}

    def finish_rows(ahead):
        chunk = lax.rem(y + ahead, n_y)
        where_rows = pl.ds(pl.multiple_of(chunk * CHUNK, CHUNK), CHUNK)
        for head in range(heads):
            raw = dot(from_state_ref[head, where_rows, :], state_ref[head])
            raw = raw + local_ref[head, where_rows, :]
            squares = jnp.mean(raw * raw, axis=-1, keepdims=True)
            normed = (raw * lax.rsqrt(squares + EPSILON) * head_gain).astype(BF16)
            store_halves(chunk, slice(256 + head * 128, 384 + head * 128), normed)

    def produce(ahead, piece):
        chunk = lax.rem(y + ahead, n_y)
        for block, (dz, dx) in enumerate(ORDER[4 * piece : 4 * piece + 4]):
            lanes = slice(block * 256, block * 256 + 256)
            product = dot(mixed_ref[chunk], out_w_ref[out.shard(dz, dx)])
            part_ref[slots[ahead], piece, :, lanes] = product[:128]
            pair_out_ref[ahead, piece, :, lanes] = product[128:].astype(BF16)
        index = ahead * 4 + piece
        copy = remote(pair_out_ref.at[ahead, piece], pair_in_ref.at[ahead, piece],
                      pair_send.at[index], pair_recv.at[index], partner)
        copy.start()
        pairs[ahead, piece] = copy

    def chip_sum(ahead, piece):
        pairs[ahead, piece].wait_recv()
        return part_ref[slots[ahead], piece] + pair_in_ref[ahead, piece].astype(F32)

    def pass_on(ahead, piece, place, target, merge=False):
        value = chip_sum(ahead, piece)
        if merge:
            halves[piece].wait_recv()
            value = value + half_ref[piece].astype(F32)
        ring_out_ref[ahead - 1, piece] = value.astype(BF16)
        index = len(rings)
        copy = remote(ring_out_ref.at[ahead - 1, piece], target, ring_send.at[index],
                      ring_recv.at[index], place)
        copy.start()
        rings.append(copy)
        return copy

    up, down = device_at(tp=2), device_at(tp=-2)

    def far(piece):
        halves[piece] = pass_on(2, piece, down if piece % 2 else up, half_ref.at[piece])

    def near(ahead, piece, merge=False):
        side = 0 if ahead == 1 else 1
        finals[side, piece] = pass_on(ahead, piece, down if side else up,
                                      final_ref.at[side, piece], merge)

    finish_rows(2)
    produce(2, 0)
    produce(2, 1)
    far(0)
    far(1)
    out.fifth()
    finish_rows(1)
    finish_rows(3)
    produce(1, 1)
    produce(3, 0)
    near(1, 1)
    near(3, 0)
    for dz, dx in ORDER[9:]:
        out.last(dz, dx)
    produce(2, 2)
    produce(2, 3)
    far(2)
    far(3)
    produce(1, 3)
    produce(3, 2)
    near(1, 3)
    near(3, 2)
    for piece in (0, 2):
        produce(1, piece)
        produce(3, piece + 1)
    finish_rows(0)
    for piece in range(4):
        produce(0, piece)
    for piece in (0, 2):
        near(1, piece, merge=True)
        near(3, piece + 1, merge=True)
    for piece in range(4):
        part_ref[0, piece] = chip_sum(0, piece)
    arrived = set()
    for key in ((0, 1), (1, 0), (0, 3), (1, 2), (0, 0), (1, 1), (0, 2), (1, 3)):
        side, piece = key
        finals[key].wait_recv()
        value = part_ref[0, piece] + final_ref[side, piece].astype(F32)
        if (1 - side, piece) not in arrived:
            part_ref[0, piece] = value
        else:
            for block, (dz, dx) in enumerate(ORDER[4 * piece : 4 * piece + 4]):
                lanes = pl.ds(pl.multiple_of(out.shard(dz, dx) * 256, 256), 256)
                out_ref[:, lanes] = value[:, block * 256 : block * 256 + 256].astype(BF16)
        arrived.add(key)
    for copy in along_x + along_z + list(pairs.values()) + rings:
        copy.wait_send()
    for gather in (early, pool, out):
        gather.drain()


def per_device(tokens, input_norm_scale, mean_input_weight, query_matrix, key_matrix, value_matrix,
               strength_weight, decay_input_weight, causal_filter_weight, head_decay_logrates,
               decay_input_shift, strength_shift, decay_spike, head_norm_scale,
               group_mixing_weight, mean_channel_scale, mean_output_weight, delta_output_weight):
    tok_rows, depth = tokens.shape
    heads = strength_weight.shape[1]
    n_z, n_x = lax.axis_size("sp_0"), lax.axis_size("sp_1")
    chunks = tok_rows // CHUNK
    pairs = heads * chunks
    width = n_z * n_x * 256
    pieces = width // PIECE
    vmem = pl.BlockSpec(memory_space=pltpu.VMEM)
    smem = pl.BlockSpec(memory_space=pltpu.SMEM)
    hbm = pl.BlockSpec(memory_space=pl.ANY)
    dma = pltpu.SemaphoreType.DMA
    return pl.pallas_call(
        lambda *refs: layer_kernel(heads, *refs),
        out_shape=jax.ShapeDtypeStruct((128, width), BF16),
        in_specs=[hbm] * 9 + [vmem] * 6 + [smem] * 3,
        out_specs=vmem,
        scratch_shapes=[
            pltpu.VMEM((tok_rows + HALO, depth), BF16),
            pltpu.VMEM((16, 272, 768), BF16),
            pltpu.VMEM((16, 256, 256), BF16),
            pltpu.VMEM((16, 512, 256), BF16),
            pltpu.VMEM((tok_rows + HALO, 768), F32),
            pltpu.VMEM((tok_rows + HALO, 256), F32),
            pltpu.VMEM((tok_rows + HALO, 16), F32),
            pltpu.VMEM((8, depth), F32),
            pltpu.VMEM((3, CONV, 256), BF16),
            pltpu.VMEM((3, CONV, 256), F32),
            pltpu.VMEM((2, 128, 128), BF16),
            pltpu.VMEM((pairs, 8, CHUNK), F32),
            pltpu.VMEM((pairs, CHUNK, 128), F32),
            pltpu.VMEM((pairs, CHUNK, 128), F32),
            pltpu.VMEM((8, CHUNK, CHUNK), BF16),
            pltpu.VMEM((heads, 128, 256), F32),
            pltpu.VMEM((heads, tok_rows, 128), BF16),
            pltpu.VMEM((heads, tok_rows, 128), F32),
            pltpu.VMEM((heads, 128, 256), BF16),
            pltpu.VMEM((n_x, heads, 128, 256), BF16),
            pltpu.VMEM((heads, 128, 256), BF16),
            pltpu.VMEM((n_z, heads, 128, 256), BF16),
            pltpu.VMEM((heads, 128, 128), BF16),
            pltpu.VMEM((chunks, CHUNK, 512), BF16),
            pltpu.VMEM((3, pieces, 128, PIECE), F32),
            pltpu.VMEM((4, pieces, 128, PIECE), BF16),
            pltpu.VMEM((4, pieces, 128, PIECE), BF16),
            pltpu.VMEM((3, pieces, 128, PIECE), BF16),
            pltpu.VMEM((pieces, 128, PIECE), BF16),
            pltpu.VMEM((2, pieces, 128, PIECE), BF16),
            dma((chunks,)), dma((8,)), dma((8,)), dma((8,)),
            dma((32,)), dma((32,)), dma((32,)), dma((32,)), dma((32,)), dma((32,)),
            dma((n_x,)), dma((n_x,)), dma((n_z,)), dma((n_z,)),
            dma((16,)), dma((16,)), dma((12,)), dma((12,)),
        ],
        compiler_params=pltpu.CompilerParams(
            vmem_limit_bytes=VMEM_LIMIT, collective_id=0, has_side_effects=True),
        name="layer",
    )(tokens, mean_input_weight, query_matrix, key_matrix, value_matrix, mean_output_weight,
      delta_output_weight, jnp.transpose(causal_filter_weight, (1, 0, 2)), group_mixing_weight,
      input_norm_scale.reshape(-1, 128), head_norm_scale.reshape(1, HEAD_DIM),
      mean_channel_scale.reshape(-1, 128), strength_weight.T, decay_input_weight.T, decay_spike.T,
      head_decay_logrates, decay_input_shift, strength_shift)


def solution(mesh):
    finer = Mesh(mesh.devices.reshape(4, 4, mesh.shape["tp"]), SP_TP)
    in_specs = (
        P(SP, None), P(), P(SP, "tp"), P(SP, "tp"), P(SP, "tp"), P(SP, "tp"), P(SP, "tp"),
        P(SP, "tp"), P(), P(), P(), P(), P(SP, "tp"), P(), P(), P(), P("tp", SP), P("tp", SP),
    )
    return jax.shard_map(
        per_device, mesh=finer, in_specs=in_specs, out_specs=P(SP_TP, None), check_vma=False
    )
```

```python
import jax
import jax.numpy as jnp
from jax import lax
from jax.experimental import pallas as pl
from jax.experimental.pallas import tpu as pltpu
from jax.sharding import Mesh
from jax.sharding import PartitionSpec as P

HEAD_DIM = 128
CONV = 4
CHUNK = 256
HALO = 16
EPSILON = 1e-06
SP = ("sp_0", "sp_1")
SP_TP = ("sp_0", "sp_1", "tp")
MESH_ID = pl.DeviceIdType.MESH
F32 = jnp.float32
BF16 = jnp.bfloat16
VMEM_LIMIT = 63 * 1000 * 1000


def dot(a, b):
    return jnp.dot(a, b, preferred_element_type=F32)


def dot_nt(a, b):
    return lax.dot_general(a, b, (((1,), (1,)), ((), ())), preferred_element_type=F32)


def dot_tn(a, b):
    return lax.dot_general(a, b, (((0,), (0,)), ((), ())), preferred_element_type=F32)


def unit_rows(values):
    return values * lax.rsqrt(jnp.sum(values * values, axis=-1, keepdims=True) + EPSILON)


def fill_masks(masks_ref):
    rows = lax.broadcasted_iota(jnp.int32, (CHUNK, CHUNK), 0)
    cols = lax.broadcasted_iota(jnp.int32, (CHUNK, CHUNK), 1)
    apart = jnp.bitwise_xor(rows, cols)
    for level in range(masks_ref.shape[0]):
        inside = (rows > cols) & (apart >= 2**level) & (apart < 2 ** (level + 1))
        masks_ref[level] = jnp.where(inside, 1.0, 0.0).astype(BF16)


def conv_rows(raw_ref, taps_ref, head, start, part):
    lanes = slice(part * 128, part * 128 + 128)
    tap_lanes = slice(head * 128, head * 128 + 128)
    rows = raw_ref[head, start + HALO - 8 : start + HALO + CHUNK, lanes]
    mixed = taps_ref[part, CONV - 1 : CONV, tap_lanes] * rows[8:]
    for back in range(1, CONV):
        tap = taps_ref[part, CONV - 1 - back : CONV - back, tap_lanes]
        mixed = mixed + tap * pltpu.roll(rows, back, 0)[8:]
    return mixed / (1.0 + jnp.exp(-mixed))


def delta_head(head, chunks, raw_ref, taps_ref, grow_ref, gcol_ref, bcol_ref, masks_ref, map_ref,
               from_state_ref, local_ref, events):
    rows = lax.broadcasted_iota(jnp.int32, (CHUNK, CHUNK), 0)
    cols = lax.broadcasted_iota(jnp.int32, (CHUNK, CHUNK), 1)
    work = []
    for chunk in range(chunks):
        row = head * chunks + chunk
        start = chunk * CHUNK
        query = unit_rows(conv_rows(raw_ref, taps_ref, head, start, 0)) * HEAD_DIM ** (-0.5)
        key = unit_rows(conv_rows(raw_ref, taps_ref, head, start, 1))
        value = conv_rows(raw_ref, taps_ref, head, start, 2)
        gcol, bcol, grow = gcol_ref[row], bcol_ref[row], grow_ref[row][0:1]
        key_b = key.astype(BF16)
        both = jnp.concatenate([query.astype(BF16), key_b], axis=0)
        inner = dot_nt(both, key_b)
        spread = jnp.exp(jnp.minimum(jnp.concatenate([gcol, gcol], axis=1) - grow, 0.0))
        scores = jnp.where(rows >= cols, inner[:CHUNK] * spread, 0.0).astype(BF16)
        strict = jnp.where(rows > cols, inner[CHUNK:] * spread, 0.0)
        strict = (strict * jnp.concatenate([bcol, bcol], axis=1)).astype(BF16)
        grown = jnp.exp(gcol)
        right = jnp.concatenate([value * bcol, key * bcol * grown], axis=1).astype(BF16)
        last = grow[:, CHUNK - 1 : CHUNK]
        key_dec = (key * jnp.exp(last - gcol)).astype(BF16)
        inverse = jnp.where(rows == cols, 1.0, 0.0).astype(BF16) - strict * masks_ref[0]
        work.append([strict, inverse, scores, right, key_dec, query * grown, jnp.exp(last)])
        events.get(("chunk", chunk), lambda: None)()
    for level in range(1, masks_ref.shape[0]):
        inner = [dot(w[0] * masks_ref[level], w[1]).astype(BF16) for w in work]
        for w, part in zip(work, inner):
            w[1] = w[1] - dot(w[1], part).astype(BF16)
        events.get(("level", level), lambda: None)()
    solved = [dot(w[1], w[3]).astype(BF16) for w in work]
    seen = [dot(w[2], s) for w, s in zip(work, solved)]
    moved = [dot_tn(w[4], s) for w, s in zip(work, solved)]
    current = map_ref[head]
    for chunk in range(chunks):
        where_rows = slice(chunk * CHUNK, chunk * CHUNK + CHUNK)
        current_b = current.astype(BF16)
        asked = (work[chunk][5] - seen[chunk][:, 128:]).astype(BF16)
        answer = dot(asked, current_b)
        from_state_ref[head, where_rows, :] = answer[:, :128].astype(BF16)
        local_ref[head, where_rows, :] = answer[:, 128:] + seen[chunk][:, :128]
        added = jnp.concatenate([jnp.zeros((128, 128), F32), moved[chunk][:, :128]], axis=1)
        current = (current * work[chunk][6] - dot(moved[chunk][:, 128:].astype(BF16), current_b)
                   + added)
    map_ref[head] = current


SPLIT_A = 128
PIECE = 1024
ORDER = ((0, 0), (0, 1), (0, -1), (1, 0), (-1, 0), (1, 1), (1, -1), (-1, 1), (-1, -1), (0, 2), (2, 0),
         (1, 2), (-1, 2), (2, 1), (2, -1), (2, 2))


class PlaneGather:
    def __init__(self, buf, split, send_sems, recv_sems):
        self.buf, self.split = buf, split
        self.send_sems, self.recv_sems = send_sems, recv_sems
        self.z, self.x = lax.axis_index("sp_0"), lax.axis_index("sp_1")
        self.copies = {}

    def shard(self, dz, dx):
        return lax.rem(self.z + dz + 4, 4) * 4 + lax.rem(self.x + dx + 4, 4)

    def rows(self, part):
        split, total = self.split, self.buf.shape[1]
        quarter = split // 32 * 16
        rest = split + (total - split) // 32 * 16
        return {"a": (0, split), "b": (split, total), "a0": (0, quarter), "a1": (quarter, split),
                "b0": (split, rest), "b1": (rest, total)}[part]

    def region(self, dz, dx, part):
        low, high = self.rows(part)
        return self.buf.at[self.shard(dz, dx), pl.ds(low, high - low), :]

    def copy(self, name, way, source):
        index, _, part = self.copies[name, way]
        ref = self.region(source[0], source[1], part)
        return remote(ref, ref, self.send_sems.at[index], self.recv_sems.at[index],
                      {"sp_0": lax.rem(self.z + way[0] + 4, 4),
                       "sp_1": lax.rem(self.x + way[1] + 4, 4)})

    def send(self, name, source, part, way):
        self.copies[name, way] = (len(self.copies), source, part)
        self.copy(name, way, source).start()

    def got(self, name, way):
        source = self.copies[name, way][1]
        self.copy(name, way, (source[0] - way[0], source[1] - way[1])).wait_recv()

    def own(self, along="xz"):
        for part in range(2):
            for step in (1, -1):
                if "x" in along:
                    self.send("ab"[part], (0, 0), "ab"[part], (0, step))
                if "z" in along:
                    self.send("ba"[part], (0, 0), "ba"[part], (step, 0))

    def first(self):
        for step in (1, -1):
            self.got("a", (0, step))
            self.got("b", (step, 0))
        self.send("a2", (0, -1), "a0", (0, 1))
        self.send("a2", (0, 1), "a1", (0, -1))
        self.send("b2", (-1, 0), "b0", (1, 0))
        self.send("b2", (1, 0), "b1", (-1, 0))
        for at in (1, -1):
            for step in (1, -1):
                self.send(("a3", at), (0, at), "a", (step, 0))
                self.send(("b3", at), (at, 0), "b", (0, step))

    def second(self):
        for step in (1, -1):
            self.got("b", (0, step))
            self.got("a", (step, 0))
        self.send(("a4", 0), (-1, 0), "a", (1, 0))
        self.send(("b4", 0), (0, -1), "b", (0, 1))

    def third(self, along="xz"):
        for step in (1, -1):
            self.got("a2", (0, step)) if "z" in along else None
            self.got("b2", (step, 0)) if "x" in along else None
        for step in (-1, 1):
            if "z" in along:
                self.send(("a3", 2), (0, 2), "a", (step, 0))
            if "x" in along:
                self.send(("b3", 2), (2, 0), "b", (0, step))

    def fourth(self):
        for at in (1, -1):
            for step in (1, -1):
                self.got(("a3", at), (step, 0))
                self.got(("b3", at), (0, step))
        for at in (1, -1):
            self.send(("a4", at), (-at, at), "a", (at, 0))
            self.send(("b4", at), (at, -at), "b", (0, at))

    def fifth(self):
        for step in (1, -1):
            self.got(("a3", 2), (step, 0))
            self.got(("b3", 2), (0, step))
        self.send(("a4", 2), (1, 2), "a", (-1, 0))
        self.send(("b4", 2), (2, 1), "b", (0, -1))

    def last(self, dz, dx):
        side = {0: 1, 1: 1, -1: -1, 2: -1}
        if dz == 2:
            self.got(("a4", dx), (side[dx], 0))
        if dx == 2:
            self.got(("b4", dz), (0, side[dz]))

    def drain(self):
        for (name, way), (_, source, _) in self.copies.items():
            self.copy(name, way, source).wait_send()


def after(later, earlier):
    offset = jnp.concatenate([jnp.zeros((128, 128), F32), later[:, 128:].astype(F32)], axis=1)
    return dot(later[:, :128], earlier.astype(BF16)) + offset


def device_at(z=0, x=0, tp=0):
    place = {}
    for name, step in (("sp_0", z), ("sp_1", x), ("tp", tp)):
        if step:
            size = lax.axis_size(name)
            place[name] = lax.rem(lax.axis_index(name) + step + size, size)
    return place


def remote(src, dst, send_sem, recv_sem, place):
    return pltpu.make_async_remote_copy(
        src_ref=src, dst_ref=dst, send_sem=send_sem, recv_sem=recv_sem, device_id=place,
        device_id_type=MESH_ID)


def pooled_rows(pool_ref, chunk, position, wide, mix_ref, scales):
    parts = []
    for group in range(2):
        lanes = slice(group * 128, group * 128 + 128)
        rows = pool_ref[pl.ds(pl.multiple_of(chunk * CHUNK, CHUNK), CHUNK + HALO), lanes]
        reach = 1
        sums = rows
        for _ in range(group + 1):
            sums = sums + pltpu.roll(sums, reach, 0)
            reach *= 2
        broad = sums
        for _ in range(2):
            broad = broad + pltpu.roll(broad, reach, 0)
            reach *= 2
        short, long = 2 << group, 8 << group
        seen = lax.broadcasted_iota(jnp.int32, (CHUNK, 128), 0) + (position + chunk * CHUNK + 1)
        count = jnp.minimum(seen, jnp.where(wide, long, short)).astype(F32)
        window = jnp.where(wide, broad[HALO:], sums[HALO:])
        diff = (window / count - rows[HALO:]).astype(BF16)
        parts.append((dot(diff, mix_ref[group]) * scales[group]).astype(BF16))
    return parts


def norm_rows(tok_ref, gain_ref, start, count, step_rows):
    @pl.loop(0, count // step_rows)
    def _(step):
        rows = pl.ds(pl.multiple_of(start + step * step_rows, 16), step_rows)
        values = tok_ref[rows, :].astype(F32)
        scale = lax.rsqrt(jnp.mean(values * values, axis=-1, keepdims=True) + EPSILON)
        tok_ref[rows, :] = (tok_ref[rows, :].astype(F32) * scale * gain_ref[0:1, :]).astype(BF16)


def layer_kernel(heads, tok_hbm, pool_hbm, query_hbm, key_hbm, value_hbm, pool_out_hbm,
                 delta_out_hbm, taps_hbm, mix_hbm, gain_in_ref, head_gain_ref, scale_in_ref,
                 strength_ref, decay_ref, spike_ref, rate_ref, decay_shift_ref, strength_shift_ref,
                 out_ref,
                 tok_ref, wide_ref, next_ref, pool_w_ref, out_w_ref, acc_ref, pool_ref, thin_ref, gain_ref,
                 taps_in_ref, taps_ref, mix_ref, grow_ref, gcol_ref, bcol_ref, masks_ref, map_ref,
                 from_state_ref, local_ref, own_ref, row_ref, total_ref, column_ref, state_ref,
                 mixed_ref, part_ref, pair_out_ref, pair_in_ref, ring_out_ref, half_ref, final_ref,
                 tok_sems, load_sems, halo_send, halo_recv, send_a, recv_a, send_d, recv_d, send_b, recv_b,
                 send_c, recv_c, send_x, recv_x, send_z, recv_z, pair_send, pair_recv, ring_send,
                 ring_recv):
    z, x, tp = lax.axis_index("sp_0"), lax.axis_index("sp_1"), lax.axis_index("tp")
    n_z, n_x, n_tp = lax.axis_size("sp_0"), lax.axis_size("sp_1"), lax.axis_size("tp")
    y, core = tp // 2, lax.rem(tp, 2)
    n_y = n_tp // 2
    tok_rows, depth = tok_hbm.shape
    chunks = tok_rows // CHUNK
    mine = z * n_x + x
    position = mine * tok_rows
    loads = []
    for k, (hbm, ref) in enumerate((
            (query_hbm.at[:, pl.ds(0, 128)], wide_ref.at[mine, pl.ds(0, 256), pl.ds(0, 128)]),
            (key_hbm.at[:, pl.ds(0, 128)], wide_ref.at[mine, pl.ds(0, 256), pl.ds(128, 128)]),
            (value_hbm.at[:, pl.ds(0, 128)], wide_ref.at[mine, pl.ds(0, 256), pl.ds(256, 128)]),
            (query_hbm.at[:, pl.ds(128, 128)], next_ref.at[mine, :, pl.ds(0, 128)]),
            (key_hbm.at[:, pl.ds(128, 128)], next_ref.at[mine, :, pl.ds(128, 128)]),
            (value_hbm.at[:, pl.ds(128, 128)], next_ref.at[mine, :, pl.ds(256, 128)]),
            (pool_hbm, pool_w_ref.at[mine]),
            (pool_out_hbm, out_w_ref.at[mine, pl.ds(0, 256), :]),
            (delta_out_hbm, out_w_ref.at[mine, pl.ds(256, 256), :]),
            (taps_hbm.at[:, :, pl.ds(pl.multiple_of(tp * 256, 256), 256)], taps_in_ref),
            (mix_hbm.at[pl.ds(tp * 2, 2)], mix_ref))):
        load = pltpu.make_async_copy(hbm, ref, load_sems.at[k])
        load.start()
        loads.append(load)
    tok_loads = []
    for k in range(chunks):
        load = pltpu.make_async_copy(
            tok_hbm.at[pl.ds(k * CHUNK, CHUNK), :],
            tok_ref.at[pl.ds(HALO + k * CHUNK, CHUNK), :], tok_sems.at[k])
        load.start()
        tok_loads.append(load)
    following, before = lax.rem(mine + 1, 16), lax.rem(mine + 15, 16)
    next_place = {"sp_0": following // 4, "sp_1": lax.rem(following, 4)}
    last_place = {"sp_0": before // 4, "sp_1": lax.rem(before, 4)}
    peers = [device_at(x=step) for step in range(1, n_x)]
    peers += [device_at(z=step) for step in range(1, n_z)]
    peers += [device_at(tp=step) for step in range(1, n_tp)]
    peers += [next_place, last_place]
    barrier = pltpu.get_barrier_semaphore()
    for peer in peers:
        pl.semaphore_signal(barrier, 1, device_id=peer, device_id_type=MESH_ID)
    at = lax.broadcasted_iota(jnp.int32, (16, 256), 0)
    thin = jnp.zeros((16, 256), F32)
    for k, (ref, row) in enumerate(((strength_ref, 0), (strength_ref, 1), (decay_ref, 0),
                                    (decay_ref, 1))):
        row_values = ref[...].astype(F32)[row : row + 1]
        thin = jnp.where(at == k, jnp.broadcast_to(row_values, (16, 256)), thin)
    wide_ref[mine, 256:272, 0:256] = thin.astype(BF16)
    wide_ref[mine, 256:272, 256:384] = jnp.zeros((16, 128), BF16)
    gains = gain_in_ref[...].astype(F32)
    for k in range(depth // 128):
        gain_ref[:, k * 128 : k * 128 + 128] = jnp.broadcast_to(gains[k : k + 1], (8, 128))
    fill_masks(masks_ref)
    for load in loads[:3]:
        load.wait()
    pl.semaphore_wait(barrier, len(peers))

    early = PlaneGather(wide_ref, SPLIT_A, send_a, recv_a)
    slices = depth // n_tp

    def halo_part(owner):
        return tok_ref.at[pl.ds(0, HALO), pl.ds(pl.multiple_of(owner * slices, 128), slices)]

    halos = [remote(
        tok_hbm.at[pl.ds(tok_rows - HALO, HALO), pl.ds(pl.multiple_of(tp * slices, 128), slices)],
        halo_part(tp), halo_send.at[0], halo_recv.at[0], next_place)]
    halos[0].start()
    early.own()
    for k in range(chunks):
        tok_loads[k].wait()
        norm_rows(tok_ref, gain_ref, HALO + k * CHUNK, CHUNK, 64)
        if k == 1:
            halos[0].wait_recv()
            for step in range(1, n_tp):
                copy = remote(halo_part(tp), halo_part(tp), halo_send.at[step],
                              halo_recv.at[step], device_at(tp=step))
                copy.start()
                halos.append(copy)
    for step in range(1, n_tp):
        owner = lax.rem(tp - step + n_tp, n_tp)
        remote(halo_part(owner), halo_part(owner), halo_send.at[step], halo_recv.at[step],
               device_at(tp=step)).wait_recv()
    for copy in halos:
        copy.wait_send()

    @pl.when(mine == 0)
    def _():
        tok_ref[0:HALO, :] = jnp.zeros((HALO, depth), BF16)

    norm_rows(tok_ref, gain_ref, 0, HALO, HALO)
    tile = 208

    def project(gather, places, into, first=False):
        @pl.loop(0, tok_ref.shape[0] // tile)
        def _(step):
            rows = pl.ds(pl.multiple_of(step * tile, 16), tile)
            total = None if first else into[rows, :]
            narrow = None if first or gather is not early else thin_ref[rows, :]
            for dz, dx in places:
                shard = gather.shard(dz, dx)
                normed = tok_ref[rows, pl.ds(pl.multiple_of(shard * 256, 256), 256)]
                term = dot(normed, gather.buf[shard, 0:256, :])
                total = term if total is None else total + term
                if gather is early:
                    term = dot_nt(normed, gather.buf[shard, 256:272, 0:256])
                    narrow = term if narrow is None else narrow + term
            into[rows, :] = total
            if gather is early:
                thin_ref[rows, :] = narrow

    first_acc, second_acc = acc_ref.at[0], acc_ref.at[1]
    early.first()
    project(early, ORDER[:1], first_acc, first=True)
    early.second()
    project(early, ORDER[1:5], first_acc)
    early.third()
    for load in loads[3:]:
        load.wait()
    early.fourth()
    later = PlaneGather(next_ref, SPLIT_A, send_d, recv_d)
    later.own()
    project(early, ORDER[5:9], first_acc)
    early.fifth()
    for dz, dx in ORDER[9:13]:
        early.last(dz, dx)
    project(early, ORDER[9:13], first_acc)
    later.first()
    for dz, dx in ORDER[13:]:
        early.last(dz, dx)
    project(early, ORDER[13:], first_acc)
    later.second()

    taps_ref[...] = taps_in_ref[...].astype(F32)
    narrow = thin_ref[HALO:, :].T
    for head in range(heads):
        strength = narrow[head : head + 1] + strength_shift_ref[tp * heads + head]
        beta = 1.0 / (1.0 + jnp.exp(-strength))
        level = narrow[heads + head : heads + head + 1] + decay_shift_ref[tp * heads + head]
        soft = jnp.maximum(level, 0.0) + jnp.log1p(jnp.exp(-jnp.abs(level)))
        rate = jnp.exp(jnp.full((1, tok_rows), rate_ref[tp * heads + head], F32))
        decay = spike_ref[head : head + 1, :] - rate * soft
        lane = lax.rem(lax.broadcasted_iota(jnp.int32, (8, tok_rows), 1), CHUNK)
        summed = jnp.broadcast_to(decay, (8, tok_rows))
        step = 1
        while step < CHUNK:
            summed = summed + jnp.where(lane >= step, pltpu.roll(summed, step, 1), 0.0)
            step *= 2
        for chunk in range(chunks):
            row = head * chunks + chunk
            part = slice(chunk * CHUNK, chunk * CHUNK + CHUNK)
            grow_ref[row] = summed[:, part]
            gcol_ref[row] = jnp.broadcast_to(summed[0:1, part], (128, CHUNK)).T
            bcol_ref[row] = jnp.broadcast_to(beta[:, part], (128, CHUNK)).T
    rows = lax.broadcasted_iota(jnp.int32, (128, 256), 0)
    cols = lax.broadcasted_iota(jnp.int32, (128, 256), 1)
    identity = jnp.where(rows == cols, 1.0, 0.0)
    for head in range(heads):
        map_ref[head] = identity

    pool = PlaneGather(pool_w_ref, 128, send_b, recv_b)
    out = PlaneGather(out_w_ref, 256, send_c, recv_c)
    along_x, along_z = {}, {}

    def delta(head, events):
        delta_head(head, chunks, acc_ref, taps_ref, grow_ref, gcol_ref, bcol_ref, masks_ref,
                   map_ref, from_state_ref, local_ref, events)

    def send_x_maps(head):
        own_ref[head] = map_ref[head].astype(BF16)
        row_ref[0, head] = own_ref[head]
        along_x[head] = [
            remote(own_ref.at[head], row_ref.at[step, head], send_x.at[head, step],
                   recv_x.at[head, step], device_at(x=step)) for step in range(1, n_x)]
        for copy in along_x[head]:
            copy.start()

    def send_z_maps(head):
        for copy in along_x[head]:
            copy.wait_recv()
        so_far = before_here = identity
        for k in range(n_x):
            piece = row_ref[lax.rem(x - k + n_x, n_x), head]
            so_far = piece.astype(F32) if k == 0 else after(piece, so_far)
            before_here = jnp.where(k < x, so_far, before_here)
        map_ref[head] = before_here
        total_ref[head] = so_far.astype(BF16)
        column_ref[0, head] = total_ref[head]
        along_z[head] = [
            remote(total_ref.at[head], column_ref.at[step, head], send_z.at[head, step],
                   recv_z.at[head, step], device_at(z=step)) for step in range(1, n_z)]
        for copy in along_z[head]:
            copy.start()

    def enter(head):
        for copy in along_z[head]:
            copy.wait_recv()
        so_far = state = jnp.zeros((128, 128), F32)
        for k in range(n_z - 1):
            piece = column_ref[lax.rem(z - k + n_z, n_z), head]
            offset = piece[:, 128:].astype(F32)
            so_far = offset if k == 0 else dot(piece[:, :128], so_far.astype(BF16)) + offset
            state = jnp.where(k < z, so_far, state)
        entering = dot(map_ref[head, :, 0:128].astype(BF16), state.astype(BF16))
        state_ref[head] = (entering + map_ref[head, :, 128:256]).astype(BF16)

    delta(0, {("chunk", 3): later.third, ("level", 3): later.fourth})
    later.fifth()
    pool.own()
    send_x_maps(0)
    project(later, ORDER[:5], second_acc, first=True)
    project(later, ORDER[5:9], second_acc)
    for places in (ORDER[9:13], ORDER[13:]):
        for dz, dx in places:
            later.last(dz, dx)
        project(later, places, second_acc)

    def pool_early():
        pool.first()
        pool.second()

    def pool_middle():
        pool.third()
        pool.fourth()

    pool_early()
    delta(1, {("chunk", 1): lambda: send_z_maps(0), ("chunk", 3): pool_middle,
              ("level", 4): pool.fifth})
    send_x_maps(1)
    out.own("x")
    enter(0)
    wide = core == 1
    scales_at = lax.broadcasted_iota(jnp.int32, scale_in_ref.shape, 0)
    scales = [jnp.sum(jnp.where(scales_at == tp * 2 + group, scale_in_ref[...].astype(F32), 0.0),
                      axis=0, keepdims=True) for group in range(2)]

    def store_halves(chunk, lanes, values):
        for half in range(2):
            slot = lax.rem(half + core, 2)
            mixed_ref[chunk, pl.ds(pl.multiple_of(slot * 128, 128), 128), lanes] = (
                values[half * 128 : half * 128 + 128])

    project(pool, ORDER[:8], pool_ref, first=True)
    send_z_maps(1)
    out.own("z")
    for dz, dx in ORDER[9:]:
        pool.last(dz, dx)
    project(pool, ORDER[8:], pool_ref)
    out.first()

    @pl.loop(0, chunks)
    def _(chunk):
        for group, values in enumerate(
                pooled_rows(pool_ref, chunk, position, wide, mix_ref, scales)):
            store_halves(chunk, slice(group * 128, group * 128 + 128), values)

    enter(1)
    out.second()

    head_gain = head_gain_ref[...].astype(F32)
    partner = {"tp": y * 2 + (1 - core)}
    pairs, rings, finals, halves = {}, [], {}, {}
    slots = {2: 0, 1: 1, 3: 2, 0: 0}

    def finish_rows(ahead):
        chunk = lax.rem(y + ahead, n_y)
        where_rows = pl.ds(pl.multiple_of(chunk * CHUNK, CHUNK), CHUNK)
        for head in range(heads):
            raw = dot(from_state_ref[head, where_rows, :], state_ref[head])
            raw = raw + local_ref[head, where_rows, :]
            squares = jnp.mean(raw * raw, axis=-1, keepdims=True)
            normed = (raw * lax.rsqrt(squares + EPSILON) * head_gain).astype(BF16)
            store_halves(chunk, slice(256 + head * 128, 384 + head * 128), normed)

    def produce(ahead, piece):
        chunk = lax.rem(y + ahead, n_y)
        for block, (dz, dx) in enumerate(ORDER[4 * piece : 4 * piece + 4]):
            lanes = slice(block * 256, block * 256 + 256)
            product = dot(mixed_ref[chunk], out_w_ref[out.shard(dz, dx)])
            part_ref[slots[ahead], piece, :, lanes] = product[:128]
            pair_out_ref[ahead, piece, :, lanes] = product[128:].astype(BF16)
        index = ahead * 4 + piece
        copy = remote(pair_out_ref.at[ahead, piece], pair_in_ref.at[ahead, piece],
                      pair_send.at[index], pair_recv.at[index], partner)
        copy.start()
        pairs[ahead, piece] = copy

    def chip_sum(ahead, piece):
        pairs[ahead, piece].wait_recv()
        return part_ref[slots[ahead], piece] + pair_in_ref[ahead, piece].astype(F32)

    def pass_on(ahead, piece, place, target, merge=False):
        value = chip_sum(ahead, piece)
        if merge:
            halves[piece].wait_recv()
            value = value + half_ref[piece].astype(F32)
        ring_out_ref[ahead - 1, piece] = value.astype(BF16)
        index = len(rings)
        copy = remote(ring_out_ref.at[ahead - 1, piece], target, ring_send.at[index],
                      ring_recv.at[index], place)
        copy.start()
        rings.append(copy)
        return copy

    up, down = device_at(tp=2), device_at(tp=-2)

    def far(piece):
        halves[piece] = pass_on(2, piece, down if piece % 2 else up, half_ref.at[piece])

    def near(ahead, piece, merge=False):
        side = 0 if ahead == 1 else 1
        finals[side, piece] = pass_on(ahead, piece, down if side else up,
                                      final_ref.at[side, piece], merge)

    finish_rows(2)
    produce(2, 0)
    far(0)
    out.third()
    finish_rows(1)
    finish_rows(3)
    out.fourth()
    produce(2, 1)
    far(1)
    produce(1, 1)
    produce(3, 0)
    near(1, 1)
    near(3, 0)
    out.fifth()
    produce(1, 0)
    produce(3, 1)
    early.drain()
    later.drain()
    near(1, 0, merge=True)
    near(3, 1, merge=True)
    for dz, dx in ORDER[9:]:
        out.last(dz, dx)
    for piece in (2, 3):
        produce(2, piece)
        far(piece)
    produce(1, 3)
    near(1, 3)
    produce(3, 2)
    near(3, 2)
    produce(1, 2)
    produce(3, 3)
    finish_rows(0)
    for piece in range(4):
        produce(0, piece)
    pool.drain()
    out.drain()
    near(1, 2, merge=True)
    near(3, 3, merge=True)
    for piece in range(4):
        part_ref[0, piece] = chip_sum(0, piece)
    for head in range(heads):
        for copy in along_x[head] + along_z[head]:
            copy.wait_send()
    for copy in pairs.values():
        copy.wait_send()
    for copy in rings[:8]:
        copy.wait_send()
    arrived = set()
    for key in ((0, 1), (1, 0), (0, 0), (1, 1), (0, 3), (1, 2), (0, 2), (1, 3)):
        side, piece = key
        finals[key].wait_recv()
        value = part_ref[0, piece] + final_ref[side, piece].astype(F32)
        if (1 - side, piece) not in arrived:
            part_ref[0, piece] = value
        else:
            for block, (dz, dx) in enumerate(ORDER[4 * piece : 4 * piece + 4]):
                lanes = pl.ds(pl.multiple_of(out.shard(dz, dx) * 256, 256), 256)
                out_ref[:, lanes] = value[:, block * 256 : block * 256 + 256].astype(BF16)
        arrived.add(key)
    for copy in rings[8:]:
        copy.wait_send()


def per_device(tokens, input_norm_scale, mean_input_weight, query_matrix, key_matrix, value_matrix,
               strength_weight, decay_input_weight, causal_filter_weight, head_decay_logrates,
               decay_input_shift, strength_shift, decay_spike, head_norm_scale,
               group_mixing_weight, mean_channel_scale, mean_output_weight, delta_output_weight):
    tok_rows, depth = tokens.shape
    heads = strength_weight.shape[1]
    n_z, n_x = lax.axis_size("sp_0"), lax.axis_size("sp_1")
    chunks = tok_rows // CHUNK
    pairs = heads * chunks
    width = n_z * n_x * 256
    pieces = width // PIECE
    vmem = pl.BlockSpec(memory_space=pltpu.VMEM)
    smem = pl.BlockSpec(memory_space=pltpu.SMEM)
    hbm = pl.BlockSpec(memory_space=pl.ANY)
    dma = pltpu.SemaphoreType.DMA
    return pl.pallas_call(
        lambda *refs: layer_kernel(heads, *refs),
        out_shape=jax.ShapeDtypeStruct((128, width), BF16),
        in_specs=[hbm] * 9 + [vmem] * 6 + [smem] * 3,
        out_specs=vmem,
        scratch_shapes=[
            pltpu.VMEM((tok_rows + HALO, depth), BF16),
            pltpu.VMEM((16, 272, 384), BF16),
            pltpu.VMEM((16, 256, 384), BF16),
            pltpu.VMEM((16, 256, 256), BF16),
            pltpu.VMEM((16, 512, 256), BF16),
            pltpu.VMEM((heads, tok_rows + HALO, 384), F32),
            pltpu.VMEM((tok_rows + HALO, 256), F32),
            pltpu.VMEM((tok_rows + HALO, 16), F32),
            pltpu.VMEM((8, depth), F32),
            pltpu.VMEM((3, CONV, 256), BF16),
            pltpu.VMEM((3, CONV, 256), F32),
            pltpu.VMEM((2, 128, 128), BF16),
            pltpu.VMEM((pairs, 8, CHUNK), F32),
            pltpu.VMEM((pairs, CHUNK, 128), F32),
            pltpu.VMEM((pairs, CHUNK, 128), F32),
            pltpu.VMEM((8, CHUNK, CHUNK), BF16),
            pltpu.VMEM((heads, 128, 256), F32),
            pltpu.VMEM((heads, tok_rows, 128), BF16),
            pltpu.VMEM((heads, tok_rows, 128), F32),
            pltpu.VMEM((heads, 128, 256), BF16),
            pltpu.VMEM((n_x, heads, 128, 256), BF16),
            pltpu.VMEM((heads, 128, 256), BF16),
            pltpu.VMEM((n_z, heads, 128, 256), BF16),
            pltpu.VMEM((heads, 128, 128), BF16),
            pltpu.VMEM((chunks, CHUNK, 512), BF16),
            pltpu.VMEM((3, pieces, 128, PIECE), F32),
            pltpu.VMEM((4, pieces, 128, PIECE), BF16),
            pltpu.VMEM((4, pieces, 128, PIECE), BF16),
            pltpu.VMEM((3, pieces, 128, PIECE), BF16),
            pltpu.VMEM((pieces, 128, PIECE), BF16),
            pltpu.VMEM((2, pieces, 128, PIECE), BF16),
            dma((chunks,)), dma((11,)), dma((8,)), dma((8,)),
            dma((32,)), dma((32,)), dma((32,)), dma((32,)), dma((32,)), dma((32,)), dma((32,)), dma((32,)),
            dma((heads, n_x)), dma((heads, n_x)), dma((heads, n_z)), dma((heads, n_z)),
            dma((16,)), dma((16,)), dma((12,)), dma((12,)),
        ],
        compiler_params=pltpu.CompilerParams(
            vmem_limit_bytes=VMEM_LIMIT, collective_id=0, has_side_effects=True),
        name="layer",
    )(tokens, mean_input_weight, query_matrix, key_matrix, value_matrix, mean_output_weight,
      delta_output_weight, jnp.transpose(causal_filter_weight, (1, 0, 2)), group_mixing_weight,
      input_norm_scale.reshape(-1, 128), head_norm_scale.reshape(1, HEAD_DIM),
      mean_channel_scale.reshape(-1, 128), strength_weight.T, decay_input_weight.T, decay_spike.T,
      head_decay_logrates, decay_input_shift, strength_shift)


def solution(mesh):
    finer = Mesh(mesh.devices.reshape(4, 4, mesh.shape["tp"]), SP_TP)
    in_specs = (
        P(SP, None), P(), P(SP, "tp"), P(SP, "tp"), P(SP, "tp"), P(SP, "tp"), P(SP, "tp"),
        P(SP, "tp"), P(), P(), P(), P(), P(SP, "tp"), P(), P(), P(), P("tp", SP), P("tp", SP),
    )
    return jax.shard_map(
        per_device, mesh=finer, in_specs=in_specs, out_specs=P(SP_TP, None), check_vma=False
    )
```

```python
import jax
import jax.numpy as jnp
from jax import lax
from jax.experimental import pallas as pl
from jax.experimental.pallas import tpu as pltpu
from jax.sharding import Mesh
from jax.sharding import PartitionSpec as P

HEAD_DIM = 128
CONV = 4
CHUNK = 256
HALO = 16
EPSILON = 1e-06
SP = ("sp_0", "sp_1")
SP_TP = ("sp_0", "sp_1", "tp")
MESH_ID = pl.DeviceIdType.MESH
F32 = jnp.float32
BF16 = jnp.bfloat16
VMEM_LIMIT = 63 * 1000 * 1000


def dot(a, b):
    return jnp.dot(a, b, preferred_element_type=F32)


def dot_nt(a, b):
    return lax.dot_general(a, b, (((1,), (1,)), ((), ())), preferred_element_type=F32)


def dot_tn(a, b):
    return lax.dot_general(a, b, (((0,), (0,)), ((), ())), preferred_element_type=F32)


def unit_rows(values):
    return values * lax.rsqrt(jnp.sum(values * values, axis=-1, keepdims=True) + EPSILON)


def fill_masks(masks_ref):
    rows = lax.broadcasted_iota(jnp.int32, (CHUNK, CHUNK), 0)
    cols = lax.broadcasted_iota(jnp.int32, (CHUNK, CHUNK), 1)
    apart = jnp.bitwise_xor(rows, cols)
    for level in range(masks_ref.shape[0]):
        inside = (rows > cols) & (apart >= 2**level) & (apart < 2 ** (level + 1))
        masks_ref[level] = jnp.where(inside, 1.0, 0.0).astype(BF16)


def conv_rows(raw_ref, taps_ref, head, start, part):
    lanes = slice(part * 128, part * 128 + 128)
    tap_lanes = slice(head * 128, head * 128 + 128)
    rows = raw_ref[head, start + HALO - 8 : start + HALO + CHUNK, lanes]
    mixed = taps_ref[part, CONV - 1 : CONV, tap_lanes] * rows[8:]
    for back in range(1, CONV):
        tap = taps_ref[part, CONV - 1 - back : CONV - back, tap_lanes]
        mixed = mixed + tap * pltpu.roll(rows, back, 0)[8:]
    return mixed / (1.0 + jnp.exp(-mixed))


def delta_head(head, chunks, raw_ref, taps_ref, grow_ref, gcol_ref, bcol_ref, masks_ref, map_ref,
               from_state_ref, local_ref, events):
    rows = lax.broadcasted_iota(jnp.int32, (CHUNK, CHUNK), 0)
    cols = lax.broadcasted_iota(jnp.int32, (CHUNK, CHUNK), 1)
    work = []
    for chunk in range(chunks):
        row = head * chunks + chunk
        start = chunk * CHUNK
        query = unit_rows(conv_rows(raw_ref, taps_ref, head, start, 0)) * HEAD_DIM ** (-0.5)
        key = unit_rows(conv_rows(raw_ref, taps_ref, head, start, 1))
        value = conv_rows(raw_ref, taps_ref, head, start, 2)
        gcol, bcol, grow = gcol_ref[row], bcol_ref[row], grow_ref[row][0:1]
        key_b = key.astype(BF16)
        both = jnp.concatenate([query.astype(BF16), key_b], axis=0)
        inner = dot_nt(both, key_b)
        spread = jnp.exp(jnp.minimum(jnp.concatenate([gcol, gcol], axis=1) - grow, 0.0))
        scores = jnp.where(rows >= cols, inner[:CHUNK] * spread, 0.0).astype(BF16)
        strict = jnp.where(rows > cols, inner[CHUNK:] * spread, 0.0)
        strict = (strict * jnp.concatenate([bcol, bcol], axis=1)).astype(BF16)
        grown = jnp.exp(gcol)
        right = jnp.concatenate([value * bcol, key * bcol * grown], axis=1).astype(BF16)
        last = grow[:, CHUNK - 1 : CHUNK]
        key_dec = (key * jnp.exp(last - gcol)).astype(BF16)
        inverse = jnp.where(rows == cols, 1.0, 0.0).astype(BF16) - strict * masks_ref[0]
        work.append([strict, inverse, scores, right, key_dec, query * grown, jnp.exp(last)])
        events.get(("chunk", chunk), lambda: None)()
    for level in range(1, masks_ref.shape[0]):
        inner = [dot(w[0] * masks_ref[level], w[1]).astype(BF16) for w in work]
        for w, part in zip(work, inner):
            w[1] = w[1] - dot(w[1], part).astype(BF16)
        events.get(("level", level), lambda: None)()
    solved = [dot(w[1], w[3]).astype(BF16) for w in work]
    moved = [dot_tn(w[4], s) for w, s in zip(work, solved)]
    current = map_ref[head]
    starts = []
    for chunk in range(chunks):
        current_b = current.astype(BF16)
        starts.append(current_b)
        added = jnp.concatenate([jnp.zeros((128, 128), F32), moved[chunk][:, :128]], axis=1)
        current = (current * work[chunk][6] - dot(moved[chunk][:, 128:].astype(BF16), current_b)
                   + added)
    map_ref[head] = current
    events.get(("maps", 0), lambda: None)()
    seen = [dot(w[2], s) for w, s in zip(work, solved)]
    for chunk in range(chunks):
        where_rows = slice(chunk * CHUNK, chunk * CHUNK + CHUNK)
        asked = (work[chunk][5] - seen[chunk][:, 128:]).astype(BF16)
        answer = dot(asked, starts[chunk])
        from_state_ref[head, where_rows, :] = answer[:, :128].astype(BF16)
        local_ref[head, where_rows, :] = answer[:, 128:] + seen[chunk][:, :128]


SPLIT_A = 128
PIECE = 1024
ORDER = ((0, 0), (0, 1), (0, -1), (1, 0), (-1, 0), (1, 1), (1, -1), (-1, 1), (-1, -1), (0, 2), (2, 0),
         (1, 2), (-1, 2), (2, 1), (2, -1), (2, 2))


class PlaneGather:
    def __init__(self, buf, split, send_sem, recv_sems):
        self.buf, self.split = buf, split
        self.send_sem, self.recv_sems = send_sem, recv_sems
        self.z, self.x = lax.axis_index("sp_0"), lax.axis_index("sp_1")

    def shard(self, dz, dx):
        return lax.rem(self.z + dz + 4, 4) * 4 + lax.rem(self.x + dx + 4, 4)

    def rows(self, part):
        split, total = self.split, self.buf.shape[1]
        quarter = split // 32 * 16
        rest = split + (total - split) // 32 * 16
        return {"a": (0, split), "b": (split, total), "a0": (0, quarter), "a1": (quarter, split),
                "b0": (split, rest), "b1": (rest, total)}[part]

    def send(self, group, source, part, way):
        low, high = self.rows(part)
        ref = self.buf.at[self.shard(*source), pl.ds(low, high - low), :]
        remote(ref, ref, self.send_sem, self.recv_sems.at[group],
               {"sp_0": lax.rem(self.z + way[0] + 4, 4),
                "sp_1": lax.rem(self.x + way[1] + 4, 4)}).start()

    def got(self, group, blocks):
        ref = self.buf.at[pl.ds(0, blocks)]
        pltpu.make_async_copy(ref, ref, self.recv_sems.at[group]).wait()

    def own(self, along="xz", parts=(0, 1)):
        for part in parts:
            for step in (1, -1):
                if "x" in along:
                    self.send(part, (0, 0), "ab"[part], (0, step))
                if "z" in along:
                    self.send(part, (0, 0), "ba"[part], (step, 0))

    def first(self):
        self.got(0, 2)
        self.send(2, (0, -1), "a0", (0, 1))
        self.send(2, (0, 1), "a1", (0, -1))
        self.send(2, (-1, 0), "b0", (1, 0))
        self.send(2, (1, 0), "b1", (-1, 0))
        for side, group in ((1, 3), (-1, 4)):
            for step in (1, -1):
                self.send(group, (0, side * step), "a", (step, 0))
                self.send(group, (side * step, 0), "b", (0, step))

    def second(self):
        self.got(1, 2)
        self.send(6, (-1, 0), "a", (1, 0))
        self.send(6, (0, -1), "b", (0, 1))

    def third(self):
        self.got(2, 1)
        for step, group in ((-1, 5), (1, 7)):
            self.send(group, (0, 2), "a", (step, 0))
            self.send(group, (2, 0), "b", (0, step))

    def fourth(self):
        self.got(3, 2)
        for at in (1, -1):
            self.send(7, (-at, at), "a", (at, 0))
            self.send(7, (at, -at), "b", (0, at))

    def corners(self):
        self.got(4, 2)

    def fifth(self):
        self.got(5, 1)
        self.send(7, (1, 2), "a", (-1, 0))
        self.send(7, (2, 1), "b", (0, -1))

    def straight(self):
        self.got(6, 1)

    def last(self):
        self.got(7, 4)

    def drain(self):
        ref = self.buf.at[pl.ds(0, 15)]
        pltpu.make_async_copy(ref, ref, self.send_sem).wait()


def after(later, earlier):
    offset = jnp.concatenate([jnp.zeros((128, 128), F32), later[:, 128:].astype(F32)], axis=1)
    return dot(later[:, :128], earlier.astype(BF16)) + offset


def device_at(z=0, x=0, tp=0):
    place = {}
    for name, step in (("sp_0", z), ("sp_1", x), ("tp", tp)):
        if step:
            size = lax.axis_size(name)
            place[name] = lax.rem(lax.axis_index(name) + step + size, size)
    return place


def remote(src, dst, send_sem, recv_sem, place):
    return pltpu.make_async_remote_copy(
        src_ref=src, dst_ref=dst, send_sem=send_sem, recv_sem=recv_sem, device_id=place,
        device_id_type=MESH_ID)


def pooled_rows(pool_ref, chunk, position, wide, mix_ref, scales):
    parts = []
    for group in range(2):
        lanes = slice(group * 128, group * 128 + 128)
        rows = pool_ref[pl.ds(pl.multiple_of(chunk * CHUNK, CHUNK), CHUNK + HALO), lanes]
        reach = 1
        sums = rows
        for _ in range(group + 1):
            sums = sums + pltpu.roll(sums, reach, 0)
            reach *= 2
        broad = sums
        for _ in range(2):
            broad = broad + pltpu.roll(broad, reach, 0)
            reach *= 2
        short, long = 2 << group, 8 << group
        seen = lax.broadcasted_iota(jnp.int32, (CHUNK, 128), 0) + (position + chunk * CHUNK + 1)
        count = jnp.minimum(seen, jnp.where(wide, long, short)).astype(F32)
        window = jnp.where(wide, broad[HALO:], sums[HALO:])
        diff = (window / count - rows[HALO:]).astype(BF16)
        parts.append((dot(diff, mix_ref[group]) * scales[group]).astype(BF16))
    return parts


def norm_rows(tok_ref, gain_ref, start, count, step_rows):
    @pl.loop(0, count // step_rows)
    def _(step):
        rows = pl.ds(pl.multiple_of(start + step * step_rows, 16), step_rows)
        values = tok_ref[rows, :].astype(F32)
        scale = lax.rsqrt(jnp.mean(values * values, axis=-1, keepdims=True) + EPSILON)
        tok_ref[rows, :] = (tok_ref[rows, :].astype(F32) * scale * gain_ref[0:1, :]).astype(BF16)


def layer_kernel(heads, tok_hbm, pool_hbm, query_hbm, key_hbm, value_hbm, pool_out_hbm,
                 delta_out_hbm, taps_hbm, mix_hbm, gain_in_ref, head_gain_ref, scale_in_ref,
                 strength_ref, decay_ref, spike_ref, rate_ref, decay_shift_ref, strength_shift_ref,
                 out_ref,
                 tok_ref, wide_ref, next_ref, pool_w_ref, out_w_ref, acc_ref, pool_ref, thin_ref, gain_ref,
                 taps_in_ref, taps_ref, mix_ref, grow_ref, gcol_ref, bcol_ref, masks_ref, map_ref,
                 from_state_ref, local_ref, own_ref, row_ref, total_ref, column_ref, state_ref,
                 mixed_ref, part_ref, pair_out_ref, pair_in_ref, ring_out_ref, half_ref, final_ref,
                 tok_sems, load_sems, halo_send, halo_recv, send_a, recv_a, send_d, recv_d, send_b, recv_b,
                 send_c, recv_c, send_x, recv_x, send_z, recv_z, pair_send, pair_recv, ring_send,
                 ring_recv, gate):
    z, x, tp = lax.axis_index("sp_0"), lax.axis_index("sp_1"), lax.axis_index("tp")
    n_z, n_x, n_tp = lax.axis_size("sp_0"), lax.axis_size("sp_1"), lax.axis_size("tp")
    y, core = tp // 2, lax.rem(tp, 2)
    n_y = n_tp // 2
    tok_rows, depth = tok_hbm.shape
    chunks = tok_rows // CHUNK
    mine = z * n_x + x
    position = mine * tok_rows
    loads = []
    for k, (hbm, ref) in enumerate((
            (query_hbm.at[:, pl.ds(0, 128)], wide_ref.at[mine, pl.ds(0, 256), pl.ds(0, 128)]),
            (key_hbm.at[:, pl.ds(0, 128)], wide_ref.at[mine, pl.ds(0, 256), pl.ds(128, 128)]),
            (value_hbm.at[:, pl.ds(0, 128)], wide_ref.at[mine, pl.ds(0, 256), pl.ds(256, 128)]),
            (query_hbm.at[:, pl.ds(128, 128)], next_ref.at[mine, :, pl.ds(0, 128)]),
            (key_hbm.at[:, pl.ds(128, 128)], next_ref.at[mine, :, pl.ds(128, 128)]),
            (value_hbm.at[:, pl.ds(128, 128)], next_ref.at[mine, :, pl.ds(256, 128)]),
            (pool_hbm, pool_w_ref.at[mine]),
            (pool_out_hbm, out_w_ref.at[mine, pl.ds(0, 256), :]),
            (delta_out_hbm, out_w_ref.at[mine, pl.ds(256, 256), :]),
            (taps_hbm.at[:, :, pl.ds(pl.multiple_of(tp * 256, 256), 256)], taps_in_ref),
            (mix_hbm.at[pl.ds(tp * 2, 2)], mix_ref))):
        load = pltpu.make_async_copy(hbm, ref, load_sems.at[max(k - 2, 0)])
        load.start()
        loads.append(load)
    own_block = wide_ref.at[mine, pl.ds(0, 256), :]
    tok_loads = []
    for k in range(chunks):
        load = pltpu.make_async_copy(
            tok_hbm.at[pl.ds(k * CHUNK, CHUNK), :],
            tok_ref.at[pl.ds(HALO + k * CHUNK, CHUNK), :], tok_sems.at[k])
        load.start()
        tok_loads.append(load)
    following, before = lax.rem(mine + 1, 16), lax.rem(mine + 15, 16)
    next_place = {"sp_0": following // 4, "sp_1": lax.rem(following, 4)}
    last_place = {"sp_0": before // 4, "sp_1": lax.rem(before, 4)}
    peers = [device_at(x=step) for step in range(1, n_x)]
    peers += [device_at(z=step) for step in range(1, n_z)]
    peers += [device_at(tp=step) for step in range(1, n_tp)]
    peers += [next_place, last_place]
    barrier = pltpu.get_barrier_semaphore()
    for peer in peers:
        pl.semaphore_signal(barrier, 1, device_id=peer, device_id_type=MESH_ID)
    at = lax.broadcasted_iota(jnp.int32, (16, 256), 0)
    thin = jnp.zeros((16, 256), F32)
    for k, (ref, row) in enumerate(((strength_ref, 0), (strength_ref, 1), (decay_ref, 0),
                                    (decay_ref, 1))):
        row_values = ref[...].astype(F32)[row : row + 1]
        thin = jnp.where(at == k, jnp.broadcast_to(row_values, (16, 256)), thin)
    wide_ref[mine, 256:272, 0:256] = thin.astype(BF16)
    wide_ref[mine, 256:272, 256:384] = jnp.zeros((16, 128), BF16)
    gains = gain_in_ref[...].astype(F32)
    for k in range(depth // 128):
        gain_ref[:, k * 128 : k * 128 + 128] = jnp.broadcast_to(gains[k : k + 1], (8, 128))
    fill_masks(masks_ref)
    pltpu.make_async_copy(own_block, own_block, load_sems.at[0]).wait()
    pl.semaphore_wait(barrier, len(peers))

    early = PlaneGather(wide_ref, SPLIT_A, send_a, recv_a)
    slices = depth // n_tp

    def halo_part(owner):
        return tok_ref.at[pl.ds(0, HALO), pl.ds(pl.multiple_of(owner * slices, 128), slices)]

    halos = [remote(
        tok_hbm.at[pl.ds(tok_rows - HALO, HALO), pl.ds(pl.multiple_of(tp * slices, 128), slices)],
        halo_part(tp), halo_send, halo_recv.at[0], next_place)]
    halos[0].start()
    early.own()
    for k in range(chunks):
        tok_loads[k].wait()
        norm_rows(tok_ref, gain_ref, HALO + k * CHUNK, CHUNK, 64)
        if k == 2:
            halos[0].wait_recv()
            for step in range(1, n_tp):
                remote(halo_part(tp), halo_part(tp), halo_send, halo_recv.at[1],
                       device_at(tp=step)).start()
    early.first()
    others = tok_ref.at[pl.ds(0, HALO), pl.ds(0, depth - slices)]
    pltpu.make_async_copy(others, others, halo_recv.at[1]).wait()
    sent = tok_ref.at[pl.ds(0, HALO), :]
    pltpu.make_async_copy(sent, sent, halo_send).wait()

    @pl.when(mine == 0)
    def _():
        tok_ref[0:HALO, :] = jnp.zeros((HALO, depth), BF16)

    norm_rows(tok_ref, gain_ref, 0, HALO, HALO)
    tile = 208

    def project(gather, places, into, first=False):
        @pl.loop(0, tok_ref.shape[0] // tile)
        def _(step):
            rows = pl.ds(pl.multiple_of(step * tile, 16), tile)
            total = None if first else into[rows, :]
            narrow = None if first or gather is not early else thin_ref[rows, :]
            for dz, dx in places:
                shard = gather.shard(dz, dx)
                normed = tok_ref[rows, pl.ds(pl.multiple_of(shard * 256, 256), 256)]
                term = dot(normed, gather.buf[shard, 0:256, :])
                total = term if total is None else total + term
                if gather is early:
                    term = dot_nt(normed, gather.buf[shard, 256:272, 0:256])
                    narrow = term if narrow is None else narrow + term
            into[rows, :] = total
            if gather is early:
                thin_ref[rows, :] = narrow

    first_acc, second_acc = acc_ref.at[0], acc_ref.at[1]
    partner = {"tp": y * 2 + (1 - core)}

    def meet():
        pl.semaphore_signal(gate, 1, device_id=partner, device_id_type=MESH_ID)
        pl.semaphore_wait(gate, 1)

    project(early, ORDER[:1], first_acc, first=True)
    early.second()
    project(early, ORDER[1:5], first_acc)
    early.third()
    for load in loads[3:]:
        load.wait()
    early.fourth()
    early.corners()
    project(early, ORDER[5:9], first_acc)
    early.fifth()
    later = PlaneGather(next_ref, SPLIT_A, send_d, recv_d)
    meet()
    later.own()
    early.straight()
    project(early, ORDER[9:11], first_acc)
    early.last()
    project(early, ORDER[11:], first_acc)
    later.first()

    taps_ref[...] = taps_in_ref[...].astype(F32)
    narrow = thin_ref[HALO:, :].T
    for head in range(heads):
        strength = narrow[head : head + 1] + strength_shift_ref[tp * heads + head]
        beta = 1.0 / (1.0 + jnp.exp(-strength))
        level = narrow[heads + head : heads + head + 1] + decay_shift_ref[tp * heads + head]
        soft = jnp.maximum(level, 0.0) + jnp.log1p(jnp.exp(-jnp.abs(level)))
        rate = jnp.exp(jnp.full((1, tok_rows), rate_ref[tp * heads + head], F32))
        decay = spike_ref[head : head + 1, :] - rate * soft
        lane = lax.rem(lax.broadcasted_iota(jnp.int32, (8, tok_rows), 1), CHUNK)
        summed = jnp.broadcast_to(decay, (8, tok_rows))
        step = 1
        while step < CHUNK:
            summed = summed + jnp.where(lane >= step, pltpu.roll(summed, step, 1), 0.0)
            step *= 2
        for chunk in range(chunks):
            row = head * chunks + chunk
            part = slice(chunk * CHUNK, chunk * CHUNK + CHUNK)
            grow_ref[row] = summed[:, part]
            gcol_ref[row] = jnp.broadcast_to(summed[0:1, part], (128, CHUNK)).T
            bcol_ref[row] = jnp.broadcast_to(beta[:, part], (128, CHUNK)).T
    rows = lax.broadcasted_iota(jnp.int32, (128, 256), 0)
    cols = lax.broadcasted_iota(jnp.int32, (128, 256), 1)
    identity = jnp.where(rows == cols, 1.0, 0.0)
    for head in range(heads):
        map_ref[head] = identity

    pool = PlaneGather(pool_w_ref, 128, send_b, recv_b)
    out = PlaneGather(out_w_ref, 256, send_c, recv_c)
    along_x, along_z = {}, {}

    def delta(head, events):
        delta_head(head, chunks, acc_ref, taps_ref, grow_ref, gcol_ref, bcol_ref, masks_ref,
                   map_ref, from_state_ref, local_ref, events)

    def send_x_maps(head):
        own_ref[head] = map_ref[head].astype(BF16)
        row_ref[0, head] = own_ref[head]
        along_x[head] = [
            remote(own_ref.at[head], row_ref.at[step, head], send_x.at[head], recv_x.at[head],
                   device_at(x=step)) for step in range(1, n_x)]
        for copy in along_x[head]:
            copy.start()

    def send_z_maps(head):
        moved = row_ref.at[pl.ds(1, n_x - 1), head]
        pltpu.make_async_copy(moved, moved, recv_x.at[head]).wait()
        so_far = before_here = identity
        for k in range(n_x):
            piece = row_ref[lax.rem(x - k + n_x, n_x), head]
            so_far = piece.astype(F32) if k == 0 else after(piece, so_far)
            before_here = jnp.where(k < x, so_far, before_here)
        map_ref[head] = before_here
        total_ref[head] = so_far.astype(BF16)
        column_ref[0, head] = total_ref[head]
        along_z[head] = [
            remote(total_ref.at[head], column_ref.at[step, head], send_z.at[head],
                   recv_z.at[head], device_at(z=step)) for step in range(1, n_z)]
        for copy in along_z[head]:
            copy.start()

    def enter(head):
        moved = column_ref.at[pl.ds(1, n_z - 1), head]
        pltpu.make_async_copy(moved, moved, recv_z.at[head]).wait()
        so_far = state = jnp.zeros((128, 128), F32)
        for k in range(n_z - 1):
            piece = column_ref[lax.rem(z - k + n_z, n_z), head]
            offset = piece[:, 128:].astype(F32)
            so_far = offset if k == 0 else dot(piece[:, :128], so_far.astype(BF16)) + offset
            state = jnp.where(k < z, so_far, state)
        entering = dot(map_ref[head, :, 0:128].astype(BF16), state.astype(BF16))
        state_ref[head] = (entering + map_ref[head, :, 128:256]).astype(BF16)

    later.second()
    delta(0, {("chunk", 3): later.third, ("level", 3): later.fourth})
    project(later, ORDER[:5], second_acc, first=True)
    later.fifth()
    send_x_maps(0)
    meet()
    pool.own()
    later.corners()
    project(later, ORDER[5:9], second_acc)
    later.straight()
    later.last()
    project(later, ORDER[9:], second_acc)
    pool.first()
    pool.second()
    delta(1, {("chunk", 0): lambda: send_z_maps(0), ("chunk", 3): pool.third,
              ("level", 4): pool.fourth, ("maps", 0): lambda: send_x_maps(1)})
    pool.fifth()
    meet()
    out.own("x")
    enter(0)
    wide = core == 1
    scales_at = lax.broadcasted_iota(jnp.int32, scale_in_ref.shape, 0)
    scales = [jnp.sum(jnp.where(scales_at == tp * 2 + group, scale_in_ref[...].astype(F32), 0.0),
                      axis=0, keepdims=True) for group in range(2)]

    def store_halves(chunk, lanes, values):
        for half in range(2):
            slot = lax.rem(half + core, 2)
            mixed_ref[chunk, pl.ds(pl.multiple_of(slot * 128, 128), 128), lanes] = (
                values[half * 128 : half * 128 + 128])

    pool.corners()
    project(pool, ORDER[:9], pool_ref, first=True)
    send_z_maps(1)
    out.own("z")
    pool.straight()
    pool.last()
    project(pool, ORDER[9:], pool_ref)

    @pl.loop(0, chunks)
    def _(chunk):
        for group, values in enumerate(
                pooled_rows(pool_ref, chunk, position, wide, mix_ref, scales)):
            store_halves(chunk, slice(group * 128, group * 128 + 128), values)

    enter(1)

    head_gain = head_gain_ref[...].astype(F32)
    pairs = {}
    slots = {2: 0, 1: 1, 3: 2, 0: 0}

    def finish_rows(ahead):
        chunk = lax.rem(y + ahead, n_y)
        where_rows = pl.ds(pl.multiple_of(chunk * CHUNK, CHUNK), CHUNK)
        for head in range(heads):
            raw = dot(from_state_ref[head, where_rows, :], state_ref[head])
            raw = raw + local_ref[head, where_rows, :]
            squares = jnp.mean(raw * raw, axis=-1, keepdims=True)
            normed = (raw * lax.rsqrt(squares + EPSILON) * head_gain).astype(BF16)
            store_halves(chunk, slice(256 + head * 128, 384 + head * 128), normed)

    def produce(ahead, piece):
        chunk = lax.rem(y + ahead, n_y)
        for block, (dz, dx) in enumerate(ORDER[4 * piece : 4 * piece + 4]):
            lanes = slice(block * 256, block * 256 + 256)
            product = dot(mixed_ref[chunk], out_w_ref[out.shard(dz, dx)])
            part_ref[slots[ahead], piece, :, lanes] = product[:128]
            pair_out_ref[ahead, piece, :, lanes] = product[128:].astype(BF16)
        index = ahead * 4 + piece if ahead else 0
        copy = remote(pair_out_ref.at[ahead, piece], pair_in_ref.at[ahead, piece],
                      pair_send, pair_recv.at[index], partner)
        copy.start()
        pairs[ahead, piece] = copy

    def chip_sum(ahead, piece):
        pairs[ahead, piece].wait_recv()
        return part_ref[slots[ahead], piece] + pair_in_ref[ahead, piece].astype(F32)

    up, down = device_at(tp=2), device_at(tp=-2)
    half = 64
    top, bottom = slice(0, half), slice(half, 2 * half)

    def pass_on(group, ahead, piece, rows, value, place, target):
        ring_out_ref[ahead - 1, piece, rows, :] = value.astype(BF16)
        where_rows = pl.ds(rows.start, half)
        copy = remote(ring_out_ref.at[ahead - 1, piece, where_rows],
                      target.at[piece, where_rows], ring_send, ring_recv.at[group], place)
        copy.start()

    def far(piece):
        value = chip_sum(2, piece)
        pass_on(piece, 2, piece, top, value[top], up, half_ref)
        pass_on(piece, 2, piece, bottom, value[bottom], down, half_ref)

    def near(piece):
        for ahead, rows, place, side in ((1, bottom, up, 0), (3, top, down, 1)):
            value = chip_sum(ahead, piece)
            part_ref[slots[ahead], piece] = value
            pass_on(4 + piece, ahead, piece, rows, value[rows], place, final_ref.at[side])

    def merged(piece):
        pltpu.make_async_copy(half_ref.at[piece], half_ref.at[piece], ring_recv.at[piece]).wait()
        for ahead, rows, place, side in ((1, top, up, 0), (3, bottom, down, 1)):
            value = part_ref[slots[ahead], piece, rows, :] + half_ref[piece, rows, :].astype(F32)
            pass_on(4 + piece, ahead, piece, rows, value, place, final_ref.at[side])

    def send_piece(piece):
        produce(2, piece)
        produce(1, piece)
        produce(3, piece)
        far(piece)
        near(piece)

    finish_rows(2)
    finish_rows(1)
    finish_rows(3)
    out.first()
    out.second()
    send_piece(0)
    finish_rows(0)
    out.third()
    merged(0)
    out.fourth()
    out.corners()
    send_piece(1)
    out.fifth()
    for piece in range(2):
        produce(0, piece)
    merged(1)
    out.straight()
    out.last()
    send_piece(2)
    merged(2)
    send_piece(3)
    for piece in range(2, 4):
        produce(0, piece)
    for gather in (early, later, pool, out):
        gather.drain()
    for head in range(heads):
        for ref, sem in ((row_ref, send_x), (column_ref, send_z)):
            moved = ref.at[pl.ds(1, n_x - 1), head]
            pltpu.make_async_copy(moved, moved, sem.at[head]).wait()
    merged(3)
    pltpu.make_async_copy(pair_in_ref.at[0], pair_in_ref.at[0], pair_recv.at[0]).wait()
    for piece in range(4):
        part_ref[0, piece] = part_ref[0, piece] + pair_in_ref[0, piece].astype(F32)
    pltpu.make_async_copy(pair_out_ref, pair_out_ref, pair_send).wait()
    for piece in range(4):
        arrived = final_ref.at[:, piece]
        pltpu.make_async_copy(arrived, arrived, ring_recv.at[4 + piece]).wait()
        value = part_ref[0, piece] + final_ref[0, piece].astype(F32)
        value = value + final_ref[1, piece].astype(F32)
        for block, (dz, dx) in enumerate(ORDER[4 * piece : 4 * piece + 4]):
            lanes = pl.ds(pl.multiple_of(out.shard(dz, dx) * 256, 256), 256)
            out_ref[:, lanes] = value[:, block * 256 : block * 256 + 256].astype(BF16)
    pltpu.make_async_copy(ring_out_ref, ring_out_ref, ring_send).wait()


def per_device(tokens, input_norm_scale, mean_input_weight, query_matrix, key_matrix, value_matrix,
               strength_weight, decay_input_weight, causal_filter_weight, head_decay_logrates,
               decay_input_shift, strength_shift, decay_spike, head_norm_scale,
               group_mixing_weight, mean_channel_scale, mean_output_weight, delta_output_weight):
    tok_rows, depth = tokens.shape
    heads = strength_weight.shape[1]
    n_z, n_x = lax.axis_size("sp_0"), lax.axis_size("sp_1")
    chunks = tok_rows // CHUNK
    pairs = heads * chunks
    width = n_z * n_x * 256
    pieces = width // PIECE
    vmem = pl.BlockSpec(memory_space=pltpu.VMEM)
    smem = pl.BlockSpec(memory_space=pltpu.SMEM)
    hbm = pl.BlockSpec(memory_space=pl.ANY)
    dma = pltpu.SemaphoreType.DMA
    return pl.pallas_call(
        lambda *refs: layer_kernel(heads, *refs),
        out_shape=jax.ShapeDtypeStruct((128, width), BF16),
        in_specs=[hbm] * 9 + [vmem] * 6 + [smem] * 3,
        out_specs=vmem,
        scratch_shapes=[
            pltpu.VMEM((tok_rows + HALO, depth), BF16),
            pltpu.VMEM((16, 272, 384), BF16),
            pltpu.VMEM((16, 256, 384), BF16),
            pltpu.VMEM((16, 256, 256), BF16),
            pltpu.VMEM((16, 512, 256), BF16),
            pltpu.VMEM((heads, tok_rows + HALO, 384), F32),
            pltpu.VMEM((tok_rows + HALO, 256), F32),
            pltpu.VMEM((tok_rows + HALO, 16), F32),
            pltpu.VMEM((8, depth), F32),
            pltpu.VMEM((3, CONV, 256), BF16),
            pltpu.VMEM((3, CONV, 256), F32),
            pltpu.VMEM((2, 128, 128), BF16),
            pltpu.VMEM((pairs, 8, CHUNK), F32),
            pltpu.VMEM((pairs, CHUNK, 128), F32),
            pltpu.VMEM((pairs, CHUNK, 128), F32),
            pltpu.VMEM((8, CHUNK, CHUNK), BF16),
            pltpu.VMEM((heads, 128, 256), F32),
            pltpu.VMEM((heads, tok_rows, 128), BF16),
            pltpu.VMEM((heads, tok_rows, 128), F32),
            pltpu.VMEM((heads, 128, 256), BF16),
            pltpu.VMEM((n_x, heads, 128, 256), BF16),
            pltpu.VMEM((heads, 128, 256), BF16),
            pltpu.VMEM((n_z, heads, 128, 256), BF16),
            pltpu.VMEM((heads, 128, 128), BF16),
            pltpu.VMEM((chunks, CHUNK, 512), BF16),
            pltpu.VMEM((3, pieces, 128, PIECE), F32),
            pltpu.VMEM((4, pieces, 128, PIECE), BF16),
            pltpu.VMEM((4, pieces, 128, PIECE), BF16),
            pltpu.VMEM((3, pieces, 128, PIECE), BF16),
            pltpu.VMEM((pieces, 128, PIECE), BF16),
            pltpu.VMEM((2, pieces, 128, PIECE), BF16),
            dma((chunks,)), dma((9,)), dma(()), dma((2,)),
            dma(()), dma((8,)), dma(()), dma((8,)), dma(()), dma((8,)), dma(()), dma((8,)),
            dma((heads,)), dma((heads,)), dma((heads,)), dma((heads,)),
            dma(()), dma((16,)), dma(()), dma((8,)),
            pltpu.SemaphoreType.REGULAR,
        ],
        compiler_params=pltpu.CompilerParams(
            vmem_limit_bytes=VMEM_LIMIT, collective_id=0, has_side_effects=True),
        name="layer",
    )(tokens, mean_input_weight, query_matrix, key_matrix, value_matrix, mean_output_weight,
      delta_output_weight, jnp.transpose(causal_filter_weight, (1, 0, 2)), group_mixing_weight,
      input_norm_scale.reshape(-1, 128), head_norm_scale.reshape(1, HEAD_DIM),
      mean_channel_scale.reshape(-1, 128), strength_weight.T, decay_input_weight.T, decay_spike.T,
      head_decay_logrates, decay_input_shift, strength_shift)


def solution(mesh):
    finer = Mesh(mesh.devices.reshape(4, 4, mesh.shape["tp"]), SP_TP)
    in_specs = (
        P(SP, None), P(), P(SP, "tp"), P(SP, "tp"), P(SP, "tp"), P(SP, "tp"), P(SP, "tp"),
        P(SP, "tp"), P(), P(), P(), P(), P(SP, "tp"), P(), P(), P(), P("tp", SP), P("tp", SP),
    )
    return jax.shard_map(
        per_device, mesh=finer, in_specs=in_specs, out_specs=P(SP_TP, None), check_vma=False
    )
```

```python
import jax
import jax.numpy as jnp
from jax import lax
from jax.experimental import pallas as pl
from jax.experimental.pallas import tpu as pltpu
from jax.sharding import Mesh
from jax.sharding import PartitionSpec as P

HEAD_DIM = 128
CONV = 4
CHUNK = 256
HALO = 16
EPSILON = 1e-06
SP = ("sp_0", "sp_1")
SP_TP = ("sp_0", "sp_1", "tp")
MESH_ID = pl.DeviceIdType.MESH
F32 = jnp.float32
BF16 = jnp.bfloat16
VMEM_LIMIT = 63 * 1000 * 1000


def dot(a, b):
    return jnp.dot(a, b, preferred_element_type=F32)


def dot_nt(a, b):
    return lax.dot_general(a, b, (((1,), (1,)), ((), ())), preferred_element_type=F32)


def dot_tn(a, b):
    return lax.dot_general(a, b, (((0,), (0,)), ((), ())), preferred_element_type=F32)


def unit_rows(values):
    return values * lax.rsqrt(jnp.sum(values * values, axis=-1, keepdims=True) + EPSILON)


def fill_masks(masks_ref):
    rows = lax.broadcasted_iota(jnp.int32, (CHUNK, CHUNK), 0)
    cols = lax.broadcasted_iota(jnp.int32, (CHUNK, CHUNK), 1)
    apart = jnp.bitwise_xor(rows, cols)
    for level in range(masks_ref.shape[0]):
        inside = (rows > cols) & (apart >= 2**level) & (apart < 2 ** (level + 1))
        masks_ref[level] = jnp.where(inside, 1.0, 0.0).astype(BF16)


def conv_rows(raw_ref, taps_ref, head, start, part):
    lanes = slice(part * 128, part * 128 + 128)
    tap_lanes = slice(head * 128, head * 128 + 128)
    rows = raw_ref[head, start + HALO - 8 : start + HALO + CHUNK, lanes]
    mixed = taps_ref[part, CONV - 1 : CONV, tap_lanes] * rows[8:]
    for back in range(1, CONV):
        tap = taps_ref[part, CONV - 1 - back : CONV - back, tap_lanes]
        mixed = mixed + tap * pltpu.roll(rows, back, 0)[8:]
    return mixed / (1.0 + jnp.exp(-mixed))


def delta_head(head, chunks, raw_ref, taps_ref, grow_ref, gcol_ref, bcol_ref, masks_ref, map_ref,
               from_state_ref, local_ref, events):
    rows = lax.broadcasted_iota(jnp.int32, (CHUNK, CHUNK), 0)
    cols = lax.broadcasted_iota(jnp.int32, (CHUNK, CHUNK), 1)
    work = []
    for chunk in range(chunks):
        row = head * chunks + chunk
        start = chunk * CHUNK
        query = unit_rows(conv_rows(raw_ref, taps_ref, head, start, 0)) * HEAD_DIM ** (-0.5)
        key = unit_rows(conv_rows(raw_ref, taps_ref, head, start, 1))
        value = conv_rows(raw_ref, taps_ref, head, start, 2)
        gcol, bcol, grow = gcol_ref[row], bcol_ref[row], grow_ref[row][0:1]
        key_b = key.astype(BF16)
        both = jnp.concatenate([query.astype(BF16), key_b], axis=0)
        inner = dot_nt(both, key_b)
        spread = jnp.exp(jnp.minimum(jnp.concatenate([gcol, gcol], axis=1) - grow, 0.0))
        scores = jnp.where(rows >= cols, inner[:CHUNK] * spread, 0.0).astype(BF16)
        strict = jnp.where(rows > cols, inner[CHUNK:] * spread, 0.0)
        strict = (strict * jnp.concatenate([bcol, bcol], axis=1)).astype(BF16)
        grown = jnp.exp(gcol)
        right = jnp.concatenate([value * bcol, key * bcol * grown], axis=1).astype(BF16)
        last = grow[:, CHUNK - 1 : CHUNK]
        key_dec = (key * jnp.exp(last - gcol)).astype(BF16)
        inverse = jnp.where(rows == cols, 1.0, 0.0).astype(BF16) - strict * masks_ref[0]
        work.append([strict, inverse, scores, right, key_dec, query * grown, jnp.exp(last)])
        events.get(("chunk", chunk), lambda: None)()
    for level in range(1, masks_ref.shape[0]):
        inner = [dot(w[0] * masks_ref[level], w[1]).astype(BF16) for w in work]
        for w, part in zip(work, inner):
            w[1] = w[1] - dot(w[1], part).astype(BF16)
        events.get(("level", level), lambda: None)()
    solved = [dot(w[1], w[3]).astype(BF16) for w in work]
    moved = [dot_tn(w[4], s) for w, s in zip(work, solved)]
    current = map_ref[head]
    starts = []
    for chunk in range(chunks):
        current_b = current.astype(BF16)
        starts.append(current_b)
        added = jnp.concatenate([jnp.zeros((128, 128), F32), moved[chunk][:, :128]], axis=1)
        current = (current * work[chunk][6] - dot(moved[chunk][:, 128:].astype(BF16), current_b)
                   + added)
    map_ref[head] = current
    events.get(("maps", 0), lambda: None)()
    seen = [dot(w[2], s) for w, s in zip(work, solved)]
    for chunk in range(chunks):
        where_rows = slice(chunk * CHUNK, chunk * CHUNK + CHUNK)
        asked = (work[chunk][5] - seen[chunk][:, 128:]).astype(BF16)
        answer = dot(asked, starts[chunk])
        from_state_ref[head, where_rows, :] = answer[:, :128].astype(BF16)
        local_ref[head, where_rows, :] = answer[:, 128:] + seen[chunk][:, :128]


SPLIT_A = 128
PIECE = 512
ORDER = ((0, 0), (0, 1), (0, -1), (1, 0), (-1, 0), (1, 1), (1, -1), (-1, 1), (-1, -1), (0, 2), (2, 0),
         (1, 2), (-1, 2), (2, 1), (2, -1), (2, 2))


class PlaneGather:
    def __init__(self, buf, split, send_sem, recv_sems):
        self.buf, self.split = buf, split
        self.send_sem, self.recv_sems = send_sem, recv_sems
        self.z, self.x = lax.axis_index("sp_0"), lax.axis_index("sp_1")

    def shard(self, dz, dx):
        return lax.rem(self.z + dz + 4, 4) * 4 + lax.rem(self.x + dx + 4, 4)

    def rows(self, part):
        split, total = self.split, self.buf.shape[1]
        quarter = split // 32 * 16
        rest = split + (total - split) // 32 * 16
        return {"a": (0, split), "b": (split, total), "a0": (0, quarter), "a1": (quarter, split),
                "b0": (split, rest), "b1": (rest, total)}[part]

    def send(self, group, source, part, way):
        low, high = self.rows(part)
        ref = self.buf.at[self.shard(*source), pl.ds(low, high - low), :]
        remote(ref, ref, self.send_sem, self.recv_sems.at[group],
               {"sp_0": lax.rem(self.z + way[0] + 4, 4),
                "sp_1": lax.rem(self.x + way[1] + 4, 4)}).start()

    def got(self, group, blocks, part=None):
        ref = self.buf.at[pl.ds(0, blocks)]
        if part is not None:
            low, high = self.rows(part)
            ref = self.buf.at[pl.ds(0, blocks), pl.ds(low, high - low), :]
        pltpu.make_async_copy(ref, ref, self.recv_sems.at[group]).wait()

    def got_own(self, along, part):
        name = "ab"[part] if along == "x" else "ba"[part]
        self.got(part if along == "x" else 8 + part, 2, name)

    def own(self, along="xz", parts=(0, 1)):
        for part in parts:
            for step in (1, -1):
                if "x" in along:
                    self.send(part, (0, 0), "ab"[part], (0, step))
                if "z" in along:
                    self.send(8 + part, (0, 0), "ba"[part], (step, 0))

    def quarters(self):
        self.send(2, (0, -1), "a0", (0, 1))
        self.send(2, (0, 1), "a1", (0, -1))
        self.send(2, (-1, 0), "b0", (1, 0))
        self.send(2, (1, 0), "b1", (-1, 0))

    def first(self, waits="xz", quarters_last=False):
        for along in waits:
            self.got_own(along, 0)
        if not quarters_last:
            self.quarters()
        for side, group in ((1, 3), (-1, 4)):
            for step in (1, -1):
                self.send(group, (0, side * step), "a", (step, 0))
                self.send(group, (side * step, 0), "b", (0, step))
        if quarters_last:
            self.quarters()

    def second(self, waits="xz"):
        for along in waits:
            self.got_own(along, 1)
        self.send(6, (-1, 0), "a", (1, 0))
        self.send(6, (0, -1), "b", (0, 1))

    def third(self):
        self.got(2, 1)
        for step, group in ((-1, 5), (1, 10)):
            self.send(group, (0, 2), "a", (step, 0))
            self.send(group, (2, 0), "b", (0, step))

    def fourth(self):
        self.got(3, 2)
        for at, group in ((1, 7), (-1, 10)):
            self.send(group, (-at, at), "a", (at, 0))
            self.send(group, (at, -at), "b", (0, at))

    def corners(self):
        self.got(4, 2)

    def fifth(self):
        self.got(5, 1)
        self.send(11, (1, 2), "a", (-1, 0))
        self.send(11, (2, 1), "b", (0, -1))

    def straight(self):
        self.got(6, 1)

    def last(self, stages=(0, 1, 2)):
        for stage in stages:
            self.got((7, 10, 11)[stage], (1, 2, 1)[stage])

    def drain(self):
        ref = self.buf.at[pl.ds(0, 15)]
        pltpu.make_async_copy(ref, ref, self.send_sem).wait()


def after(later, earlier):
    offset = jnp.concatenate([jnp.zeros((128, 128), F32), later[:, 128:].astype(F32)], axis=1)
    return dot(later[:, :128], earlier.astype(BF16)) + offset


def device_at(z=0, x=0, tp=0):
    place = {}
    for name, step in (("sp_0", z), ("sp_1", x), ("tp", tp)):
        if step:
            size = lax.axis_size(name)
            place[name] = lax.rem(lax.axis_index(name) + step + size, size)
    return place


def remote(src, dst, send_sem, recv_sem, place):
    return pltpu.make_async_remote_copy(
        src_ref=src, dst_ref=dst, send_sem=send_sem, recv_sem=recv_sem, device_id=place,
        device_id_type=MESH_ID)


def pooled_rows(pool_ref, chunk, position, wide, mix_ref, scales):
    parts = []
    for group in range(2):
        lanes = slice(group * 128, group * 128 + 128)
        rows = pool_ref[pl.ds(pl.multiple_of(chunk * CHUNK, CHUNK), CHUNK + HALO), lanes]
        reach = 1
        sums = rows
        for _ in range(group + 1):
            sums = sums + pltpu.roll(sums, reach, 0)
            reach *= 2
        broad = sums
        for _ in range(2):
            broad = broad + pltpu.roll(broad, reach, 0)
            reach *= 2
        short, long = 2 << group, 8 << group
        seen = lax.broadcasted_iota(jnp.int32, (CHUNK, 128), 0) + (position + chunk * CHUNK + 1)
        count = jnp.minimum(seen, jnp.where(wide, long, short)).astype(F32)
        window = jnp.where(wide, broad[HALO:], sums[HALO:])
        diff = (window / count - rows[HALO:]).astype(BF16)
        parts.append((dot(diff, mix_ref[group]) * scales[group]).astype(BF16))
    return parts


def norm_rows(tok_ref, gain_ref, start, count, step_rows):
    @pl.loop(0, count // step_rows)
    def _(step):
        rows = pl.ds(pl.multiple_of(start + step * step_rows, 16), step_rows)
        values = tok_ref[rows, :].astype(F32)
        scale = lax.rsqrt(jnp.mean(values * values, axis=-1, keepdims=True) + EPSILON)
        tok_ref[rows, :] = (tok_ref[rows, :].astype(F32) * scale * gain_ref[0:1, :]).astype(BF16)


def layer_kernel(heads, tok_hbm, pool_hbm, query_hbm, key_hbm, value_hbm, pool_out_hbm,
                 delta_out_hbm, taps_hbm, mix_hbm, gain_in_ref, head_gain_ref, scale_in_ref,
                 strength_ref, decay_ref, spike_ref, rate_ref, decay_shift_ref, strength_shift_ref,
                 out_ref,
                 tok_ref, wide_ref, next_ref, pool_w_ref, out_w_ref, acc_ref, pool_ref, thin_ref, gain_ref,
                 taps_in_ref, taps_ref, mix_ref, grow_ref, gcol_ref, bcol_ref, masks_ref, map_ref,
                 from_state_ref, local_ref, own_ref, row_ref, total_ref, column_ref, state_ref,
                 mixed_ref, part_ref, pair_out_ref, pair_in_ref, ring_out_ref, half_ref, final_ref,
                 tok_sems, load_sems, halo_send, halo_recv, send_a, recv_a, send_d, recv_d, send_b, recv_b,
                 send_c, recv_c, send_x, recv_x, send_z, recv_z, pair_send, pair_recv, ring_send,
                 ring_recv, gate):
    z, x, tp = lax.axis_index("sp_0"), lax.axis_index("sp_1"), lax.axis_index("tp")
    n_z, n_x, n_tp = lax.axis_size("sp_0"), lax.axis_size("sp_1"), lax.axis_size("tp")
    y, core = tp // 2, lax.rem(tp, 2)
    n_y = n_tp // 2
    tok_rows, depth = tok_hbm.shape
    chunks = tok_rows // CHUNK
    mine = z * n_x + x
    position = mine * tok_rows
    loads = []
    for k, (hbm, ref) in enumerate((
            (query_hbm.at[:, pl.ds(0, 128)], wide_ref.at[mine, pl.ds(0, 256), pl.ds(0, 128)]),
            (key_hbm.at[:, pl.ds(0, 128)], wide_ref.at[mine, pl.ds(0, 256), pl.ds(128, 128)]),
            (value_hbm.at[:, pl.ds(0, 128)], wide_ref.at[mine, pl.ds(0, 256), pl.ds(256, 128)]),
            (query_hbm.at[:, pl.ds(128, 128)], next_ref.at[mine, :, pl.ds(0, 128)]),
            (key_hbm.at[:, pl.ds(128, 128)], next_ref.at[mine, :, pl.ds(128, 128)]),
            (value_hbm.at[:, pl.ds(128, 128)], next_ref.at[mine, :, pl.ds(256, 128)]),
            (pool_hbm, pool_w_ref.at[mine]),
            (pool_out_hbm, out_w_ref.at[mine, pl.ds(0, 256), :]),
            (delta_out_hbm, out_w_ref.at[mine, pl.ds(256, 256), :]),
            (taps_hbm.at[:, :, pl.ds(pl.multiple_of(tp * 256, 256), 256)], taps_in_ref),
            (mix_hbm.at[pl.ds(tp * 2, 2)], mix_ref))):
        load = pltpu.make_async_copy(hbm, ref, load_sems.at[max(k - 2, 0)])
        load.start()
        loads.append(load)
    own_block = wide_ref.at[mine, pl.ds(0, 256), :]
    tok_loads = []
    for k in range(chunks):
        load = pltpu.make_async_copy(
            tok_hbm.at[pl.ds(k * CHUNK, CHUNK), :],
            tok_ref.at[pl.ds(HALO + k * CHUNK, CHUNK), :], tok_sems.at[k])
        load.start()
        tok_loads.append(load)
    following, before = lax.rem(mine + 1, 16), lax.rem(mine + 15, 16)
    next_place = {"sp_0": following // 4, "sp_1": lax.rem(following, 4)}
    last_place = {"sp_0": before // 4, "sp_1": lax.rem(before, 4)}
    peers = [device_at(x=step) for step in range(1, n_x)]
    peers += [device_at(z=step) for step in range(1, n_z)]
    peers += [device_at(tp=step) for step in range(1, n_tp)]
    peers += [next_place, last_place]
    barrier = pltpu.get_barrier_semaphore()
    for peer in peers:
        pl.semaphore_signal(barrier, 1, device_id=peer, device_id_type=MESH_ID)
    at = lax.broadcasted_iota(jnp.int32, (16, 256), 0)
    thin = jnp.zeros((16, 256), F32)
    for k, (ref, row) in enumerate(((strength_ref, 0), (strength_ref, 1), (decay_ref, 0),
                                    (decay_ref, 1))):
        row_values = ref[...].astype(F32)[row : row + 1]
        thin = jnp.where(at == k, jnp.broadcast_to(row_values, (16, 256)), thin)
    wide_ref[mine, 256:272, 0:256] = thin.astype(BF16)
    wide_ref[mine, 256:272, 256:384] = jnp.zeros((16, 128), BF16)
    pltpu.make_async_copy(own_block, own_block, load_sems.at[0]).wait()
    pl.semaphore_wait(barrier, len(peers))

    early = PlaneGather(wide_ref, SPLIT_A, send_a, recv_a)
    slices = depth // n_tp

    def halo_part(owner):
        return tok_ref.at[pl.ds(0, HALO), pl.ds(pl.multiple_of(owner * slices, 128), slices)]

    halos = [remote(
        tok_hbm.at[pl.ds(tok_rows - HALO, HALO), pl.ds(pl.multiple_of(tp * slices, 128), slices)],
        halo_part(tp), halo_send, halo_recv.at[0], next_place)]
    halos[0].start()
    early.own()
    gains = gain_in_ref[...].astype(F32)
    for k in range(depth // 128):
        gain_ref[:, k * 128 : k * 128 + 128] = jnp.broadcast_to(gains[k : k + 1], (8, 128))
    for k in range(chunks):
        tok_loads[k].wait()
        norm_rows(tok_ref, gain_ref, HALO + k * CHUNK, CHUNK, 64)
    early.first()
    halos[0].wait_recv()
    for step in range(1, n_tp):
        remote(halo_part(tp), halo_part(tp), halo_send, halo_recv.at[1],
               device_at(tp=step)).start()
    early.second()
    others = tok_ref.at[pl.ds(0, HALO), pl.ds(0, depth - slices)]
    pltpu.make_async_copy(others, others, halo_recv.at[1]).wait()
    sent = tok_ref.at[pl.ds(0, HALO), :]
    pltpu.make_async_copy(sent, sent, halo_send).wait()

    @pl.when(mine == 0)
    def _():
        tok_ref[0:HALO, :] = jnp.zeros((HALO, depth), BF16)

    norm_rows(tok_ref, gain_ref, 0, HALO, HALO)
    fill_masks(masks_ref)
    tile = 208

    def project(gather, places, into, first=False):
        @pl.loop(0, tok_ref.shape[0] // tile)
        def _(step):
            rows = pl.ds(pl.multiple_of(step * tile, 16), tile)
            total = None if first else into[rows, :]
            narrow = None if first or gather is not early else thin_ref[rows, :]
            for dz, dx in places:
                shard = gather.shard(dz, dx)
                normed = tok_ref[rows, pl.ds(pl.multiple_of(shard * 256, 256), 256)]
                term = dot(normed, gather.buf[shard, 0:256, :])
                total = term if total is None else total + term
                if gather is early:
                    term = dot_nt(normed, gather.buf[shard, 256:272, 0:256])
                    narrow = term if narrow is None else narrow + term
            into[rows, :] = total
            if gather is early:
                thin_ref[rows, :] = narrow

    first_acc, second_acc = acc_ref.at[0], acc_ref.at[1]
    partner = {"tp": y * 2 + (1 - core)}

    def meet():
        pl.semaphore_signal(gate, 1, device_id=partner, device_id_type=MESH_ID)
        pl.semaphore_wait(gate, 1)

    project(early, ORDER[:1], first_acc, first=True)
    early.third()
    for load in loads[3:]:
        load.wait()
    early.fourth()
    project(early, ORDER[1:5], first_acc)
    early.corners()
    early.fifth()
    later = PlaneGather(next_ref, SPLIT_A, send_d, recv_d)
    meet()
    later.own()
    project(early, ORDER[5:9], first_acc)
    early.straight()
    project(early, ORDER[9:11], first_acc)
    early.last()
    later.first()
    project(early, ORDER[11:], first_acc)
    later.second()

    taps_ref[...] = taps_in_ref[...].astype(F32)
    narrow = thin_ref[HALO:, :].T
    for head in range(heads):
        strength = narrow[head : head + 1] + strength_shift_ref[tp * heads + head]
        beta = 1.0 / (1.0 + jnp.exp(-strength))
        level = narrow[heads + head : heads + head + 1] + decay_shift_ref[tp * heads + head]
        soft = jnp.maximum(level, 0.0) + jnp.log1p(jnp.exp(-jnp.abs(level)))
        rate = jnp.exp(jnp.full((1, tok_rows), rate_ref[tp * heads + head], F32))
        decay = spike_ref[head : head + 1, :] - rate * soft
        lane = lax.rem(lax.broadcasted_iota(jnp.int32, (8, tok_rows), 1), CHUNK)
        summed = jnp.broadcast_to(decay, (8, tok_rows))
        step = 1
        while step < CHUNK:
            summed = summed + jnp.where(lane >= step, pltpu.roll(summed, step, 1), 0.0)
            step *= 2
        for chunk in range(chunks):
            row = head * chunks + chunk
            part = slice(chunk * CHUNK, chunk * CHUNK + CHUNK)
            grow_ref[row] = summed[:, part]
            gcol_ref[row] = jnp.broadcast_to(summed[0:1, part], (128, CHUNK)).T
            bcol_ref[row] = jnp.broadcast_to(beta[:, part], (128, CHUNK)).T
    rows = lax.broadcasted_iota(jnp.int32, (128, 256), 0)
    cols = lax.broadcasted_iota(jnp.int32, (128, 256), 1)
    identity = jnp.where(rows == cols, 1.0, 0.0)
    for head in range(heads):
        map_ref[head] = identity

    pool = PlaneGather(pool_w_ref, 128, send_b, recv_b)
    out = PlaneGather(out_w_ref, 256, send_c, recv_c)
    along_x, along_z = {}, {}

    def delta(head, events):
        delta_head(head, chunks, acc_ref, taps_ref, grow_ref, gcol_ref, bcol_ref, masks_ref,
                   map_ref, from_state_ref, local_ref, events)

    def send_x_maps(head):
        own_ref[head] = map_ref[head].astype(BF16)
        row_ref[0, head] = own_ref[head]
        along_x[head] = [
            remote(own_ref.at[head], row_ref.at[step, head], send_x.at[head], recv_x.at[head],
                   device_at(x=step)) for step in range(1, n_x)]
        for copy in along_x[head]:
            copy.start()

    def send_z_maps(head):
        moved = row_ref.at[pl.ds(1, n_x - 1), head]
        pltpu.make_async_copy(moved, moved, recv_x.at[head]).wait()
        so_far = before_here = identity
        for k in range(n_x):
            piece = row_ref[lax.rem(x - k + n_x, n_x), head]
            so_far = piece.astype(F32) if k == 0 else after(piece, so_far)
            before_here = jnp.where(k < x, so_far, before_here)
        map_ref[head] = before_here
        total_ref[head] = so_far.astype(BF16)
        column_ref[0, head] = total_ref[head]
        along_z[head] = [
            remote(total_ref.at[head], column_ref.at[step, head], send_z.at[head],
                   recv_z.at[head], device_at(z=step)) for step in range(1, n_z)]
        for copy in along_z[head]:
            copy.start()

    def enter(head):
        moved = column_ref.at[pl.ds(1, n_z - 1), head]
        pltpu.make_async_copy(moved, moved, recv_z.at[head]).wait()
        so_far = state = jnp.zeros((128, 128), F32)
        for k in range(n_z - 1):
            piece = column_ref[lax.rem(z - k + n_z, n_z), head]
            offset = piece[:, 128:].astype(F32)
            so_far = offset if k == 0 else dot(piece[:, :128], so_far.astype(BF16)) + offset
            state = jnp.where(k < z, so_far, state)
        entering = dot(map_ref[head, :, 0:128].astype(BF16), state.astype(BF16))
        state_ref[head] = (entering + map_ref[head, :, 128:256]).astype(BF16)

    delta(0, {("chunk", 2): later.third, ("level", 2): later.fourth})
    later.fifth()
    send_x_maps(0)
    meet()
    pool.own()
    project(later, ORDER[:5], second_acc, first=True)
    later.corners()
    project(later, ORDER[5:9], second_acc)
    later.straight()
    project(later, ORDER[9:11], second_acc)
    later.last()
    project(later, ORDER[11:], second_acc)
    delta(1, {("chunk", 0): lambda: send_z_maps(0), ("chunk", 2): pool.first,
              ("level", 2): pool.second, ("maps", 0): lambda: send_x_maps(1)})
    pool.third()
    project(pool, ORDER[:5], pool_ref, first=True)
    pool.fourth()
    enter(0)
    pool.corners()
    project(pool, ORDER[5:9], pool_ref)
    pool.fifth()
    meet()
    out.own("x")
    send_z_maps(1)
    out.own("z")
    wide = core == 1
    scales_at = lax.broadcasted_iota(jnp.int32, scale_in_ref.shape, 0)
    scales = [jnp.sum(jnp.where(scales_at == tp * 2 + group, scale_in_ref[...].astype(F32), 0.0),
                      axis=0, keepdims=True) for group in range(2)]

    def store_halves(chunk, lanes, values):
        for half in range(2):
            slot = lax.rem(half + core, 2)
            mixed_ref[chunk, pl.ds(pl.multiple_of(slot * 128, 128), 128), lanes] = (
                values[half * 128 : half * 128 + 128])

    pool.straight()
    pool.last()
    project(pool, ORDER[9:], pool_ref)

    @pl.loop(0, chunks)
    def _(chunk):
        for group, values in enumerate(
                pooled_rows(pool_ref, chunk, position, wide, mix_ref, scales)):
            store_halves(chunk, slice(group * 128, group * 128 + 128), values)

    enter(1)

    head_gain = head_gain_ref[...].astype(F32)
    pairs = {}
    slots = {2: 0, 1: 1, 3: 2, 0: 0}

    def finish_rows(ahead):
        chunk = lax.rem(y + ahead, n_y)
        where_rows = pl.ds(pl.multiple_of(chunk * CHUNK, CHUNK), CHUNK)
        for head in range(heads):
            raw = dot(from_state_ref[head, where_rows, :], state_ref[head])
            raw = raw + local_ref[head, where_rows, :]
            squares = jnp.mean(raw * raw, axis=-1, keepdims=True)
            normed = (raw * lax.rsqrt(squares + EPSILON) * head_gain).astype(BF16)
            store_halves(chunk, slice(256 + head * 128, 384 + head * 128), normed)

    def produce(ahead, piece):
        chunk = lax.rem(y + ahead, n_y)
        for block, (dz, dx) in enumerate(ORDER[2 * piece : 2 * piece + 2]):
            lanes = slice(block * 256, block * 256 + 256)
            product = dot(mixed_ref[chunk], out_w_ref[out.shard(dz, dx)])
            part_ref[slots[ahead], piece, :, lanes] = product[:128]
            pair_out_ref[ahead, piece, :, lanes] = product[128:].astype(BF16)
        index = ahead * 8 + piece if ahead else 0
        copy = remote(pair_out_ref.at[ahead, piece], pair_in_ref.at[ahead, piece],
                      pair_send, pair_recv.at[index], partner)
        copy.start()
        pairs[ahead, piece] = copy

    def chip_sum(ahead, piece):
        pairs[ahead, piece].wait_recv()
        return part_ref[slots[ahead], piece] + pair_in_ref[ahead, piece].astype(F32)

    up, down = device_at(tp=2), device_at(tp=-2)
    half = 64
    top, bottom = slice(0, half), slice(half, 2 * half)

    def pass_on(group, ahead, piece, rows, value, place, target):
        ring_out_ref[ahead - 1, piece, rows, :] = value.astype(BF16)
        where_rows = pl.ds(rows.start, half)
        copy = remote(ring_out_ref.at[ahead - 1, piece, where_rows],
                      target.at[piece, where_rows], ring_send, ring_recv.at[group], place)
        copy.start()

    def far(piece):
        value = chip_sum(2, piece)
        pass_on(piece, 2, piece, top, value[top], up, half_ref)
        pass_on(piece, 2, piece, bottom, value[bottom], down, half_ref)

    def near(piece):
        for ahead, rows, place, side in ((1, bottom, up, 0), (3, top, down, 1)):
            value = chip_sum(ahead, piece)
            part_ref[slots[ahead], piece] = value
            pass_on(8 + piece, ahead, piece, rows, value[rows], place, final_ref.at[side])

    def merged(piece):
        pltpu.make_async_copy(half_ref.at[piece], half_ref.at[piece], ring_recv.at[piece]).wait()
        for ahead, rows, place, side in ((1, top, up, 0), (3, bottom, down, 1)):
            value = part_ref[slots[ahead], piece, rows, :] + half_ref[piece, rows, :].astype(F32)
            pass_on(8 + piece, ahead, piece, rows, value, place, final_ref.at[side])

    def send_piece(piece):
        produce(2, piece)
        produce(1, piece)
        produce(3, piece)
        far(piece)
        near(piece)

    finish_rows(2)
    finish_rows(1)
    finish_rows(3)
    out.first(quarters_last=True)
    out.got_own("x", 1)
    send_piece(0)
    out.second(waits="z")
    send_piece(1)
    finish_rows(0)
    merged(0)
    out.fourth()
    out.corners()
    send_piece(2)
    out.third()
    merged(1)
    send_piece(3)
    out.fifth()
    for piece in range(4):
        produce(0, piece)
    merged(2)
    out.straight()
    send_piece(4)
    merged(3)
    out.last((0,))
    produce(2, 5)
    far(5)
    merged(4)
    out.last((1,))
    produce(2, 6)
    far(6)
    produce(1, 5)
    produce(3, 5)
    near(5)
    merged(5)
    out.last((2,))
    produce(2, 7)
    far(7)
    for piece in (6, 7):
        produce(1, piece)
        produce(3, piece)
        near(piece)
        merged(piece)
    for piece in range(4, 8):
        produce(0, piece)
    for gather in (early, later, pool, out):
        gather.drain()
    for head in range(heads):
        for ref, sem in ((row_ref, send_x), (column_ref, send_z)):
            moved = ref.at[pl.ds(1, n_x - 1), head]
            pltpu.make_async_copy(moved, moved, sem.at[head]).wait()
    pltpu.make_async_copy(pair_in_ref.at[0], pair_in_ref.at[0], pair_recv.at[0]).wait()
    for piece in range(8):
        part_ref[0, piece] = part_ref[0, piece] + pair_in_ref[0, piece].astype(F32)
    pltpu.make_async_copy(pair_out_ref, pair_out_ref, pair_send).wait()
    for piece in range(8):
        arrived = final_ref.at[:, piece]
        pltpu.make_async_copy(arrived, arrived, ring_recv.at[8 + piece]).wait()
        value = part_ref[0, piece] + final_ref[0, piece].astype(F32)
        value = value + final_ref[1, piece].astype(F32)
        for block, (dz, dx) in enumerate(ORDER[2 * piece : 2 * piece + 2]):
            lanes = pl.ds(pl.multiple_of(out.shard(dz, dx) * 256, 256), 256)
            out_ref[:, lanes] = value[:, block * 256 : block * 256 + 256].astype(BF16)
    pltpu.make_async_copy(ring_out_ref, ring_out_ref, ring_send).wait()


def per_device(tokens, input_norm_scale, mean_input_weight, query_matrix, key_matrix, value_matrix,
               strength_weight, decay_input_weight, causal_filter_weight, head_decay_logrates,
               decay_input_shift, strength_shift, decay_spike, head_norm_scale,
               group_mixing_weight, mean_channel_scale, mean_output_weight, delta_output_weight):
    tok_rows, depth = tokens.shape
    heads = strength_weight.shape[1]
    n_z, n_x = lax.axis_size("sp_0"), lax.axis_size("sp_1")
    chunks = tok_rows // CHUNK
    pairs = heads * chunks
    width = n_z * n_x * 256
    pieces = width // PIECE
    vmem = pl.BlockSpec(memory_space=pltpu.VMEM)
    smem = pl.BlockSpec(memory_space=pltpu.SMEM)
    hbm = pl.BlockSpec(memory_space=pl.ANY)
    dma = pltpu.SemaphoreType.DMA
    return pl.pallas_call(
        lambda *refs: layer_kernel(heads, *refs),
        out_shape=jax.ShapeDtypeStruct((128, width), BF16),
        in_specs=[hbm] * 9 + [vmem] * 6 + [smem] * 3,
        out_specs=vmem,
        scratch_shapes=[
            pltpu.VMEM((tok_rows + HALO, depth), BF16),
            pltpu.VMEM((16, 272, 384), BF16),
            pltpu.VMEM((16, 256, 384), BF16),
            pltpu.VMEM((16, 256, 256), BF16),
            pltpu.VMEM((16, 512, 256), BF16),
            pltpu.VMEM((heads, tok_rows + HALO, 384), F32),
            pltpu.VMEM((tok_rows + HALO, 256), F32),
            pltpu.VMEM((tok_rows + HALO, 16), F32),
            pltpu.VMEM((8, depth), F32),
            pltpu.VMEM((3, CONV, 256), BF16),
            pltpu.VMEM((3, CONV, 256), F32),
            pltpu.VMEM((2, 128, 128), BF16),
            pltpu.VMEM((pairs, 8, CHUNK), F32),
            pltpu.VMEM((pairs, CHUNK, 128), F32),
            pltpu.VMEM((pairs, CHUNK, 128), F32),
            pltpu.VMEM((8, CHUNK, CHUNK), BF16),
            pltpu.VMEM((heads, 128, 256), F32),
            pltpu.VMEM((heads, tok_rows, 128), BF16),
            pltpu.VMEM((heads, tok_rows, 128), F32),
            pltpu.VMEM((heads, 128, 256), BF16),
            pltpu.VMEM((n_x, heads, 128, 256), BF16),
            pltpu.VMEM((heads, 128, 256), BF16),
            pltpu.VMEM((n_z, heads, 128, 256), BF16),
            pltpu.VMEM((heads, 128, 128), BF16),
            pltpu.VMEM((chunks, CHUNK, 512), BF16),
            pltpu.VMEM((3, pieces, 128, PIECE), F32),
            pltpu.VMEM((4, pieces, 128, PIECE), BF16),
            pltpu.VMEM((4, pieces, 128, PIECE), BF16),
            pltpu.VMEM((3, pieces, 128, PIECE), BF16),
            pltpu.VMEM((pieces, 128, PIECE), BF16),
            pltpu.VMEM((2, pieces, 128, PIECE), BF16),
            dma((chunks,)), dma((9,)), dma(()), dma((2,)),
            dma(()), dma((12,)), dma(()), dma((12,)), dma(()), dma((12,)), dma(()), dma((12,)),
            dma((heads,)), dma((heads,)), dma((heads,)), dma((heads,)),
            dma(()), dma((32,)), dma(()), dma((16,)),
            pltpu.SemaphoreType.REGULAR,
        ],
        compiler_params=pltpu.CompilerParams(
            vmem_limit_bytes=VMEM_LIMIT, collective_id=0, has_side_effects=True),
        name="layer",
    )(tokens, mean_input_weight, query_matrix, key_matrix, value_matrix, mean_output_weight,
      delta_output_weight, jnp.transpose(causal_filter_weight, (1, 0, 2)), group_mixing_weight,
      input_norm_scale.reshape(-1, 128), head_norm_scale.reshape(1, HEAD_DIM),
      mean_channel_scale.reshape(-1, 128), strength_weight.T, decay_input_weight.T, decay_spike.T,
      head_decay_logrates, decay_input_shift, strength_shift)


def solution(mesh):
    finer = Mesh(mesh.devices.reshape(4, 4, mesh.shape["tp"]), SP_TP)
    in_specs = (
        P(SP, None), P(), P(SP, "tp"), P(SP, "tp"), P(SP, "tp"), P(SP, "tp"), P(SP, "tp"),
        P(SP, "tp"), P(), P(), P(), P(), P(SP, "tp"), P(), P(), P(), P("tp", SP), P("tp", SP),
    )
    return jax.shard_map(
        per_device, mesh=finer, in_specs=in_specs, out_specs=P(SP_TP, None), check_vma=False
    )
```

```python
import jax
import jax.numpy as jnp
from jax import lax
from jax.experimental import pallas as pl
from jax.experimental.pallas import tpu as pltpu
from jax.sharding import Mesh
from jax.sharding import PartitionSpec as P

HEAD_DIM = 128
CONV = 4
CHUNK = 256
HALO = 16
EPSILON = 1e-06
SP = ("sp_0", "sp_1")
SP_TP = ("sp_0", "sp_1", "tp")
MESH_ID = pl.DeviceIdType.MESH
F32 = jnp.float32
BF16 = jnp.bfloat16
VMEM_LIMIT = 63 * 1000 * 1000


def dot(a, b):
    return jnp.dot(a, b, preferred_element_type=F32)


def dot_nt(a, b):
    return lax.dot_general(a, b, (((1,), (1,)), ((), ())), preferred_element_type=F32)


def dot_tn(a, b):
    return lax.dot_general(a, b, (((0,), (0,)), ((), ())), preferred_element_type=F32)


def unit_rows(values):
    return values * lax.rsqrt(jnp.sum(values * values, axis=-1, keepdims=True) + EPSILON)


def fill_masks(masks_ref):
    rows = lax.broadcasted_iota(jnp.int32, (CHUNK, CHUNK), 0)
    cols = lax.broadcasted_iota(jnp.int32, (CHUNK, CHUNK), 1)
    apart = jnp.bitwise_xor(rows, cols)
    for level in range(masks_ref.shape[0]):
        inside = (rows > cols) & (apart >= 2**level) & (apart < 2 ** (level + 1))
        masks_ref[level] = jnp.where(inside, 1.0, 0.0).astype(BF16)


def conv_rows(raw_ref, taps_ref, head, start, part):
    lanes = slice(part * 128, part * 128 + 128)
    tap_lanes = slice(head * 128, head * 128 + 128)
    rows = raw_ref[head, start + HALO - 8 : start + HALO + CHUNK, lanes]
    mixed = taps_ref[part, CONV - 1 : CONV, tap_lanes] * rows[8:]
    for back in range(1, CONV):
        tap = taps_ref[part, CONV - 1 - back : CONV - back, tap_lanes]
        mixed = mixed + tap * pltpu.roll(rows, back, 0)[8:]
    return mixed / (1.0 + jnp.exp(-mixed))


def delta_head(head, chunks, raw_ref, taps_ref, grow_ref, gcol_ref, bcol_ref, masks_ref, map_ref,
               from_state_ref, local_ref, events):
    rows = lax.broadcasted_iota(jnp.int32, (CHUNK, CHUNK), 0)
    cols = lax.broadcasted_iota(jnp.int32, (CHUNK, CHUNK), 1)
    work = []
    for chunk in range(chunks):
        row = head * chunks + chunk
        start = chunk * CHUNK
        query = unit_rows(conv_rows(raw_ref, taps_ref, head, start, 0)) * HEAD_DIM ** (-0.5)
        key = unit_rows(conv_rows(raw_ref, taps_ref, head, start, 1))
        value = conv_rows(raw_ref, taps_ref, head, start, 2)
        gcol, bcol, grow = gcol_ref[row], bcol_ref[row], grow_ref[row][0:1]
        key_b = key.astype(BF16)
        both = jnp.concatenate([query.astype(BF16), key_b], axis=0)
        inner = dot_nt(both, key_b)
        spread = jnp.exp(jnp.minimum(jnp.concatenate([gcol, gcol], axis=1) - grow, 0.0))
        scores = jnp.where(rows >= cols, inner[:CHUNK] * spread, 0.0).astype(BF16)
        strict = jnp.where(rows > cols, inner[CHUNK:] * spread, 0.0)
        strict = (strict * jnp.concatenate([bcol, bcol], axis=1)).astype(BF16)
        grown = jnp.exp(gcol)
        right = jnp.concatenate([value * bcol, key * bcol * grown], axis=1).astype(BF16)
        last = grow[:, CHUNK - 1 : CHUNK]
        key_dec = (key * jnp.exp(last - gcol)).astype(BF16)
        inverse = jnp.where(rows == cols, 1.0, 0.0).astype(BF16) - strict * masks_ref[0]
        work.append([strict, inverse, scores, right, key_dec, query * grown, jnp.exp(last)])
        events.get(("chunk", chunk), lambda: None)()
    for level in range(1, masks_ref.shape[0]):
        inner = [dot(w[0] * masks_ref[level], w[1]).astype(BF16) for w in work]
        for w, part in zip(work, inner):
            w[1] = w[1] - dot(w[1], part).astype(BF16)
        events.get(("level", level), lambda: None)()
    solved = [dot(w[1], w[3]).astype(BF16) for w in work]
    moved = [dot_tn(w[4], s) for w, s in zip(work, solved)]
    current = map_ref[head]
    starts = []
    for chunk in range(chunks):
        current_b = current.astype(BF16)
        starts.append(current_b)
        added = jnp.concatenate([jnp.zeros((128, 128), F32), moved[chunk][:, :128]], axis=1)
        current = (current * work[chunk][6] - dot(moved[chunk][:, 128:].astype(BF16), current_b)
                   + added)
    map_ref[head] = current
    events.get(("maps", 0), lambda: None)()
    seen = [dot(w[2], s) for w, s in zip(work, solved)]
    for chunk in range(chunks):
        where_rows = slice(chunk * CHUNK, chunk * CHUNK + CHUNK)
        asked = (work[chunk][5] - seen[chunk][:, 128:]).astype(BF16)
        answer = dot(asked, starts[chunk])
        from_state_ref[head, where_rows, :] = answer[:, :128].astype(BF16)
        local_ref[head, where_rows, :] = answer[:, 128:] + seen[chunk][:, :128]


SPLIT_A = 128
PIECE = 512
ORDER = ((0, 0), (0, 1), (0, -1), (1, 0), (-1, 0), (1, 1), (1, -1), (-1, 1), (-1, -1), (0, 2), (2, 0),
         (1, 2), (-1, 2), (2, 1), (2, -1), (2, 2))


class PlaneGather:
    def __init__(self, buf, split, send_sem, recv_sems):
        self.buf, self.split = buf, split
        self.send_sem, self.recv_sems = send_sem, recv_sems
        self.z, self.x = lax.axis_index("sp_0"), lax.axis_index("sp_1")

    def shard(self, dz, dx):
        return lax.rem(self.z + dz + 4, 4) * 4 + lax.rem(self.x + dx + 4, 4)

    def rows(self, part):
        split, total = self.split, self.buf.shape[1]
        quarter = split // 32 * 16
        rest = split + (total - split) // 32 * 16
        return {"a": (0, split), "b": (split, total), "a0": (0, quarter), "a1": (quarter, split),
                "b0": (split, rest), "b1": (rest, total)}[part]

    def send(self, group, source, part, way):
        low, high = self.rows(part)
        ref = self.buf.at[self.shard(*source), pl.ds(low, high - low), :]
        remote(ref, ref, self.send_sem, self.recv_sems.at[group],
               {"sp_0": lax.rem(self.z + way[0] + 4, 4),
                "sp_1": lax.rem(self.x + way[1] + 4, 4)}).start()

    def got(self, group, blocks, part=None):
        ref = self.buf.at[pl.ds(0, blocks)]
        if part is not None:
            low, high = self.rows(part)
            ref = self.buf.at[pl.ds(0, blocks), pl.ds(low, high - low), :]
        pltpu.make_async_copy(ref, ref, self.recv_sems.at[group]).wait()

    def got_own(self, along, part):
        name = "ab"[part] if along == "x" else "ba"[part]
        self.got(part if along == "x" else 8 + part, 2, name)

    def own(self, along="xz", parts=(0, 1)):
        for part in parts:
            for step in (1, -1):
                if "x" in along:
                    self.send(part, (0, 0), "ab"[part], (0, step))
                if "z" in along:
                    self.send(8 + part, (0, 0), "ba"[part], (step, 0))

    def quarters(self):
        self.send(2, (0, -1), "a0", (0, 1))
        self.send(2, (0, 1), "a1", (0, -1))
        self.send(2, (-1, 0), "b0", (1, 0))
        self.send(2, (1, 0), "b1", (-1, 0))

    def first(self, waits="xz", quarters_last=False):
        for along in waits:
            self.got_own(along, 0)
        if not quarters_last:
            self.quarters()
        for side, group in ((1, 3), (-1, 4)):
            for step in (1, -1):
                self.send(group, (0, side * step), "a", (step, 0))
                self.send(group, (side * step, 0), "b", (0, step))
        if quarters_last:
            self.quarters()

    def second(self, waits="xz"):
        for along in waits:
            self.got_own(along, 1)
        self.send(6, (-1, 0), "a", (1, 0))
        self.send(6, (0, -1), "b", (0, 1))

    def third(self):
        self.got(2, 1)
        for step, group in ((-1, 5), (1, 10)):
            self.send(group, (0, 2), "a", (step, 0))
            self.send(group, (2, 0), "b", (0, step))

    def fourth(self):
        self.got(3, 2)
        for at, group in ((1, 7), (-1, 10)):
            self.send(group, (-at, at), "a", (at, 0))
            self.send(group, (at, -at), "b", (0, at))

    def corners(self):
        self.got(4, 2)

    def fifth(self):
        self.got(5, 1)
        self.send(11, (1, 2), "a", (-1, 0))
        self.send(11, (2, 1), "b", (0, -1))

    def straight(self):
        self.got(6, 1)

    def last(self, stages=(0, 1, 2)):
        for stage in stages:
            self.got((7, 10, 11)[stage], (1, 2, 1)[stage])

    def drain(self):
        ref = self.buf.at[pl.ds(0, 15)]
        pltpu.make_async_copy(ref, ref, self.send_sem).wait()


def after(later, earlier):
    offset = jnp.concatenate([jnp.zeros((128, 128), F32), later[:, 128:].astype(F32)], axis=1)
    return dot(later[:, :128], earlier.astype(BF16)) + offset


def device_at(z=0, x=0, tp=0):
    place = {}
    for name, step in (("sp_0", z), ("sp_1", x), ("tp", tp)):
        if step:
            size = lax.axis_size(name)
            place[name] = lax.rem(lax.axis_index(name) + step + size, size)
    return place


def remote(src, dst, send_sem, recv_sem, place):
    return pltpu.make_async_remote_copy(
        src_ref=src, dst_ref=dst, send_sem=send_sem, recv_sem=recv_sem, device_id=place,
        device_id_type=MESH_ID)


def pooled_rows(pool_ref, chunk, position, wide, mix_ref, scales):
    parts = []
    for group in range(2):
        lanes = slice(group * 128, group * 128 + 128)
        rows = pool_ref[pl.ds(pl.multiple_of(chunk * CHUNK, CHUNK), CHUNK + HALO), lanes]
        reach = 1
        sums = rows
        for _ in range(group + 1):
            sums = sums + pltpu.roll(sums, reach, 0)
            reach *= 2
        broad = sums
        for _ in range(2):
            broad = broad + pltpu.roll(broad, reach, 0)
            reach *= 2
        short, long = 2 << group, 8 << group
        seen = lax.broadcasted_iota(jnp.int32, (CHUNK, 128), 0) + (position + chunk * CHUNK + 1)
        count = jnp.minimum(seen, jnp.where(wide, long, short)).astype(F32)
        window = jnp.where(wide, broad[HALO:], sums[HALO:])
        diff = (window / count - rows[HALO:]).astype(BF16)
        parts.append((dot(diff, mix_ref[group]) * scales[group]).astype(BF16))
    return parts


def norm_rows(tok_ref, gain_ref, start, count, step_rows):
    @pl.loop(0, count // step_rows)
    def _(step):
        rows = pl.ds(pl.multiple_of(start + step * step_rows, 16), step_rows)
        values = tok_ref[rows, :].astype(F32)
        scale = lax.rsqrt(jnp.mean(values * values, axis=-1, keepdims=True) + EPSILON)
        tok_ref[rows, :] = (tok_ref[rows, :].astype(F32) * scale * gain_ref[0:1, :]).astype(BF16)


def layer_kernel(heads, tok_hbm, pool_hbm, query_hbm, key_hbm, value_hbm, pool_out_hbm,
                 delta_out_hbm, taps_hbm, mix_hbm, gain_in_ref, head_gain_ref, scale_in_ref,
                 strength_ref, decay_ref, spike_ref, rate_ref, decay_shift_ref, strength_shift_ref,
                 out_ref,
                 tok_ref, wide_ref, next_ref, pool_w_ref, out_w_ref, acc_ref, pool_ref, thin_ref, gain_ref,
                 taps_in_ref, taps_ref, mix_ref, grow_ref, gcol_ref, bcol_ref, masks_ref, map_ref,
                 from_state_ref, local_ref, own_ref, row_ref, total_ref, column_ref, state_ref,
                 mixed_ref, part_ref, pair_out_ref, pair_in_ref, ring_out_ref, half_ref, final_ref,
                 tok_sems, load_sems, halo_send, halo_recv, send_a, recv_a, send_d, recv_d, send_b, recv_b,
                 send_c, recv_c, send_x, recv_x, send_z, recv_z, pair_send, pair_recv, ring_send,
                 ring_recv, gate):
    z, x, tp = lax.axis_index("sp_0"), lax.axis_index("sp_1"), lax.axis_index("tp")
    n_z, n_x, n_tp = lax.axis_size("sp_0"), lax.axis_size("sp_1"), lax.axis_size("tp")
    y, core = tp // 2, lax.rem(tp, 2)
    n_y = n_tp // 2
    tok_rows, depth = tok_hbm.shape
    chunks = tok_rows // CHUNK
    mine = z * n_x + x
    position = mine * tok_rows
    loads = []
    for k, (hbm, ref) in enumerate((
            (query_hbm.at[:, pl.ds(0, 128)], wide_ref.at[mine, pl.ds(0, 256), pl.ds(0, 128)]),
            (key_hbm.at[:, pl.ds(0, 128)], wide_ref.at[mine, pl.ds(0, 256), pl.ds(128, 128)]),
            (value_hbm.at[:, pl.ds(0, 128)], wide_ref.at[mine, pl.ds(0, 256), pl.ds(256, 128)]),
            (query_hbm.at[:, pl.ds(128, 128)], next_ref.at[mine, :, pl.ds(0, 128)]),
            (key_hbm.at[:, pl.ds(128, 128)], next_ref.at[mine, :, pl.ds(128, 128)]),
            (value_hbm.at[:, pl.ds(128, 128)], next_ref.at[mine, :, pl.ds(256, 128)]),
            (pool_hbm, pool_w_ref.at[mine]),
            (pool_out_hbm, out_w_ref.at[mine, pl.ds(0, 256), :]),
            (delta_out_hbm, out_w_ref.at[mine, pl.ds(256, 256), :]),
            (taps_hbm.at[:, :, pl.ds(pl.multiple_of(tp * 256, 256), 256)], taps_in_ref),
            (mix_hbm.at[pl.ds(tp * 2, 2)], mix_ref))):
        load = pltpu.make_async_copy(hbm, ref, load_sems.at[max(k - 2, 0)])
        load.start()
        loads.append(load)
    own_block = wide_ref.at[mine, pl.ds(0, 256), :]
    tok_loads = []
    for k in range(chunks):
        load = pltpu.make_async_copy(
            tok_hbm.at[pl.ds(k * CHUNK, CHUNK), :],
            tok_ref.at[pl.ds(HALO + k * CHUNK, CHUNK), :], tok_sems.at[k])
        load.start()
        tok_loads.append(load)
    following, before = lax.rem(mine + 1, 16), lax.rem(mine + 15, 16)
    next_place = {"sp_0": following // 4, "sp_1": lax.rem(following, 4)}
    last_place = {"sp_0": before // 4, "sp_1": lax.rem(before, 4)}
    peers = [device_at(x=step) for step in range(1, n_x)]
    peers += [device_at(z=step) for step in range(1, n_z)]
    peers += [device_at(tp=step) for step in range(1, n_tp)]
    peers += [next_place, last_place]
    barrier = pltpu.get_barrier_semaphore()
    for peer in peers:
        pl.semaphore_signal(barrier, 1, device_id=peer, device_id_type=MESH_ID)
    at = lax.broadcasted_iota(jnp.int32, (16, 256), 0)
    thin = jnp.zeros((16, 256), F32)
    for k, (ref, row) in enumerate(((strength_ref, 0), (strength_ref, 1), (decay_ref, 0),
                                    (decay_ref, 1))):
        row_values = ref[...].astype(F32)[row : row + 1]
        thin = jnp.where(at == k, jnp.broadcast_to(row_values, (16, 256)), thin)
    wide_ref[mine, 256:272, 0:256] = thin.astype(BF16)
    wide_ref[mine, 256:272, 256:384] = jnp.zeros((16, 128), BF16)
    pltpu.make_async_copy(own_block, own_block, load_sems.at[0]).wait()
    pl.semaphore_wait(barrier, len(peers))

    early = PlaneGather(wide_ref, SPLIT_A, send_a, recv_a)
    slices = depth // n_tp

    def halo_part(owner):
        return tok_ref.at[pl.ds(0, HALO), pl.ds(pl.multiple_of(owner * slices, 128), slices)]

    halos = [remote(
        tok_hbm.at[pl.ds(tok_rows - HALO, HALO), pl.ds(pl.multiple_of(tp * slices, 128), slices)],
        halo_part(tp), halo_send, halo_recv.at[0], next_place)]
    halos[0].start()
    early.own()
    gains = gain_in_ref[...].astype(F32)
    for k in range(depth // 128):
        gain_ref[:, k * 128 : k * 128 + 128] = jnp.broadcast_to(gains[k : k + 1], (8, 128))
    for k in range(chunks):
        tok_loads[k].wait()
        norm_rows(tok_ref, gain_ref, HALO + k * CHUNK, CHUNK, 64)
    early.first()
    halos[0].wait_recv()
    for step in range(1, n_tp):
        remote(halo_part(tp), halo_part(tp), halo_send, halo_recv.at[1],
               device_at(tp=step)).start()
    early.second()
    others = tok_ref.at[pl.ds(0, HALO), pl.ds(0, depth - slices)]
    pltpu.make_async_copy(others, others, halo_recv.at[1]).wait()
    sent = tok_ref.at[pl.ds(0, HALO), :]
    pltpu.make_async_copy(sent, sent, halo_send).wait()

    @pl.when(mine == 0)
    def _():
        tok_ref[0:HALO, :] = jnp.zeros((HALO, depth), BF16)

    norm_rows(tok_ref, gain_ref, 0, HALO, HALO)
    fill_masks(masks_ref)
    tile = 208

    def project(gather, places, into, first=False):
        @pl.loop(0, tok_ref.shape[0] // tile)
        def _(step):
            rows = pl.ds(pl.multiple_of(step * tile, 16), tile)
            total = None if first else into[rows, :]
            narrow = None if first or gather is not early else thin_ref[rows, :]
            for dz, dx in places:
                shard = gather.shard(dz, dx)
                normed = tok_ref[rows, pl.ds(pl.multiple_of(shard * 256, 256), 256)]
                term = dot(normed, gather.buf[shard, 0:256, :])
                total = term if total is None else total + term
                if gather is early:
                    term = dot_nt(normed, gather.buf[shard, 256:272, 0:256])
                    narrow = term if narrow is None else narrow + term
            into[rows, :] = total
            if gather is early:
                thin_ref[rows, :] = narrow

    first_acc, second_acc = acc_ref.at[0], acc_ref.at[1]
    partner = {"tp": y * 2 + (1 - core)}

    def meet():
        pl.semaphore_signal(gate, 1, device_id=partner, device_id_type=MESH_ID)
        pl.semaphore_wait(gate, 1)

    project(early, ORDER[:1], first_acc, first=True)
    early.third()
    for load in loads[3:]:
        load.wait()
    early.fourth()
    project(early, ORDER[1:5], first_acc)
    early.corners()
    early.fifth()
    later = PlaneGather(next_ref, SPLIT_A, send_d, recv_d)
    meet()
    later.own()
    project(early, ORDER[5:9], first_acc)
    early.straight()
    project(early, ORDER[9:11], first_acc)
    early.last()
    later.first()
    project(early, ORDER[11:], first_acc)
    later.second()

    taps_ref[...] = taps_in_ref[...].astype(F32)
    narrow = thin_ref[HALO:, :].T
    for head in range(heads):
        strength = narrow[head : head + 1] + strength_shift_ref[tp * heads + head]
        beta = 1.0 / (1.0 + jnp.exp(-strength))
        level = narrow[heads + head : heads + head + 1] + decay_shift_ref[tp * heads + head]
        soft = jnp.maximum(level, 0.0) + jnp.log1p(jnp.exp(-jnp.abs(level)))
        rate = jnp.exp(jnp.full((1, tok_rows), rate_ref[tp * heads + head], F32))
        decay = spike_ref[head : head + 1, :] - rate * soft
        lane = lax.rem(lax.broadcasted_iota(jnp.int32, (8, tok_rows), 1), CHUNK)
        summed = jnp.broadcast_to(decay, (8, tok_rows))
        step = 1
        while step < CHUNK:
            summed = summed + jnp.where(lane >= step, pltpu.roll(summed, step, 1), 0.0)
            step *= 2
        for chunk in range(chunks):
            row = head * chunks + chunk
            part = slice(chunk * CHUNK, chunk * CHUNK + CHUNK)
            grow_ref[row] = summed[:, part]
            gcol_ref[row] = jnp.broadcast_to(summed[0:1, part], (128, CHUNK)).T
            bcol_ref[row] = jnp.broadcast_to(beta[:, part], (128, CHUNK)).T
    rows = lax.broadcasted_iota(jnp.int32, (128, 256), 0)
    cols = lax.broadcasted_iota(jnp.int32, (128, 256), 1)
    identity = jnp.where(rows == cols, 1.0, 0.0)
    for head in range(heads):
        map_ref[head] = identity

    pool = PlaneGather(pool_w_ref, 128, send_b, recv_b)
    out = PlaneGather(out_w_ref, 256, send_c, recv_c)
    along_x, along_z = {}, {}

    def delta(head, events):
        delta_head(head, chunks, acc_ref, taps_ref, grow_ref, gcol_ref, bcol_ref, masks_ref,
                   map_ref, from_state_ref, local_ref, events)

    def send_x_maps(head):
        own_ref[head] = map_ref[head].astype(BF16)
        row_ref[0, head] = own_ref[head]
        along_x[head] = [
            remote(own_ref.at[head], row_ref.at[step, head], send_x.at[head], recv_x.at[head],
                   device_at(x=step)) for step in range(1, n_x)]
        for copy in along_x[head]:
            copy.start()

    def send_z_maps(head):
        moved = row_ref.at[pl.ds(1, n_x - 1), head]
        pltpu.make_async_copy(moved, moved, recv_x.at[head]).wait()
        so_far = before_here = identity
        for k in range(n_x):
            piece = row_ref[lax.rem(x - k + n_x, n_x), head]
            so_far = piece.astype(F32) if k == 0 else after(piece, so_far)
            before_here = jnp.where(k < x, so_far, before_here)
        map_ref[head] = before_here
        total_ref[head] = so_far.astype(BF16)
        column_ref[0, head] = total_ref[head]
        along_z[head] = [
            remote(total_ref.at[head], column_ref.at[step, head], send_z.at[head],
                   recv_z.at[head], device_at(z=step)) for step in range(1, n_z)]
        for copy in along_z[head]:
            copy.start()

    def enter(head):
        moved = column_ref.at[pl.ds(1, n_z - 1), head]
        pltpu.make_async_copy(moved, moved, recv_z.at[head]).wait()
        so_far = state = jnp.zeros((128, 128), F32)
        for k in range(n_z - 1):
            piece = column_ref[lax.rem(z - k + n_z, n_z), head]
            offset = piece[:, 128:].astype(F32)
            so_far = offset if k == 0 else dot(piece[:, :128], so_far.astype(BF16)) + offset
            state = jnp.where(k < z, so_far, state)
        entering = dot(map_ref[head, :, 0:128].astype(BF16), state.astype(BF16))
        state_ref[head] = (entering + map_ref[head, :, 128:256]).astype(BF16)

    delta(0, {("chunk", 2): later.third, ("level", 2): later.fourth})
    later.fifth()
    send_x_maps(0)
    meet()
    pool.own()
    project(later, ORDER[:5], second_acc, first=True)
    later.corners()
    project(later, ORDER[5:9], second_acc)
    later.straight()
    project(later, ORDER[9:11], second_acc)
    later.last()
    project(later, ORDER[11:], second_acc)
    delta(1, {("chunk", 2): pool.first, ("chunk", 3): lambda: send_z_maps(0),
              ("maps", 0): lambda: send_x_maps(1)})
    pool.second()
    pool.third()
    project(pool, ORDER[:5], pool_ref, first=True)
    pool.fourth()
    enter(0)
    pool.corners()
    project(pool, ORDER[5:9], pool_ref)
    pool.fifth()
    meet()
    out.own("x")
    send_z_maps(1)
    out.own("z")
    wide = core == 1
    scales_at = lax.broadcasted_iota(jnp.int32, scale_in_ref.shape, 0)
    scales = [jnp.sum(jnp.where(scales_at == tp * 2 + group, scale_in_ref[...].astype(F32), 0.0),
                      axis=0, keepdims=True) for group in range(2)]

    def store_halves(chunk, lanes, values):
        for half in range(2):
            slot = lax.rem(half + core, 2)
            mixed_ref[chunk, pl.ds(pl.multiple_of(slot * 128, 128), 128), lanes] = (
                values[half * 128 : half * 128 + 128])

    pool.straight()
    pool.last()
    project(pool, ORDER[9:], pool_ref)

    @pl.loop(0, chunks)
    def _(chunk):
        for group, values in enumerate(
                pooled_rows(pool_ref, chunk, position, wide, mix_ref, scales)):
            store_halves(chunk, slice(group * 128, group * 128 + 128), values)

    enter(1)

    head_gain = head_gain_ref[...].astype(F32)
    pairs = {}
    slots = {2: 0, 1: 1, 3: 2, 0: 0}

    def finish_rows(ahead):
        chunk = lax.rem(y + ahead, n_y)
        where_rows = pl.ds(pl.multiple_of(chunk * CHUNK, CHUNK), CHUNK)
        for head in range(heads):
            raw = dot(from_state_ref[head, where_rows, :], state_ref[head])
            raw = raw + local_ref[head, where_rows, :]
            squares = jnp.mean(raw * raw, axis=-1, keepdims=True)
            normed = (raw * lax.rsqrt(squares + EPSILON) * head_gain).astype(BF16)
            store_halves(chunk, slice(256 + head * 128, 384 + head * 128), normed)

    def produce(ahead, piece):
        chunk = lax.rem(y + ahead, n_y)
        for block, (dz, dx) in enumerate(ORDER[2 * piece : 2 * piece + 2]):
            lanes = slice(block * 256, block * 256 + 256)
            product = dot(mixed_ref[chunk], out_w_ref[out.shard(dz, dx)])
            part_ref[slots[ahead], piece, :, lanes] = product[:128]
            pair_out_ref[ahead, piece, :, lanes] = product[128:].astype(BF16)
        index = ahead * 8 + piece if ahead else 0
        copy = remote(pair_out_ref.at[ahead, piece], pair_in_ref.at[ahead, piece],
                      pair_send, pair_recv.at[index], partner)
        copy.start()
        pairs[ahead, piece] = copy

    def chip_sum(ahead, piece):
        pairs[ahead, piece].wait_recv()
        return part_ref[slots[ahead], piece] + pair_in_ref[ahead, piece].astype(F32)

    up, down = device_at(tp=2), device_at(tp=-2)
    half = 64
    top, bottom = slice(0, half), slice(half, 2 * half)

    def pass_on(group, ahead, piece, rows, value, place, target):
        ring_out_ref[ahead - 1, piece, rows, :] = value.astype(BF16)
        where_rows = pl.ds(rows.start, half)
        copy = remote(ring_out_ref.at[ahead - 1, piece, where_rows],
                      target.at[piece, where_rows], ring_send, ring_recv.at[group], place)
        copy.start()

    def far(piece):
        value = chip_sum(2, piece)
        pass_on(piece, 2, piece, top, value[top], up, half_ref)
        pass_on(piece, 2, piece, bottom, value[bottom], down, half_ref)

    def near(piece):
        for ahead, rows, place, side in ((1, bottom, up, 0), (3, top, down, 1)):
            value = chip_sum(ahead, piece)
            part_ref[slots[ahead], piece] = value
            pass_on(8 + piece, ahead, piece, rows, value[rows], place, final_ref.at[side])

    def merged(piece):
        pltpu.make_async_copy(half_ref.at[piece], half_ref.at[piece], ring_recv.at[piece]).wait()
        for ahead, rows, place, side in ((1, top, up, 0), (3, bottom, down, 1)):
            value = part_ref[slots[ahead], piece, rows, :] + half_ref[piece, rows, :].astype(F32)
            pass_on(8 + piece, ahead, piece, rows, value, place, final_ref.at[side])

    def send_piece(piece):
        produce(2, piece)
        produce(1, piece)
        produce(3, piece)
        far(piece)
        near(piece)

    finish_rows(2)
    out.first(quarters_last=True)
    out.got_own("x", 1)
    produce(2, 0)
    finish_rows(1)
    finish_rows(3)
    produce(1, 0)
    far(0)
    produce(3, 0)
    near(0)
    out.second(waits="z")
    send_piece(1)
    finish_rows(0)
    merged(0)
    out.fourth()
    out.corners()
    send_piece(2)
    out.third()
    merged(1)
    send_piece(3)
    out.fifth()
    for piece in range(4):
        produce(0, piece)
    merged(2)
    out.straight()
    send_piece(4)
    merged(3)
    out.last((0,))
    produce(2, 5)
    far(5)
    merged(4)
    out.last((1,))
    produce(2, 6)
    far(6)
    produce(1, 5)
    produce(3, 5)
    near(5)
    merged(5)
    out.last((2,))
    produce(2, 7)
    far(7)
    for piece in (6, 7):
        produce(1, piece)
        produce(3, piece)
        near(piece)
        merged(piece)
    for piece in range(4, 8):
        produce(0, piece)
    for gather in (early, later, pool, out):
        gather.drain()
    for head in range(heads):
        for ref, sem in ((row_ref, send_x), (column_ref, send_z)):
            moved = ref.at[pl.ds(1, n_x - 1), head]
            pltpu.make_async_copy(moved, moved, sem.at[head]).wait()
    pltpu.make_async_copy(pair_in_ref.at[0], pair_in_ref.at[0], pair_recv.at[0]).wait()
    for piece in range(8):
        part_ref[0, piece] = part_ref[0, piece] + pair_in_ref[0, piece].astype(F32)
    pltpu.make_async_copy(pair_out_ref, pair_out_ref, pair_send).wait()
    for piece in range(8):
        arrived = final_ref.at[:, piece]
        pltpu.make_async_copy(arrived, arrived, ring_recv.at[8 + piece]).wait()
        value = part_ref[0, piece] + final_ref[0, piece].astype(F32)
        value = value + final_ref[1, piece].astype(F32)
        for block, (dz, dx) in enumerate(ORDER[2 * piece : 2 * piece + 2]):
            lanes = pl.ds(pl.multiple_of(out.shard(dz, dx) * 256, 256), 256)
            out_ref[:, lanes] = value[:, block * 256 : block * 256 + 256].astype(BF16)
    pltpu.make_async_copy(ring_out_ref, ring_out_ref, ring_send).wait()


def per_device(tokens, input_norm_scale, mean_input_weight, query_matrix, key_matrix, value_matrix,
               strength_weight, decay_input_weight, causal_filter_weight, head_decay_logrates,
               decay_input_shift, strength_shift, decay_spike, head_norm_scale,
               group_mixing_weight, mean_channel_scale, mean_output_weight, delta_output_weight):
    tok_rows, depth = tokens.shape
    heads = strength_weight.shape[1]
    n_z, n_x = lax.axis_size("sp_0"), lax.axis_size("sp_1")
    chunks = tok_rows // CHUNK
    pairs = heads * chunks
    width = n_z * n_x * 256
    pieces = width // PIECE
    vmem = pl.BlockSpec(memory_space=pltpu.VMEM)
    smem = pl.BlockSpec(memory_space=pltpu.SMEM)
    hbm = pl.BlockSpec(memory_space=pl.ANY)
    dma = pltpu.SemaphoreType.DMA
    return pl.pallas_call(
        lambda *refs: layer_kernel(heads, *refs),
        out_shape=jax.ShapeDtypeStruct((128, width), BF16),
        in_specs=[hbm] * 9 + [vmem] * 6 + [smem] * 3,
        out_specs=vmem,
        scratch_shapes=[
            pltpu.VMEM((tok_rows + HALO, depth), BF16),
            pltpu.VMEM((16, 272, 384), BF16),
            pltpu.VMEM((16, 256, 384), BF16),
            pltpu.VMEM((16, 256, 256), BF16),
            pltpu.VMEM((16, 512, 256), BF16),
            pltpu.VMEM((heads, tok_rows + HALO, 384), F32),
            pltpu.VMEM((tok_rows + HALO, 256), F32),
            pltpu.VMEM((tok_rows + HALO, 16), F32),
            pltpu.VMEM((8, depth), F32),
            pltpu.VMEM((3, CONV, 256), BF16),
            pltpu.VMEM((3, CONV, 256), F32),
            pltpu.VMEM((2, 128, 128), BF16),
            pltpu.VMEM((pairs, 8, CHUNK), F32),
            pltpu.VMEM((pairs, CHUNK, 128), F32),
            pltpu.VMEM((pairs, CHUNK, 128), F32),
            pltpu.VMEM((8, CHUNK, CHUNK), BF16),
            pltpu.VMEM((heads, 128, 256), F32),
            pltpu.VMEM((heads, tok_rows, 128), BF16),
            pltpu.VMEM((heads, tok_rows, 128), F32),
            pltpu.VMEM((heads, 128, 256), BF16),
            pltpu.VMEM((n_x, heads, 128, 256), BF16),
            pltpu.VMEM((heads, 128, 256), BF16),
            pltpu.VMEM((n_z, heads, 128, 256), BF16),
            pltpu.VMEM((heads, 128, 128), BF16),
            pltpu.VMEM((chunks, CHUNK, 512), BF16),
            pltpu.VMEM((3, pieces, 128, PIECE), F32),
            pltpu.VMEM((4, pieces, 128, PIECE), BF16),
            pltpu.VMEM((4, pieces, 128, PIECE), BF16),
            pltpu.VMEM((3, pieces, 128, PIECE), BF16),
            pltpu.VMEM((pieces, 128, PIECE), BF16),
            pltpu.VMEM((2, pieces, 128, PIECE), BF16),
            dma((chunks,)), dma((9,)), dma(()), dma((2,)),
            dma(()), dma((12,)), dma(()), dma((12,)), dma(()), dma((12,)), dma(()), dma((12,)),
            dma((heads,)), dma((heads,)), dma((heads,)), dma((heads,)),
            dma(()), dma((32,)), dma(()), dma((16,)),
            pltpu.SemaphoreType.REGULAR,
        ],
        compiler_params=pltpu.CompilerParams(
            vmem_limit_bytes=VMEM_LIMIT, collective_id=0, has_side_effects=True),
        name="layer",
    )(tokens, mean_input_weight, query_matrix, key_matrix, value_matrix, mean_output_weight,
      delta_output_weight, jnp.transpose(causal_filter_weight, (1, 0, 2)), group_mixing_weight,
      input_norm_scale.reshape(-1, 128), head_norm_scale.reshape(1, HEAD_DIM),
      mean_channel_scale.reshape(-1, 128), strength_weight.T, decay_input_weight.T, decay_spike.T,
      head_decay_logrates, decay_input_shift, strength_shift)


def solution(mesh):
    finer = Mesh(mesh.devices.reshape(4, 4, mesh.shape["tp"]), SP_TP)
    in_specs = (
        P(SP, None), P(), P(SP, "tp"), P(SP, "tp"), P(SP, "tp"), P(SP, "tp"), P(SP, "tp"),
        P(SP, "tp"), P(), P(), P(), P(), P(SP, "tp"), P(), P(), P(), P("tp", SP), P("tp", SP),
    )
    return jax.shard_map(
        per_device, mesh=finer, in_specs=in_specs, out_specs=P(SP_TP, None), check_vma=False
    )
```

```python
import jax
import jax.numpy as jnp
from jax import lax
from jax.experimental import pallas as pl
from jax.experimental.pallas import tpu as pltpu
from jax.sharding import Mesh
from jax.sharding import PartitionSpec as P

HEAD_DIM = 128
CONV = 4
CHUNK = 256
HALO = 16
EPSILON = 1e-06
SP = ("sp_0", "sp_1")
SP_TP = ("sp_0", "sp_1", "tp")
MESH_ID = pl.DeviceIdType.MESH
F32 = jnp.float32
BF16 = jnp.bfloat16
VMEM_LIMIT = 63 * 1000 * 1000


def dot(a, b):
    return jnp.dot(a, b, preferred_element_type=F32)


def dot_nt(a, b):
    return lax.dot_general(a, b, (((1,), (1,)), ((), ())), preferred_element_type=F32)


def dot_tn(a, b):
    return lax.dot_general(a, b, (((0,), (0,)), ((), ())), preferred_element_type=F32)


def unit_rows(values):
    return values * lax.rsqrt(jnp.sum(values * values, axis=-1, keepdims=True) + EPSILON)


def fill_masks(masks_ref):
    rows = lax.broadcasted_iota(jnp.int32, (CHUNK, CHUNK), 0)
    cols = lax.broadcasted_iota(jnp.int32, (CHUNK, CHUNK), 1)
    apart = jnp.bitwise_xor(rows, cols)
    for level in range(masks_ref.shape[0]):
        inside = (rows > cols) & (apart >= 2**level) & (apart < 2 ** (level + 1))
        masks_ref[level] = jnp.where(inside, 1.0, 0.0).astype(BF16)


def conv_rows(raw_ref, taps_ref, head, start, part):
    lanes = slice(part * 128, part * 128 + 128)
    tap_lanes = slice(head * 128, head * 128 + 128)
    rows = raw_ref[head, start + HALO - 8 : start + HALO + CHUNK, lanes]
    mixed = taps_ref[part, CONV - 1 : CONV, tap_lanes] * rows[8:]
    for back in range(1, CONV):
        tap = taps_ref[part, CONV - 1 - back : CONV - back, tap_lanes]
        mixed = mixed + tap * pltpu.roll(rows, back, 0)[8:]
    return mixed / (1.0 + jnp.exp(-mixed))


def delta_head(head, chunks, raw_ref, taps_ref, grow_ref, gcol_ref, bcol_ref, masks_ref, map_ref,
               from_state_ref, local_ref, events):
    rows = lax.broadcasted_iota(jnp.int32, (CHUNK, CHUNK), 0)
    cols = lax.broadcasted_iota(jnp.int32, (CHUNK, CHUNK), 1)
    work = []
    for chunk in range(chunks):
        row = head * chunks + chunk
        start = chunk * CHUNK
        query = unit_rows(conv_rows(raw_ref, taps_ref, head, start, 0)) * HEAD_DIM ** (-0.5)
        key = unit_rows(conv_rows(raw_ref, taps_ref, head, start, 1))
        value = conv_rows(raw_ref, taps_ref, head, start, 2)
        gcol, bcol, grow = gcol_ref[row], bcol_ref[row], grow_ref[row][0:1]
        key_b = key.astype(BF16)
        both = jnp.concatenate([query.astype(BF16), key_b], axis=0)
        inner = dot_nt(both, key_b)
        spread = jnp.exp(jnp.minimum(jnp.concatenate([gcol, gcol], axis=1) - grow, 0.0))
        scores = jnp.where(rows >= cols, inner[:CHUNK] * spread, 0.0).astype(BF16)
        strict = jnp.where(rows > cols, inner[CHUNK:] * spread, 0.0)
        strict = (strict * jnp.concatenate([bcol, bcol], axis=1)).astype(BF16)
        grown = jnp.exp(gcol)
        right = jnp.concatenate([value * bcol, key * bcol * grown], axis=1).astype(BF16)
        last = grow[:, CHUNK - 1 : CHUNK]
        key_dec = (key * jnp.exp(last - gcol)).astype(BF16)
        inverse = jnp.where(rows == cols, 1.0, 0.0).astype(BF16) - strict * masks_ref[0]
        work.append([strict, inverse, scores, right, key_dec, query * grown, jnp.exp(last)])
        events.get(("chunk", chunk), lambda: None)()
    for level in range(1, masks_ref.shape[0]):
        inner = [dot(w[0] * masks_ref[level], w[1]).astype(BF16) for w in work]
        for w, part in zip(work, inner):
            w[1] = w[1] - dot(w[1], part).astype(BF16)
        events.get(("level", level), lambda: None)()
    solved = [dot(w[1], w[3]).astype(BF16) for w in work]
    moved = [dot_tn(w[4], s) for w, s in zip(work, solved)]
    current = map_ref[head]
    starts = []
    for chunk in range(chunks):
        current_b = current.astype(BF16)
        starts.append(current_b)
        added = jnp.concatenate([jnp.zeros((128, 128), F32), moved[chunk][:, :128]], axis=1)
        current = (current * work[chunk][6] - dot(moved[chunk][:, 128:].astype(BF16), current_b)
                   + added)
    map_ref[head] = current
    events.get(("maps", 0), lambda: None)()
    seen = [dot(w[2], s) for w, s in zip(work, solved)]
    for chunk in range(chunks):
        where_rows = slice(chunk * CHUNK, chunk * CHUNK + CHUNK)
        asked = (work[chunk][5] - seen[chunk][:, 128:]).astype(BF16)
        answer = dot(asked, starts[chunk])
        from_state_ref[head, where_rows, :] = answer[:, :128].astype(BF16)
        local_ref[head, where_rows, :] = answer[:, 128:] + seen[chunk][:, :128]


SPLIT_A = 128
PIECE = 512
ORDER = ((0, 0), (0, 1), (0, -1), (1, 0), (-1, 0), (1, 1), (1, -1), (-1, 1), (-1, -1), (0, 2), (2, 0),
         (1, 2), (-1, 2), (2, 1), (2, -1), (2, 2))


class PlaneGather:
    def __init__(self, buf, split, send_sem, recv_sems):
        self.buf, self.split = buf, split
        self.send_sem, self.recv_sems = send_sem, recv_sems
        self.z, self.x = lax.axis_index("sp_0"), lax.axis_index("sp_1")

    def shard(self, dz, dx):
        return lax.rem(self.z + dz + 4, 4) * 4 + lax.rem(self.x + dx + 4, 4)

    def rows(self, part):
        split, total = self.split, self.buf.shape[1]
        quarter = split // 32 * 16
        rest = split + (total - split) // 32 * 16
        return {"a": (0, split), "b": (split, total), "a0": (0, quarter), "a1": (quarter, split),
                "b0": (split, rest), "b1": (rest, total)}[part]

    def send(self, group, source, part, way):
        low, high = self.rows(part)
        ref = self.buf.at[self.shard(*source), pl.ds(low, high - low), :]
        remote(ref, ref, self.send_sem, self.recv_sems.at[group],
               {"sp_0": lax.rem(self.z + way[0] + 4, 4),
                "sp_1": lax.rem(self.x + way[1] + 4, 4)}).start()

    def got(self, group, blocks, part=None):
        ref = self.buf.at[pl.ds(0, blocks)]
        if part is not None:
            low, high = self.rows(part)
            ref = self.buf.at[pl.ds(0, blocks), pl.ds(low, high - low), :]
        pltpu.make_async_copy(ref, ref, self.recv_sems.at[group]).wait()

    def got_own(self, along, part):
        name = "ab"[part] if along == "x" else "ba"[part]
        self.got(part if along == "x" else 8 + part, 2, name)

    def own(self, along="xz", parts=(0, 1)):
        for part in parts:
            for step in (1, -1):
                if "x" in along:
                    self.send(part, (0, 0), "ab"[part], (0, step))
                if "z" in along:
                    self.send(8 + part, (0, 0), "ba"[part], (step, 0))

    def quarters(self):
        self.send(2, (0, -1), "a0", (0, 1))
        self.send(2, (0, 1), "a1", (0, -1))
        self.send(2, (-1, 0), "b0", (1, 0))
        self.send(2, (1, 0), "b1", (-1, 0))

    def first(self, waits="xz", quarters_last=False):
        for along in waits:
            self.got_own(along, 0)
        if not quarters_last:
            self.quarters()
        for side, group in ((1, 3), (-1, 4)):
            for step in (1, -1):
                self.send(group, (0, side * step), "a", (step, 0))
                self.send(group, (side * step, 0), "b", (0, step))
        if quarters_last:
            self.quarters()

    def second(self, waits="xz"):
        for along in waits:
            self.got_own(along, 1)
        self.send(6, (-1, 0), "a", (1, 0))
        self.send(6, (0, -1), "b", (0, 1))

    def third(self):
        self.got(2, 1)
        for step, group in ((-1, 5), (1, 10)):
            self.send(group, (0, 2), "a", (step, 0))
            self.send(group, (2, 0), "b", (0, step))

    def fourth(self):
        self.got(3, 2)
        for at, group in ((1, 7), (-1, 10)):
            self.send(group, (-at, at), "a", (at, 0))
            self.send(group, (at, -at), "b", (0, at))

    def corners(self):
        self.got(4, 2)

    def fifth(self):
        self.got(5, 1)
        self.send(11, (1, 2), "a", (-1, 0))
        self.send(11, (2, 1), "b", (0, -1))

    def straight(self):
        self.got(6, 1)

    def last(self, stages=(0, 1, 2)):
        for stage in stages:
            self.got((7, 10, 11)[stage], (1, 2, 1)[stage])

    def drain(self):
        ref = self.buf.at[pl.ds(0, 15)]
        pltpu.make_async_copy(ref, ref, self.send_sem).wait()


def after(later, earlier):
    offset = jnp.concatenate([jnp.zeros((128, 128), F32), later[:, 128:].astype(F32)], axis=1)
    return dot(later[:, :128], earlier.astype(BF16)) + offset


def device_at(z=0, x=0, tp=0):
    place = {}
    for name, step in (("sp_0", z), ("sp_1", x), ("tp", tp)):
        if step:
            size = lax.axis_size(name)
            place[name] = lax.rem(lax.axis_index(name) + step + size, size)
    return place


def remote(src, dst, send_sem, recv_sem, place):
    return pltpu.make_async_remote_copy(
        src_ref=src, dst_ref=dst, send_sem=send_sem, recv_sem=recv_sem, device_id=place,
        device_id_type=MESH_ID)


def pooled_rows(pool_ref, chunk, position, wide, mix_ref, scales):
    parts = []
    for group in range(2):
        lanes = slice(group * 128, group * 128 + 128)
        rows = pool_ref[pl.ds(pl.multiple_of(chunk * CHUNK, CHUNK), CHUNK + HALO), lanes]
        reach = 1
        sums = rows
        for _ in range(group + 1):
            sums = sums + pltpu.roll(sums, reach, 0)
            reach *= 2
        broad = sums
        for _ in range(2):
            broad = broad + pltpu.roll(broad, reach, 0)
            reach *= 2
        short, long = 2 << group, 8 << group
        seen = lax.broadcasted_iota(jnp.int32, (CHUNK, 128), 0) + (position + chunk * CHUNK + 1)
        count = jnp.minimum(seen, jnp.where(wide, long, short)).astype(F32)
        window = jnp.where(wide, broad[HALO:], sums[HALO:])
        diff = (window / count - rows[HALO:]).astype(BF16)
        parts.append((dot(diff, mix_ref[group]) * scales[group]).astype(BF16))
    return parts


def norm_rows(tok_ref, gain_ref, start, count, step_rows):
    @pl.loop(0, count // step_rows)
    def _(step):
        rows = pl.ds(pl.multiple_of(start + step * step_rows, 16), step_rows)
        values = tok_ref[rows, :].astype(F32)
        scale = lax.rsqrt(jnp.mean(values * values, axis=-1, keepdims=True) + EPSILON)
        tok_ref[rows, :] = (tok_ref[rows, :].astype(F32) * scale * gain_ref[0:1, :]).astype(BF16)


def layer_kernel(heads, tok_hbm, pool_hbm, query_hbm, key_hbm, value_hbm, pool_out_hbm,
                 delta_out_hbm, taps_hbm, mix_hbm, gain_in_ref, head_gain_ref, scale_in_ref,
                 strength_ref, decay_ref, spike_ref, rate_ref, decay_shift_ref, strength_shift_ref,
                 out_ref,
                 tok_ref, wide_ref, next_ref, pool_w_ref, out_w_ref, acc_ref, pool_ref, thin_ref, gain_ref,
                 taps_in_ref, taps_ref, mix_ref, grow_ref, gcol_ref, bcol_ref, masks_ref, map_ref,
                 from_state_ref, local_ref, own_ref, row_ref, total_ref, column_ref, state_ref,
                 mixed_ref, part_ref, pair_out_ref, pair_in_ref, ring_out_ref, half_ref, final_ref,
                 result_ref,
                 tok_sems, load_sems, halo_send, halo_recv, send_a, recv_a, send_d, recv_d, send_b, recv_b,
                 send_c, recv_c, send_x, recv_x, send_z, recv_z, pair_send, pair_recv, ring_send,
                 ring_recv, out_sem, gate):
    z, x, tp = lax.axis_index("sp_0"), lax.axis_index("sp_1"), lax.axis_index("tp")
    n_z, n_x, n_tp = lax.axis_size("sp_0"), lax.axis_size("sp_1"), lax.axis_size("tp")
    y, core = tp // 2, lax.rem(tp, 2)
    n_y = n_tp // 2
    tok_rows, depth = tok_hbm.shape
    chunks = tok_rows // CHUNK
    mine = z * n_x + x
    position = mine * tok_rows
    loads = []
    for k, (hbm, ref) in enumerate((
            (query_hbm.at[:, pl.ds(0, 128)], wide_ref.at[mine, pl.ds(0, 256), pl.ds(0, 128)]),
            (key_hbm.at[:, pl.ds(0, 128)], wide_ref.at[mine, pl.ds(0, 256), pl.ds(128, 128)]),
            (value_hbm.at[:, pl.ds(0, 128)], wide_ref.at[mine, pl.ds(0, 256), pl.ds(256, 128)]),
            (query_hbm.at[:, pl.ds(128, 128)], next_ref.at[mine, :, pl.ds(0, 128)]),
            (key_hbm.at[:, pl.ds(128, 128)], next_ref.at[mine, :, pl.ds(128, 128)]),
            (value_hbm.at[:, pl.ds(128, 128)], next_ref.at[mine, :, pl.ds(256, 128)]),
            (pool_hbm, pool_w_ref.at[mine]),
            (pool_out_hbm, out_w_ref.at[mine, pl.ds(0, 256), :]),
            (delta_out_hbm, out_w_ref.at[mine, pl.ds(256, 256), :]),
            (taps_hbm.at[:, :, pl.ds(pl.multiple_of(tp * 256, 256), 256)], taps_in_ref),
            (mix_hbm.at[pl.ds(tp * 2, 2)], mix_ref))):
        load = pltpu.make_async_copy(hbm, ref, load_sems.at[max(k - 2, 0)])
        load.start()
        loads.append(load)
    own_block = wide_ref.at[mine, pl.ds(0, 256), :]
    tok_loads = []
    for k in range(chunks):
        load = pltpu.make_async_copy(
            tok_hbm.at[pl.ds(k * CHUNK, CHUNK), :],
            tok_ref.at[pl.ds(HALO + k * CHUNK, CHUNK), :], tok_sems.at[k])
        load.start()
        tok_loads.append(load)
    following, before = lax.rem(mine + 1, 16), lax.rem(mine + 15, 16)
    next_place = {"sp_0": following // 4, "sp_1": lax.rem(following, 4)}
    last_place = {"sp_0": before // 4, "sp_1": lax.rem(before, 4)}
    peers = [device_at(x=step) for step in range(1, n_x)]
    peers += [device_at(z=step) for step in range(1, n_z)]
    peers += [device_at(tp=step) for step in range(1, n_tp)]
    peers += [next_place, last_place]
    barrier = pltpu.get_barrier_semaphore()
    for peer in peers:
        pl.semaphore_signal(barrier, 1, device_id=peer, device_id_type=MESH_ID)
    at = lax.broadcasted_iota(jnp.int32, (16, 256), 0)
    thin = jnp.zeros((16, 256), F32)
    for k, (ref, row) in enumerate(((strength_ref, 0), (strength_ref, 1), (decay_ref, 0),
                                    (decay_ref, 1))):
        row_values = ref[...].astype(F32)[row : row + 1]
        thin = jnp.where(at == k, jnp.broadcast_to(row_values, (16, 256)), thin)
    wide_ref[mine, 256:272, 0:256] = thin.astype(BF16)
    wide_ref[mine, 256:272, 256:384] = jnp.zeros((16, 128), BF16)
    pltpu.make_async_copy(own_block, own_block, load_sems.at[0]).wait()
    pl.semaphore_wait(barrier, len(peers))

    early = PlaneGather(wide_ref, SPLIT_A, send_a, recv_a)
    slices = depth // n_tp

    def halo_part(owner):
        return tok_ref.at[pl.ds(0, HALO), pl.ds(pl.multiple_of(owner * slices, 128), slices)]

    halos = [remote(
        tok_hbm.at[pl.ds(tok_rows - HALO, HALO), pl.ds(pl.multiple_of(tp * slices, 128), slices)],
        halo_part(tp), halo_send, halo_recv.at[0], next_place)]
    halos[0].start()
    early.own()
    gains = gain_in_ref[...].astype(F32)
    for k in range(depth // 128):
        gain_ref[:, k * 128 : k * 128 + 128] = jnp.broadcast_to(gains[k : k + 1], (8, 128))
    for k in range(chunks):
        tok_loads[k].wait()
        norm_rows(tok_ref, gain_ref, HALO + k * CHUNK, CHUNK, 64)
    early.first()
    halos[0].wait_recv()
    for step in range(1, n_tp):
        remote(halo_part(tp), halo_part(tp), halo_send, halo_recv.at[1],
               device_at(tp=step)).start()
    early.second()
    others = tok_ref.at[pl.ds(0, HALO), pl.ds(0, depth - slices)]
    pltpu.make_async_copy(others, others, halo_recv.at[1]).wait()
    sent = tok_ref.at[pl.ds(0, HALO), :]
    pltpu.make_async_copy(sent, sent, halo_send).wait()

    @pl.when(mine == 0)
    def _():
        tok_ref[0:HALO, :] = jnp.zeros((HALO, depth), BF16)

    norm_rows(tok_ref, gain_ref, 0, HALO, HALO)
    fill_masks(masks_ref)
    tile = 208

    def project(gather, places, into, first=False):
        @pl.loop(0, tok_ref.shape[0] // tile)
        def _(step):
            rows = pl.ds(pl.multiple_of(step * tile, 16), tile)
            total = None if first else into[rows, :]
            narrow = None if first or gather is not early else thin_ref[rows, :]
            for dz, dx in places:
                shard = gather.shard(dz, dx)
                normed = tok_ref[rows, pl.ds(pl.multiple_of(shard * 256, 256), 256)]
                term = dot(normed, gather.buf[shard, 0:256, :])
                total = term if total is None else total + term
                if gather is early:
                    term = dot_nt(normed, gather.buf[shard, 256:272, 0:256])
                    narrow = term if narrow is None else narrow + term
            into[rows, :] = total
            if gather is early:
                thin_ref[rows, :] = narrow

    first_acc, second_acc = acc_ref.at[0], acc_ref.at[1]
    partner = {"tp": y * 2 + (1 - core)}

    def meet():
        pl.semaphore_signal(gate, 1, device_id=partner, device_id_type=MESH_ID)
        pl.semaphore_wait(gate, 1)

    project(early, ORDER[:1], first_acc, first=True)
    early.third()
    for load in loads[3:]:
        load.wait()
    early.fourth()
    project(early, ORDER[1:5], first_acc)
    early.corners()
    early.fifth()
    later = PlaneGather(next_ref, SPLIT_A, send_d, recv_d)
    meet()
    later.own()
    project(early, ORDER[5:9], first_acc)
    early.straight()
    project(early, ORDER[9:11], first_acc)
    early.last()
    later.first()
    project(early, ORDER[11:], first_acc)
    later.second()

    taps_ref[...] = taps_in_ref[...].astype(F32)
    narrow = thin_ref[HALO:, :].T
    for head in range(heads):
        strength = narrow[head : head + 1] + strength_shift_ref[tp * heads + head]
        beta = 1.0 / (1.0 + jnp.exp(-strength))
        level = narrow[heads + head : heads + head + 1] + decay_shift_ref[tp * heads + head]
        soft = jnp.maximum(level, 0.0) + jnp.log1p(jnp.exp(-jnp.abs(level)))
        rate = jnp.exp(jnp.full((1, tok_rows), rate_ref[tp * heads + head], F32))
        decay = spike_ref[head : head + 1, :] - rate * soft
        lane = lax.rem(lax.broadcasted_iota(jnp.int32, (8, tok_rows), 1), CHUNK)
        summed = jnp.broadcast_to(decay, (8, tok_rows))
        step = 1
        while step < CHUNK:
            summed = summed + jnp.where(lane >= step, pltpu.roll(summed, step, 1), 0.0)
            step *= 2
        for chunk in range(chunks):
            row = head * chunks + chunk
            part = slice(chunk * CHUNK, chunk * CHUNK + CHUNK)
            grow_ref[row] = summed[:, part]
            gcol_ref[row] = jnp.broadcast_to(summed[0:1, part], (128, CHUNK)).T
            bcol_ref[row] = jnp.broadcast_to(beta[:, part], (128, CHUNK)).T
    rows = lax.broadcasted_iota(jnp.int32, (128, 256), 0)
    cols = lax.broadcasted_iota(jnp.int32, (128, 256), 1)
    identity = jnp.where(rows == cols, 1.0, 0.0)
    for head in range(heads):
        map_ref[head] = identity

    pool = PlaneGather(pool_w_ref, 128, send_b, recv_b)
    out = PlaneGather(out_w_ref, 256, send_c, recv_c)
    along_x, along_z = {}, {}

    def delta(head, events):
        delta_head(head, chunks, acc_ref, taps_ref, grow_ref, gcol_ref, bcol_ref, masks_ref,
                   map_ref, from_state_ref, local_ref, events)

    def send_x_maps(head):
        own_ref[head] = map_ref[head].astype(BF16)
        row_ref[0, head] = own_ref[head]
        along_x[head] = [
            remote(own_ref.at[head], row_ref.at[step, head], send_x.at[head], recv_x.at[head],
                   device_at(x=step)) for step in range(1, n_x)]
        for copy in along_x[head]:
            copy.start()

    def send_z_maps(head):
        moved = row_ref.at[pl.ds(1, n_x - 1), head]
        pltpu.make_async_copy(moved, moved, recv_x.at[head]).wait()
        so_far = before_here = identity
        for k in range(n_x):
            piece = row_ref[lax.rem(x - k + n_x, n_x), head]
            so_far = piece.astype(F32) if k == 0 else after(piece, so_far)
            before_here = jnp.where(k < x, so_far, before_here)
        map_ref[head] = before_here
        total_ref[head] = so_far.astype(BF16)
        column_ref[0, head] = total_ref[head]
        along_z[head] = [
            remote(total_ref.at[head], column_ref.at[step, head], send_z.at[head],
                   recv_z.at[head], device_at(z=step)) for step in range(1, n_z)]
        for copy in along_z[head]:
            copy.start()

    def enter(head):
        moved = column_ref.at[pl.ds(1, n_z - 1), head]
        pltpu.make_async_copy(moved, moved, recv_z.at[head]).wait()
        so_far = state = jnp.zeros((128, 128), F32)
        for k in range(n_z - 1):
            piece = column_ref[lax.rem(z - k + n_z, n_z), head]
            offset = piece[:, 128:].astype(F32)
            so_far = offset if k == 0 else dot(piece[:, :128], so_far.astype(BF16)) + offset
            state = jnp.where(k < z, so_far, state)
        entering = dot(map_ref[head, :, 0:128].astype(BF16), state.astype(BF16))
        state_ref[head] = (entering + map_ref[head, :, 128:256]).astype(BF16)

    delta(0, {("chunk", 2): later.third, ("level", 2): later.fourth})
    later.fifth()
    send_x_maps(0)
    meet()
    pool.own()
    project(later, ORDER[:5], second_acc, first=True)
    later.corners()
    project(later, ORDER[5:9], second_acc)
    later.straight()
    project(later, ORDER[9:11], second_acc)
    later.last()
    project(later, ORDER[11:], second_acc)
    delta(1, {("chunk", 2): pool.first, ("chunk", 3): lambda: send_z_maps(0),
              ("maps", 0): lambda: send_x_maps(1)})
    pool.second()
    pool.third()
    project(pool, ORDER[:5], pool_ref, first=True)
    pool.fourth()
    enter(0)
    pool.corners()
    project(pool, ORDER[5:9], pool_ref)
    pool.fifth()
    out.own("x")
    send_z_maps(1)
    out.own("z")
    wide = core == 1
    scales_at = lax.broadcasted_iota(jnp.int32, scale_in_ref.shape, 0)
    scales = [jnp.sum(jnp.where(scales_at == tp * 2 + group, scale_in_ref[...].astype(F32), 0.0),
                      axis=0, keepdims=True) for group in range(2)]

    def store_halves(chunk, lanes, values):
        for half in range(2):
            slot = lax.rem(half + core, 2)
            mixed_ref[chunk, pl.ds(pl.multiple_of(slot * 128, 128), 128), lanes] = (
                values[half * 128 : half * 128 + 128])

    pool.straight()
    pool.last()
    project(pool, ORDER[9:], pool_ref)

    @pl.loop(0, chunks)
    def _(chunk):
        for group, values in enumerate(
                pooled_rows(pool_ref, chunk, position, wide, mix_ref, scales)):
            store_halves(chunk, slice(group * 128, group * 128 + 128), values)

    enter(1)

    head_gain = head_gain_ref[...].astype(F32)
    pairs = {}
    slots = {2: 0, 1: 1, 3: 2, 0: 0}

    def finish_rows(ahead):
        chunk = lax.rem(y + ahead, n_y)
        where_rows = pl.ds(pl.multiple_of(chunk * CHUNK, CHUNK), CHUNK)
        for head in range(heads):
            raw = dot(from_state_ref[head, where_rows, :], state_ref[head])
            raw = raw + local_ref[head, where_rows, :]
            squares = jnp.mean(raw * raw, axis=-1, keepdims=True)
            normed = (raw * lax.rsqrt(squares + EPSILON) * head_gain).astype(BF16)
            store_halves(chunk, slice(256 + head * 128, 384 + head * 128), normed)

    def produce(ahead, piece):
        chunk = lax.rem(y + ahead, n_y)
        for block, (dz, dx) in enumerate(ORDER[2 * piece : 2 * piece + 2]):
            lanes = slice(block * 256, block * 256 + 256)
            product = dot(mixed_ref[chunk], out_w_ref[out.shard(dz, dx)])
            part_ref[slots[ahead], piece, :, lanes] = product[:128]
            pair_out_ref[ahead, piece, :, lanes] = product[128:].astype(BF16)
        index = ahead * 8 + piece if ahead else 0
        copy = remote(pair_out_ref.at[ahead, piece], pair_in_ref.at[ahead, piece],
                      pair_send, pair_recv.at[index], partner)
        copy.start()
        pairs[ahead, piece] = copy

    def chip_sum(ahead, piece):
        pairs[ahead, piece].wait_recv()
        return part_ref[slots[ahead], piece] + pair_in_ref[ahead, piece].astype(F32)

    up, down = device_at(tp=2), device_at(tp=-2)
    half = 64
    top, bottom = slice(0, half), slice(half, 2 * half)

    def pass_on(group, ahead, piece, rows, value, place, target):
        ring_out_ref[ahead - 1, piece, rows, :] = value.astype(BF16)
        where_rows = pl.ds(rows.start, half)
        copy = remote(ring_out_ref.at[ahead - 1, piece, where_rows],
                      target.at[piece, where_rows], ring_send, ring_recv.at[group], place)
        copy.start()

    def far(piece):
        value = chip_sum(2, piece)
        pass_on(piece, 2, piece, top, value[top], up, half_ref)
        pass_on(piece, 2, piece, bottom, value[bottom], down, half_ref)

    def near(piece):
        for ahead, rows, place, side in ((1, bottom, up, 0), (3, top, down, 1)):
            value = chip_sum(ahead, piece)
            part_ref[slots[ahead], piece] = value
            pass_on(8 + piece, ahead, piece, rows, value[rows], place, final_ref.at[side])

    def merged(piece):
        pltpu.make_async_copy(half_ref.at[piece], half_ref.at[piece], ring_recv.at[piece]).wait()
        for ahead, rows, place, side in ((1, top, up, 0), (3, bottom, down, 1)):
            value = part_ref[slots[ahead], piece, rows, :] + half_ref[piece, rows, :].astype(F32)
            pass_on(8 + piece, ahead, piece, rows, value, place, final_ref.at[side])

    def send_piece(piece):
        produce(2, piece)
        produce(1, piece)
        produce(3, piece)
        far(piece)
        near(piece)

    finish_rows(2)
    out.first(quarters_last=True)
    out.got_own("x", 1)
    produce(2, 0)
    finish_rows(1)
    finish_rows(3)
    produce(1, 0)
    far(0)
    produce(3, 0)
    near(0)
    out.second(waits="z")
    send_piece(1)
    finish_rows(0)
    merged(0)
    out.fourth()
    out.corners()
    send_piece(2)
    out.third()
    merged(1)
    send_piece(3)
    out.fifth()
    for piece in range(4):
        produce(0, piece)
    merged(2)
    out.straight()
    send_piece(4)
    merged(3)
    out.last((0,))
    produce(2, 5)
    far(5)
    merged(4)
    out.last((1,))
    produce(2, 6)
    far(6)
    produce(1, 5)
    produce(3, 5)
    near(5)
    merged(5)
    out.last((2,))
    produce(2, 7)
    far(7)
    for piece in (6, 7):
        produce(1, piece)
        produce(3, piece)
        near(piece)
        merged(piece)
    for piece in range(4, 8):
        produce(0, piece)
    for gather in (early, later, pool, out):
        gather.drain()
    for head in range(heads):
        for ref, sem in ((row_ref, send_x), (column_ref, send_z)):
            moved = ref.at[pl.ds(1, n_x - 1), head]
            pltpu.make_async_copy(moved, moved, sem.at[head]).wait()
    pltpu.make_async_copy(pair_in_ref.at[0], pair_in_ref.at[0], pair_recv.at[0]).wait()
    for piece in range(8):
        part_ref[0, piece] = part_ref[0, piece] + pair_in_ref[0, piece].astype(F32)
    pltpu.make_async_copy(pair_out_ref, pair_out_ref, pair_send).wait()
    for piece in range(8):
        arrived = final_ref.at[:, piece]
        pltpu.make_async_copy(arrived, arrived, ring_recv.at[8 + piece]).wait()
        value = part_ref[0, piece] + final_ref[0, piece].astype(F32)
        value = value + final_ref[1, piece].astype(F32)
        for block, (dz, dx) in enumerate(ORDER[2 * piece : 2 * piece + 2]):
            lanes = pl.ds(pl.multiple_of(out.shard(dz, dx) * 256, 256), 256)
            index = 2 * piece + block
            result_ref[index] = value[:, block * 256 : block * 256 + 256].astype(BF16)
            pltpu.make_async_copy(result_ref.at[index], out_ref.at[:, lanes], out_sem).start()
    pltpu.make_async_copy(result_ref, result_ref, out_sem).wait()
    pltpu.make_async_copy(ring_out_ref, ring_out_ref, ring_send).wait()


def per_device(tokens, input_norm_scale, mean_input_weight, query_matrix, key_matrix, value_matrix,
               strength_weight, decay_input_weight, causal_filter_weight, head_decay_logrates,
               decay_input_shift, strength_shift, decay_spike, head_norm_scale,
               group_mixing_weight, mean_channel_scale, mean_output_weight, delta_output_weight):
    tok_rows, depth = tokens.shape
    heads = strength_weight.shape[1]
    n_z, n_x = lax.axis_size("sp_0"), lax.axis_size("sp_1")
    chunks = tok_rows // CHUNK
    pairs = heads * chunks
    width = n_z * n_x * 256
    pieces = width // PIECE
    vmem = pl.BlockSpec(memory_space=pltpu.VMEM)
    smem = pl.BlockSpec(memory_space=pltpu.SMEM)
    hbm = pl.BlockSpec(memory_space=pl.ANY)
    dma = pltpu.SemaphoreType.DMA
    return pl.pallas_call(
        lambda *refs: layer_kernel(heads, *refs),
        out_shape=jax.ShapeDtypeStruct((128, width), BF16),
        in_specs=[hbm] * 9 + [vmem] * 6 + [smem] * 3,
        out_specs=hbm,
        scratch_shapes=[
            pltpu.VMEM((tok_rows + HALO, depth), BF16),
            pltpu.VMEM((16, 272, 384), BF16),
            pltpu.VMEM((16, 256, 384), BF16),
            pltpu.VMEM((16, 256, 256), BF16),
            pltpu.VMEM((16, 512, 256), BF16),
            pltpu.VMEM((heads, tok_rows + HALO, 384), F32),
            pltpu.VMEM((tok_rows + HALO, 256), F32),
            pltpu.VMEM((tok_rows + HALO, 16), F32),
            pltpu.VMEM((8, depth), F32),
            pltpu.VMEM((3, CONV, 256), BF16),
            pltpu.VMEM((3, CONV, 256), F32),
            pltpu.VMEM((2, 128, 128), BF16),
            pltpu.VMEM((pairs, 8, CHUNK), F32),
            pltpu.VMEM((pairs, CHUNK, 128), F32),
            pltpu.VMEM((pairs, CHUNK, 128), F32),
            pltpu.VMEM((8, CHUNK, CHUNK), BF16),
            pltpu.VMEM((heads, 128, 256), F32),
            pltpu.VMEM((heads, tok_rows, 128), BF16),
            pltpu.VMEM((heads, tok_rows, 128), F32),
            pltpu.VMEM((heads, 128, 256), BF16),
            pltpu.VMEM((n_x, heads, 128, 256), BF16),
            pltpu.VMEM((heads, 128, 256), BF16),
            pltpu.VMEM((n_z, heads, 128, 256), BF16),
            pltpu.VMEM((heads, 128, 128), BF16),
            pltpu.VMEM((chunks, CHUNK, 512), BF16),
            pltpu.VMEM((3, pieces, 128, PIECE), F32),
            pltpu.VMEM((4, pieces, 128, PIECE), BF16),
            pltpu.VMEM((4, pieces, 128, PIECE), BF16),
            pltpu.VMEM((3, pieces, 128, PIECE), BF16),
            pltpu.VMEM((pieces, 128, PIECE), BF16),
            pltpu.VMEM((2, pieces, 128, PIECE), BF16),
            pltpu.VMEM((width // 256, 128, 256), BF16),
            dma((chunks,)), dma((9,)), dma(()), dma((2,)),
            dma(()), dma((12,)), dma(()), dma((12,)), dma(()), dma((12,)), dma(()), dma((12,)),
            dma((heads,)), dma((heads,)), dma((heads,)), dma((heads,)),
            dma(()), dma((32,)), dma(()), dma((16,)),
            dma(()), pltpu.SemaphoreType.REGULAR,
        ],
        compiler_params=pltpu.CompilerParams(
            vmem_limit_bytes=VMEM_LIMIT, collective_id=0, has_side_effects=True),
        name="layer",
    )(tokens, mean_input_weight, query_matrix, key_matrix, value_matrix, mean_output_weight,
      delta_output_weight, jnp.transpose(causal_filter_weight, (1, 0, 2)), group_mixing_weight,
      input_norm_scale.reshape(-1, 128), head_norm_scale.reshape(1, HEAD_DIM),
      mean_channel_scale.reshape(-1, 128), strength_weight.T, decay_input_weight.T, decay_spike.T,
      head_decay_logrates, decay_input_shift, strength_shift)


def solution(mesh):
    finer = Mesh(mesh.devices.reshape(4, 4, mesh.shape["tp"]), SP_TP)
    in_specs = (
        P(SP, None), P(), P(SP, "tp"), P(SP, "tp"), P(SP, "tp"), P(SP, "tp"), P(SP, "tp"),
        P(SP, "tp"), P(), P(), P(), P(), P(SP, "tp"), P(), P(), P(), P("tp", SP), P("tp", SP),
    )
    return jax.shard_map(
        per_device, mesh=finer, in_specs=in_specs, out_specs=P(SP_TP, None), check_vma=False
    )
```
